32 devices in a mesh: ep: 8 (over z, core), tp: 4 (over y, x).
Axes of the slice: x: 2, y: 2, z: 4, core: 2. Of those that a mesh axis runs over, the one named last changes fastest.
Arguments:
- queries: bfloat16 [1024, 4096], P('ep', 'tp'), may hold values from -32 to 32
- keys: bfloat16 [1024, 2048], P('ep', 'tp'), may hold values from -32 to 32
- values: bfloat16 [1024, 2048], P('ep', 'tp'), may hold values from -6 to 6
- query_gain: float32 [128], replicated, may hold values from 1 to 6
- key_gain: float32 [128], replicated, may hold values from 1 to 6
- out_weight: bfloat16 [4096, 2048], P('tp'), may hold values from -0.75 to 0.75
- expert_input: bfloat16 [1024, 2048], P('ep'), may hold values from -64 to 64
- norm_gain: float32 [2048], replicated, may hold values from 0.1 to 1.9
- routes: int32 [1024, 2], P('ep'), may hold values from 0 to 7, all different within a row; in each aligned block of 128 rows (0 to 127, 128 to 255, ...) at most 40 rows name the same one
- route_logits: float32 [1024, 2], P('ep'), may hold values from -6 to 6
- gate_weight: bfloat16 [8, 2048, 2816], P('ep', None, 'tp'), may hold values from -0.125 to 0.125
- up_weight: bfloat16 [8, 2048, 2816], P('ep', None, 'tp'), may hold values from -0.125 to 0.125
- down_weight: bfloat16 [8, 2816, 2048], P('ep', 'tp'), may hold values from -0.109375 to 0.109375
Outputs:
- mixed: bfloat16 [1024, 2048], P(('ep', 'tp'))
- expert_out: bfloat16 [1024, 2048], P('ep', 'tp')
The draws below stay inside these ranges and needn't reach their ends.
Inputs may be any that keep to these rules, and one draw needn't show every extreme that they name: `routes`: A token's 2 experts differ. Among the 128 tokens of one index of ep (aligned blocks), no expert is named by more than 40 tokens, a bound that some block reaches.
All inputs are finite; a program needn't handle non-finite values.
Results may differ from the reference program's by a relative error of at most 0.015.
The reference program's roundings to bfloat16 on the way count: a program that leaves them out, or rounds other values in their place, can miss the bound.
Values may be sent and summed in bfloat16 or wider, within the bound.
A program may use at most 64 MiB of HBM per device.

```python
import math
import jax
import jax.numpy as jnp
import numpy as np
from jax import lax

D = 2048
HEADS = 32
KV_HEADS = 16
HEAD_DIM = 128
GROUP = 2
GRID_W = 64
FF_E = 2816
TOP_K = 2
TOK_B = 128
TOKENS_A = 1024
TOKENS_B = 1024
EXPERTS = 8
CAP = 40
N_EP = 8
N_TP = 4


def query_key_pair(key):
    base = jax.random.fold_in(key, 5)
    key_q, key_k, scale_q, scale_k = jax.random.split(base, 4)
    q_cols = HEADS * HEAD_DIM
    k_cols = KV_HEADS * HEAD_DIM
    q_raw = jnp.clip(jax.random.normal(key_q, (TOKENS_A, q_cols), jnp.float32), -6.0, 6.0)
    k_raw = jnp.clip(jax.random.normal(key_k, (TOKENS_A, k_cols), jnp.float32), -6.0, 6.0)
    q_scale = jnp.exp(jax.random.uniform(scale_q, (q_cols,), jnp.float32, jnp.log(0.5), jnp.log(5.0)))
    k_scale = jnp.exp(jax.random.uniform(scale_k, (k_cols,), jnp.float32, jnp.log(0.5), jnp.log(5.0)))
    q_data = q_raw * q_scale
    k_data = k_raw * k_scale
    return (jnp.clip(q_data, -32.0, 32.0), jnp.clip(k_data, -32.0, 32.0))


def draw_queries(key, part):
    return query_key_pair(key)[0].astype(jnp.bfloat16)


def draw_keys(key, part):
    return query_key_pair(key)[1].astype(jnp.bfloat16)


def draw_query_gain(key, part):
    own = jax.random.fold_in(key, 11)
    return jax.random.uniform(own, (HEAD_DIM,), jnp.float32, 1.0, 1.8)


def draw_key_gain(key, part):
    own = jax.random.fold_in(key, 13)
    return jax.random.uniform(own, (HEAD_DIM,), jnp.float32, 1.0, 1.8)


def draw_expert_input(key, part):
    own = jax.random.fold_in(key, 17)
    key_x, key_row, key_col = jax.random.split(own, 3)
    col_scale = jnp.exp(jax.random.uniform(key_col, (D,), jnp.float32, jnp.log(0.3), jnp.log(3.0)))
    raw = jnp.clip(jax.random.normal(key_x, (TOKENS_B, D), jnp.float32), -6.0, 6.0)
    row_scale = jnp.exp(jax.random.uniform(key_row, (TOKENS_B, 1), jnp.float32, jnp.log(0.3), jnp.log(3.0)))
    return jnp.clip(raw * row_scale * col_scale, -64.0, 64.0).astype(jnp.bfloat16)


def steps_of(stream_key, shape, cuts, least, largest):
    def one(axis_at, blocks):
        draws = jax.random.uniform(jax.random.fold_in(jax.random.fold_in(stream_key, 6), axis_at), (blocks,), jnp.float32, least / len(cuts), largest / len(cuts))
        return jnp.repeat(jnp.exp(draws), shape[axis_at] // blocks).reshape((-1,) + (1,) * (len(shape) - axis_at - 1))

    level = one(*cuts[0])
    for cut in cuts[1:]:
        level = level * one(*cut)
    return level


def deal_out(own_key, own, number, rows, number_of, top, limit, skew):
    sequence = jax.random.permutation(own_key, number_of)
    crowded, ordinary = load_shares(number_of, rows * top, limit, skew, True), load_shares(number_of, rows * top, limit, skew, False)
    places = jnp.arange(number_of)

    def named(lengths, turn):
        used = int((lengths > 0).sum())
        fixed = max(1, used // 4)
        moved = fixed + (places - fixed + turn * (used - fixed)) % max(1, number_of - fixed)
        return jnp.zeros((number_of,), jnp.int32).at[sequence[jnp.where(places < fixed, places, moved)]].set(jnp.asarray(lengths, jnp.int32))

    lengths = jnp.where(number % 4 == 0, named(crowded, number // 4), named(ordinary, number - number // 4 - 1))
    mixed = jax.random.permutation(jax.random.fold_in(own, 3), number_of)
    giver, taker = mixed[0:number_of // 2 * 2:2], mixed[1:number_of // 2 * 2:2]
    room = jnp.minimum(lengths[giver] - 1, limit - lengths[taker]) // 2
    room = jnp.where((giver == sequence[0]) | (taker == sequence[0]) | (lengths[taker] == 0), 0, jnp.maximum(room, 0))
    moved = jax.random.randint(jax.random.fold_in(own, 4), (number_of // 2,), 0, 1 << 20) % (room + 1)
    lengths = lengths.at[giver].add(-moved).at[taker].add(moved)
    labels = jnp.searchsorted(jnp.cumsum(lengths), jnp.arange(rows * top), side="right").astype(jnp.int32)
    table = labels.reshape(top, rows).T
    table = table[jax.random.permutation(jax.random.fold_in(own, 1), rows)]
    turn = jax.random.randint(jax.random.fold_in(own, 2), (rows, 1), 0, top)
    return jnp.take_along_axis(table, (jnp.arange(top)[None, :] + turn) % top, axis=1)


def load_shares(number_of, total, limit, skew, full):
    portions = [(1 << 20) // math.isqrt(rank ** skew) + 1 for rank in range(1, number_of + 1)]
    largest = limit if full else min(limit, max(-(-total // number_of), total * portions[0] // sum(portions)))
    least = 1 if total - largest >= number_of - 1 else 0
    counts, surplus = [largest] + [least] * (number_of - 1), total - largest - least * (number_of - 1)
    while surplus > 0:
        movable = [i for i in range(1, number_of) if counts[i] < largest] or [i for i in range(1, number_of) if counts[i] < limit]
        pool, remaining = sum([portions[i] for i in movable]), surplus
        for i in movable:
            extra = min(limit - counts[i], max(1, remaining * portions[i] // pool), surplus)
            counts[i] = counts[i] + extra
            surplus = surplus - extra
    return np.array(counts)


def centred(stream_key, extent, deviation, limit, pieces=(), kind=jnp.bfloat16):
    result = deviation * jax.random.normal(stream_key, extent, jnp.float32)
    if pieces:
        result = result * steps_of(stream_key, extent, pieces, -0.22, 0.18)
    return jnp.clip(result, -limit, limit).astype(kind)


def setup_inputs(seed: int = 0) -> dict:
    seeds = jax.random.split(jax.random.key(seed), 14)
    queries = draw_queries(jax.random.fold_in(seeds[13], 71), 0)
    keys = draw_keys(jax.random.fold_in(seeds[13], 71), 0)
    values = centred(seeds[2], (TOKENS_A, KV_HEADS * HEAD_DIM), 1.0, 6.0, ((0, 8), (1, 4)))
    query_gain = draw_query_gain(jax.random.fold_in(seeds[13], 71), 0)
    key_gain = draw_key_gain(jax.random.fold_in(seeds[13], 71), 0)
    out_weight = centred(seeds[5], (HEADS * HEAD_DIM, D), (HEADS * HEAD_DIM // 64) ** -0.5, 0.75, ((0, 4),))
    expert_input = draw_expert_input(jax.random.fold_in(seeds[13], 71), 0)
    norm_gain = jnp.clip(1.0 + 0.18 * jax.random.normal(seeds[7], (D,), jnp.float32), 0.1, 1.9)
    routes_keys = jax.random.split(jax.random.fold_in(seeds[8], 1), TOKENS_B // TOK_B)
    routes_turns = jax.random.permutation(jax.random.fold_in(seeds[8], 3), TOKENS_B // TOK_B)
    routes = jax.vmap(lambda own, number: deal_out(jax.random.fold_in(seeds[8], 2), own, number, TOK_B, EXPERTS, TOP_K, CAP, 0))(routes_keys, routes_turns).reshape((TOKENS_B, TOP_K))
    route_logits = centred(seeds[9], (TOKENS_B, TOP_K), 1.5, 6.0, ((0, 8),), jnp.float32)
    gate_weight = centred(seeds[10], (EXPERTS, D, FF_E), D ** -0.5, 0.125, ((0, 8), (2, 4)))
    up_weight = centred(seeds[11], (EXPERTS, D, FF_E), D ** -0.5, 0.125, ((0, 8), (2, 4)))
    down_weight = centred(seeds[12], (EXPERTS, FF_E, D), FF_E ** -0.5, 0.109375, ((0, 8), (1, 4)))
    return dict(queries=queries, keys=keys, values=values, query_gain=query_gain, key_gain=key_gain, out_weight=out_weight, expert_input=expert_input, norm_gain=norm_gain, routes=routes, route_logits=route_logits, gate_weight=gate_weight, up_weight=up_weight, down_weight=down_weight)


def rope_tables(count, head_dim):
    pos = jnp.arange(count, dtype=jnp.int32)
    grid_row = (pos // GRID_W).astype(jnp.float32)
    grid_col = (pos % GRID_W).astype(jnp.float32)
    quarter = head_dim // 4
    inverse = 10000.0 ** (-jnp.arange(quarter, dtype=jnp.float32) / quarter)
    angles = jnp.concatenate([grid_row[:, None] * inverse, grid_col[:, None] * inverse], axis=-1)
    return (jnp.cos(angles), jnp.sin(angles))

def norm_rotate(x, gain, cosine, sine):
    count, number, head_dim = x.shape
    y = x * lax.rsqrt(lax.optimization_barrier(jnp.mean(x * x, axis=-1, keepdims=True)) + 1e-06) * gain
    pairs = y.reshape(count, number, head_dim // 2, 2)
    first, second = (pairs[..., 0], pairs[..., 1])
    cos_b = cosine[:, None, :]
    sin_b = sine[:, None, :]
    turned = jnp.stack([first * cos_b - second * sin_b, first * sin_b + second * cos_b], axis=-1)
    return turned.reshape(count, number, head_dim).astype(jnp.bfloat16)

def round_sum(lefts, rights):

    def add_part(total, pair):
        part = jnp.dot(pair[0], pair[1], preferred_element_type=jnp.float32).astype(jnp.bfloat16)
        part = lax.optimization_barrier(part)
        return (total + part.astype(jnp.float32), None)
    start = jnp.zeros((lefts.shape[1], rights.shape[2]), jnp.float32)
    total, _ = lax.scan(add_part, start, (lefts, rights))
    return total.astype(jnp.bfloat16)

def reference(queries, keys, values, query_gain, key_gain, out_weight, expert_input, norm_gain, routes, route_logits, gate_weight, up_weight, down_weight):
    cosine, sine = rope_tables(TOKENS_A, HEAD_DIM)
    q_rot = norm_rotate(queries.astype(jnp.float32).reshape(TOKENS_A, HEADS, HEAD_DIM), query_gain, cosine, sine)
    k_rot = norm_rotate(keys.astype(jnp.float32).reshape(TOKENS_A, KV_HEADS, HEAD_DIM), key_gain, cosine, sine)
    v_heads = values.reshape(TOKENS_A, KV_HEADS, HEAD_DIM)
    q_all = q_rot.transpose(1, 0, 2)
    k_all = jnp.repeat(k_rot, GROUP, axis=1).transpose(1, 0, 2)
    v_all = jnp.repeat(v_heads, GROUP, axis=1).transpose(1, 0, 2)
    block = math.gcd(TOKENS_A, 1024)
    scale = HEAD_DIM ** (-0.5)

    def one_head(args):
        q_head, k_head, v_head = args

        def one_block(q_block):
            scores = jnp.dot(q_block, k_head.T, preferred_element_type=jnp.float32) * scale
            peak = lax.optimization_barrier(jnp.max(scores, axis=-1, keepdims=True))
            weights = jnp.exp(scores - peak)
            total = lax.optimization_barrier(jnp.sum(weights, axis=-1, keepdims=True))
            summed = jnp.dot(weights.astype(jnp.bfloat16), v_head, preferred_element_type=jnp.float32)
            return (summed / total).astype(jnp.bfloat16)
        return lax.map(one_block, q_head.reshape(TOKENS_A // block, block, HEAD_DIM)).reshape(TOKENS_A, HEAD_DIM)
    attended = lax.map(one_head, (q_all, k_all, v_all)).transpose(1, 0, 2).reshape(TOKENS_A, HEADS * HEAD_DIM)
    width = HEADS * HEAD_DIM // N_TP
    mixed = round_sum(attended.reshape(TOKENS_A, N_TP, width).transpose(1, 0, 2), out_weight.reshape(N_TP, width, D))
    x = expert_input.astype(jnp.float32)
    normed = (x * lax.rsqrt(lax.optimization_barrier(jnp.mean(x * x, axis=-1, keepdims=True)) + 1e-06) * norm_gain).astype(jnp.bfloat16)
    route_weight = jax.nn.sigmoid(route_logits - route_logits[:, ::-1])
    ids = routes.reshape(N_EP, TOK_B * TOP_K)
    onehot = (ids[..., None] == jnp.arange(EXPERTS, dtype=jnp.int32)).astype(jnp.int32)
    before = jnp.cumsum(onehot, axis=1) - onehot
    slot = lax.optimization_barrier(jnp.sum(before * onehot, axis=-1))
    source = jnp.broadcast_to(jnp.arange(N_EP, dtype=jnp.int32)[:, None], ids.shape)
    token = source * TOK_B + jnp.arange(TOK_B * TOP_K, dtype=jnp.int32)[None, :] // TOP_K
    table = jnp.full((EXPERTS, N_EP, CAP), TOKENS_B, jnp.int32).at[ids, source, slot].set(token)
    padded = jnp.concatenate([normed, jnp.zeros((1, D), jnp.bfloat16)], axis=0)
    hidden_block = FF_E // N_TP

    def one_expert(args):
        rows_index, w_gate, w_up, w_down = args
        rows = padded[rows_index.reshape(-1)]
        gate = jnp.dot(rows, w_gate, preferred_element_type=jnp.float32)
        upper = jnp.dot(rows, w_up, preferred_element_type=jnp.float32)
        hidden = (jax.nn.silu(gate) * upper).astype(jnp.bfloat16)
        count = rows.shape[0]
        return round_sum(hidden.reshape(count, N_TP, hidden_block).transpose(1, 0, 2), w_down.reshape(N_TP, hidden_block, D))
    results = lax.map(one_expert, (table, gate_weight, up_weight, down_weight))
    flat_index = ((ids * N_EP + source) * CAP + slot).reshape(-1)
    picked = results.reshape(EXPERTS * N_EP * CAP, D)[flat_index].reshape(TOKENS_B, TOP_K, D)
    expert_out = lax.optimization_barrier(jnp.sum(route_weight[..., None] * picked.astype(jnp.float32), axis=1)).astype(jnp.bfloat16)
    return (mixed, expert_out)
```

```python
import functools
import jax
import jax.numpy as jnp
import numpy as np
from jax import lax
from jax.experimental import pallas as pl
from jax.experimental.pallas import tpu as pltpu
from jax.sharding import PartitionSpec as P

GRID_W = 64


def rope_tables(count, offset, head_dim):
    pos = offset + lax.iota(jnp.int32, count)
    grid_row = (pos // GRID_W).astype(jnp.float32)
    grid_col = (pos % GRID_W).astype(jnp.float32)
    quarter = head_dim // 4
    inverse = 10000.0 ** (-jnp.arange(quarter, dtype=jnp.float32) / quarter)
    angles = jnp.concatenate([grid_row[:, None] * inverse, grid_col[:, None] * inverse], axis=-1)
    return (jnp.cos(angles), jnp.sin(angles))


def norm_rotate(x, gain, cosine, sine):
    count, number, head_dim = x.shape
    y = x * lax.rsqrt(jnp.mean(x * x, axis=-1, keepdims=True) + 1e-06) * gain
    pairs = y.reshape(count, number, head_dim // 2, 2)
    first, second = (pairs[..., 0], pairs[..., 1])
    cos_b = cosine[:, None, :]
    sin_b = sine[:, None, :]
    turned = jnp.stack([first * cos_b - second * sin_b, first * sin_b + second * cos_b], axis=-1)
    return turned.reshape(count, number, head_dim).astype(jnp.bfloat16)


def key_block_size(length, shard_rows):
    if length <= 2048:
        return length
    shards = length // shard_rows
    most = max(1, 2048 // shard_rows)
    best = 1
    for count in range(1, most + 1):
        if shards % count == 0:
            best = count
    return best * shard_rows


def local(
    queries,
    keys,
    values,
    query_gain,
    key_gain,
    out_weight,
    expert_input,
    norm_gain,
    routes,
    route_logits,
    gate_weight,
    up_weight,
    down_weight,
):
    tokens_here = queries.shape[0]
    head_dim = query_gain.shape[0]
    heads_here = queries.shape[1] // head_dim
    kv_here = keys.shape[1] // head_dim
    group = heads_here // kv_here
    offset = lax.axis_index("ep") * tokens_here
    cosine, sine = rope_tables(tokens_here, offset, head_dim)
    q_rot = norm_rotate(
        queries.astype(jnp.float32).reshape(tokens_here, heads_here, head_dim),
        query_gain,
        cosine,
        sine,
    )
    k_rot = norm_rotate(
        keys.astype(jnp.float32).reshape(tokens_here, kv_here, head_dim), key_gain, cosine, sine
    ).reshape(tokens_here, kv_here * head_dim)
    q_grouped = q_rot.reshape(tokens_here, kv_here, group, head_dim).transpose(1, 2, 0, 3)
    q_grouped = q_grouped.reshape(kv_here, group * tokens_here, head_dim)
    query_rows = group * tokens_here
    scale = head_dim ** (-0.5)
    start_state = (
        jnp.full((kv_here, query_rows), -1e30, jnp.float32),
        jnp.zeros((kv_here, query_rows), jnp.float32),
        jnp.zeros((kv_here, query_rows, head_dim), jnp.float32),
    )
    key_piece = lax.all_gather(k_rot, "ep", axis=0, tiled=True)
    value_piece = lax.all_gather(values, "ep", axis=0, tiled=True)
    length = key_piece.shape[0]
    block = key_block_size(length, tokens_here)
    key_blocks = key_piece.reshape(length // block, block, kv_here, head_dim)
    value_blocks = value_piece.reshape(length // block, block, kv_here, head_dim)

    def step(state, blocks):
        running_max, running_total, running_sum = state
        key_block, value_block = blocks
        scores = (
            jnp.einsum("kqd,lkd->kql", q_grouped, key_block, preferred_element_type=jnp.float32)
            * scale
        )
        new_max = jnp.maximum(running_max, jnp.max(scores, axis=-1))
        factor = jnp.exp(running_max - new_max)
        weights = jnp.exp(scores - new_max[..., None])
        new_total = running_total * factor + jnp.sum(weights, axis=-1)
        new_sum = running_sum * factor[..., None] + jnp.einsum(
            "kql,lkd->kqd",
            weights.astype(jnp.bfloat16),
            value_block,
            preferred_element_type=jnp.float32,
        )
        return ((new_max, new_total, new_sum), None)

    result, _ = lax.scan(step, start_state, (key_blocks, value_blocks))
    final_max, final_total, final_sum = result
    attended = (final_sum / final_total[..., None]).astype(jnp.bfloat16)
    attended = attended.reshape(kv_here, group, tokens_here, head_dim).transpose(2, 0, 1, 3)
    attended = attended.reshape(tokens_here, heads_here * head_dim)
    summed = lax.psum_scatter(
        jnp.dot(attended, out_weight, preferred_element_type=jnp.float32).astype(jnp.bfloat16),
        "tp",
        scatter_dimension=0,
        tiled=True,
    ).astype(jnp.float32)
    mixed = summed.astype(jnp.bfloat16)
    expert_tokens_here, width = expert_input.shape
    n_ep = lax.axis_size("ep")
    top = routes.shape[1]
    capacity = expert_tokens_here * top // n_ep * 5 // 4
    x = expert_input.astype(jnp.float32)
    normed = (x * lax.rsqrt(jnp.mean(x * x, axis=-1, keepdims=True) + 1e-06) * norm_gain).astype(
        jnp.bfloat16
    )
    expert_ids = routes.reshape(-1)
    onehot = (expert_ids[:, None] == lax.iota(jnp.int32, n_ep)[None, :]).astype(jnp.int32)
    before = jnp.cumsum(onehot, axis=0) - onehot
    slot = jnp.sum(before * onehot, axis=1)
    target = expert_ids * capacity + slot
    owner_row = lax.iota(jnp.int32, expert_tokens_here * top) // top
    w_gate = gate_weight[0]
    w_up = up_weight[0]
    w_down = down_weight[0]
    columns = normed.shape[1]
    filled = jnp.zeros((n_ep * capacity, columns), jnp.bfloat16).at[target].set(normed[owner_row])
    arrived = lax.all_to_all(
        filled.reshape(n_ep, capacity, columns), "ep", split_axis=0, concat_axis=0, tiled=True
    )
    sources, slots, work_columns = arrived.shape
    flat = arrived.reshape(sources * slots, work_columns)
    gate = jnp.dot(flat, w_gate, preferred_element_type=jnp.float32)
    upper = jnp.dot(flat, w_up, preferred_element_type=jnp.float32)
    hidden = (jax.nn.silu(gate) * upper).astype(jnp.bfloat16)
    partial_out = jnp.dot(hidden, w_down, preferred_element_type=jnp.float32)
    summed = lax.psum_scatter(
        partial_out.reshape(sources, slots, width).astype(jnp.bfloat16),
        "tp",
        scatter_dimension=2,
        tiled=True,
    ).astype(jnp.float32)
    returned = lax.all_to_all(
        summed.astype(jnp.bfloat16), "ep", split_axis=0, concat_axis=0, tiled=True
    )
    picked = returned.reshape(n_ep * capacity, -1)[target].reshape(expert_tokens_here, top, -1)
    route_weight = jax.nn.sigmoid(route_logits - route_logits[:, ::-1])
    combined = jnp.sum(route_weight[..., None] * picked.astype(jnp.float32), axis=1)
    expert_out = combined.astype(jnp.bfloat16)
    return (mixed, expert_out)


MESH = pl.DeviceIdType.MESH


def rope_constants(length, head_dim):
    pos = np.arange(length)
    quarter = head_dim // 4
    inverse = (np.float32(10000.0) ** (-np.arange(quarter, dtype=np.float32) / np.float32(quarter))).astype(np.float32)
    grid_row = (pos // GRID_W).astype(np.float32)
    grid_col = (pos % GRID_W).astype(np.float32)
    angles = np.concatenate([grid_row[:, None] * inverse, grid_col[:, None] * inverse], axis=-1)
    cosine = np.repeat(np.cos(angles), 2, axis=-1).astype(np.float32)
    sine = np.repeat(np.sin(angles), 2, axis=-1).astype(np.float32)
    sine[:, 0::2] *= -1.0
    return np.stack([cosine, sine])


def fused(
    dims,
    q_hbm,
    k_hbm,
    v_hbm,
    qg_ref,
    kg_ref,
    wo_hbm,
    x_hbm,
    ng_ref,
    rt_ref,
    lg_ref,
    wg_hbm,
    wu_hbm,
    wd_hbm,
    rope_hbm,
    mixed_hbm,
    eout_hbm,
    mixed_ref,
    eout_ref,
    q_ref,
    k_ref,
    x_ref,
    amax,
    atot,
    asum,
    wo,
    wg,
    wu,
    wd,
    rope,
    disp,
    xq,
    gacc,
    uacc,
    hid,
    part,
    rdiag,
    rsx,
    rsy,
    back,
    ret,
    kv,
    qrot,
    att,
    mpart,
    mrecv,
    wsem,
    zs,
    zr,
    axs,
    axr,
    ays,
    ayr,
    afs,
    afr,
    kvs,
    kvu,
    kvd,
    kvr,
    rds,
    rdr,
    rxs,
    rxr,
    rys,
    ryr,
    bs,
    br,
    ms,
    mr,
):
    n_ep, cap, head_dim, kv_here, group = dims
    f32, bf16 = jnp.float32, jnp.bfloat16
    chips = n_ep // 2
    me = lax.axis_index("ep")
    t = lax.axis_index("tp")
    tx = t + 1 - 2 * (t % 2)
    ty = (t + 2) % 4
    td = 3 - t
    z = me // 2
    core = me % 2
    mate = 2 * z + 1 - core
    if chips == 4:
        inner = (z == 1) | (z == 2)
        across = (z + 2) % 4
        mirror = 3 - z
        near = [z + 1 - 2 * (z % 2), jnp.where(inner, mirror, across), jnp.where(inner, across, mirror)]
    else:
        near = [(z + k) % chips for k in range(1, chips)]
    order = [me, mate]
    for chip in near:
        order += [2 * chip + core, 2 * chip + 1 - core]
    far_first = order[::-1]
    tokens = x_ref.shape[0]
    slab = disp.shape[2]
    rows = n_ep * cap

    barrier = pltpu.get_barrier_semaphore()
    for d in range(1, n_ep):
        pl.semaphore_signal(barrier, inc=1, device_id={"ep": (me + d) % n_ep}, device_id_type=MESH)
    for peer in (tx, ty, td):
        pl.semaphore_signal(barrier, inc=1, device_id={"tp": peer}, device_id_type=MESH)

    x_load = pltpu.make_async_copy(x_hbm, x_ref, wsem.at[5])
    x_load.start()
    k_load = pltpu.make_async_copy(k_hbm, k_ref, wsem.at[6])
    k_load.start()
    rope_copy = pltpu.make_async_copy(
        rope_hbm.at[:, pl.ds(pl.multiple_of(me * tokens, tokens), tokens), :], rope, wsem.at[0]
    )
    rope_copy.start()
    v_load = pltpu.make_async_copy(v_hbm, kv.at[me, 1], wsem.at[7])
    v_load.start()
    q_load = pltpu.make_async_copy(q_hbm, q_ref, wsem.at[8])
    q_load.start()
    loads = [
        pltpu.make_async_copy(wg_hbm.at[0], wg, wsem.at[1]),
        pltpu.make_async_copy(wu_hbm.at[0], wu, wsem.at[2]),
        pltpu.make_async_copy(wd_hbm.at[0], wd, wsem.at[3]),
        pltpu.make_async_copy(wo_hbm, wo, wsem.at[4]),
    ]
    for load in loads:
        load.start()

    wide = (tokens, tokens)
    lane = lax.broadcasted_iota(jnp.int32, wide, 1)
    sub = lax.broadcasted_iota(jnp.int32, wide, 0)
    routed = (sub == rt_ref[0:1, :]) | (sub == rt_ref[1:2, :])
    named_t = jnp.where(routed, 1.0, 0.0)
    named = named_t.T
    ids = rt_ref[...].astype(f32)
    logits = lg_ref[...]
    stacked = jnp.where(
        sub == 0,
        ids[0:1, :],
        jnp.where(sub == 1, ids[1:2, :], jnp.where(sub == 2, logits[0:1, :], logits[1:2, :])),
    )
    columns = stacked.T
    r0 = columns[:, 0:1].astype(jnp.int32)
    r1 = columns[:, 1:2].astype(jnp.int32)
    upper = jnp.where(sub < lane, 1.0, 0.0).astype(bf16)
    lower = jnp.where(lane < sub, 1.0, 0.0).astype(bf16)
    rank_t = jnp.dot(named_t.astype(bf16), upper, preferred_element_type=f32)
    rank = jnp.dot(lower, named.astype(bf16), preferred_element_type=f32)
    slot_iota = lax.broadcasted_iota(jnp.int32, (cap, tokens), 0).astype(f32)
    picks = [
        jnp.where((slot_iota == rank_t[e : e + 1, :]) & (named_t[e : e + 1, :] > 0.5), 1.0, 0.0)
        for e in range(n_ep)
    ]
    pick = jnp.concatenate(picks, axis=0).astype(bf16)

    x_load.wait()
    x = x_ref[...].astype(f32)
    inv = lax.rsqrt(jnp.mean(x * x, axis=-1, keepdims=True) + 1e-06)
    cols = pl.ds(pl.multiple_of(t * slab, slab), slab)
    normed = (x_ref[:, cols].astype(f32) * inv * ng_ref[:, cols]).astype(bf16)
    sent = jnp.dot(pick, normed, preferred_element_type=f32)
    for e in range(n_ep):
        disp[e] = sent[e * cap : (e + 1) * cap].astype(bf16)
    xq[t, me] = disp[me]

    pl.semaphore_wait(barrier, n_ep - 1 + 3)

    def remote(a, b, s, r, **where):
        return pltpu.make_async_remote_copy(
            src_ref=a, dst_ref=b, send_sem=s, recv_sem=r, device_id=where, device_id_type=MESH
        )

    def z_copy(d):
        e = order[d]
        return remote(disp.at[e], xq.at[t, me], zs.at[e], zr.at[me], ep=e)

    for d in range(1, n_ep):
        z_copy(d).start()

    rope_copy.wait()
    cos = rope[0]
    sin = rope[1]
    even = lax.broadcasted_iota(jnp.int32, (tokens, head_dim), 1) % 2 == 0

    def turn(piece, gain):
        a = piece.astype(f32)
        y = a * lax.rsqrt(jnp.mean(a * a, axis=-1, keepdims=True) + 1e-06) * gain
        other = jnp.where(even, pltpu.roll(y, head_dim - 1, 1), pltpu.roll(y, 1, 1))
        return (y * cos + other * sin).astype(bf16)

    k_load.wait()
    for g in range(kv_here):
        at = slice(g * head_dim, (g + 1) * head_dim)
        kv[me, 0, :, at] = turn(k_ref[:, at], kg_ref[...])
    v_load.wait()
    q_load.wait()

    for h in range(kv_here * group):
        at = slice(h * head_dim, (h + 1) * head_dim)
        qrot[h] = turn(q_ref[:, at], qg_ref[...])

    def x_copy(s):
        return remote(xq.at[t, s], xq.at[t, s], axs.at[s], axr.at[s], tp=tx)

    def y_copy(s):
        return remote(xq.at[t, s], xq.at[t, s], ays.at[s], ayr.at[s], tp=ty)

    def wait_in(ref, sem):
        pltpu.make_async_remote_copy(
            src_ref=ref, dst_ref=ref, send_sem=zs.at[0], recv_sem=sem, device_id={"tp": tx}, device_id_type=MESH
        ).wait_recv()

    def on_copy(s, q, to):
        return remote(xq.at[q, s], xq.at[q, s], afs.at[s], afr.at[s], tp=to)

    for d in range(n_ep):
        s = order[d]
        if d > 0:
            wait_in(xq.at[t, s], zr.at[s])
        x_copy(s).start()
        y_copy(s).start()

    def kv_copy(block, to, sem):
        return remote(kv.at[block], kv.at[block], sem, kvr.at[block], ep=to)

    def lane_of(chip):
        return 2 * chip + core

    def own_kv(act):
        for k in (2, 1):
            if k < chips:

                @pl.when(z + k < chips)
                def _():
                    act(kv_copy(me, lane_of(z + k), kvu.at[k]))

                @pl.when(z >= k)
                def _():
                    act(kv_copy(me, lane_of(z - k), kvd.at[k]))

        act(kv_copy(me, mate, kvs.at[me]))

    def forward_kv(k, act, arrive):
        @pl.when((z >= k) & (z + 1 < chips))
        def _():
            block = lane_of(z - k)
            if arrive:
                wait_in(kv.at[block], kvr.at[block])
            act(kv_copy(block, mate, kvs.at[block]))
            act(kv_copy(block, lane_of(z + 1), kvu.at[k + 1]))

        @pl.when((z + k < chips) & (z >= 1))
        def _():
            block = lane_of(z + k)
            if arrive:
                wait_in(kv.at[block], kvr.at[block])
            act(kv_copy(block, mate, kvs.at[block]))
            act(kv_copy(block, lane_of(z - 1), kvd.at[k + 1]))

    def relay_kv(k, act, arrive):
        below, above = z >= k, z + k < chips
        if k == 2:
            below, above = below & (z + 1 >= chips), above & (z < 1)

        @pl.when(below)
        def _():
            block = lane_of(z - k)
            if arrive:
                wait_in(kv.at[block], kvr.at[block])
            act(kv_copy(block, mate, kvs.at[block]))

        @pl.when(above)
        def _():
            block = lane_of(z + k)
            if arrive:
                wait_in(kv.at[block], kvr.at[block])
            act(kv_copy(block, mate, kvs.at[block]))

    own_kv(lambda c: c.start())
    loads[0].wait()
    loads[1].wait()

    def gate_up(q, first):
        block = xq[q].astype(f32).reshape(rows, slab).astype(bf16)
        at = pl.ds(pl.multiple_of(q * slab, slab), slab)
        g = lax.dot_general(block, wg[:, at], (((1,), (1,)), ((), ())), preferred_element_type=f32)
        u = lax.dot_general(block, wu[:, at], (((1,), (1,)), ((), ())), preferred_element_type=f32)
        if first:
            gacc[...] = g
            uacc[...] = u
        else:
            gacc[...] += g
            uacc[...] += u

    gate_up(t, True)
    for i in range(n_ep):
        s = order[i]
        if i % 2 == 0:
            wait_in(xq.at[tx, s], axr.at[s])
            on_copy(s, tx, ty).start()
        else:
            wait_in(xq.at[ty, s], ayr.at[s])
            on_copy(s, ty, tx).start()
    for i in range(n_ep):
        s = order[i]
        if i % 2 == 0:
            wait_in(xq.at[ty, s], ayr.at[s])
        else:
            wait_in(xq.at[tx, s], axr.at[s])
    gate_up(tx, False)
    gate_up(ty, False)
    for i in range(n_ep):
        wait_in(xq.at[td, order[i]], afr.at[order[i]])
    gate_up(td, False)
    gate = gacc[...]
    hid[...] = (gate / (1.0 + jnp.exp(-gate)) * uacc[...]).astype(bf16)
    loads[2].wait()

    def down(q):
        at = pl.ds(pl.multiple_of(q * slab, slab), slab)
        out = jnp.dot(hid[...], wd[:, at], preferred_element_type=f32)
        for s in range(n_ep):
            part[q, s] = out[s * cap : (s + 1) * cap].astype(bf16)

    def far_copy(i):
        s = far_first[i]
        to = tx if i % 2 == 0 else ty
        return remote(part.at[td, s], rdiag.at[s], rds.at[s], rdr.at[s], tp=to)

    def rx_copy(s):
        return remote(part.at[tx, s], rsx.at[s], rxs.at[s], rxr.at[s], tp=tx)

    def ry_copy(s):
        return remote(part.at[ty, s], rsy.at[s], rys.at[s], ryr.at[s], tp=ty)

    down(td)
    for i in range(n_ep):
        far_copy(i).start()
    down(tx)
    for i in range(0, n_ep, 2):
        rx_copy(far_first[i]).start()
    down(ty)
    for i in range(1, n_ep, 2):
        ry_copy(far_first[i]).start()
    down(t)
    forward_kv(2, lambda c: c.start(), True)
    for i in range(n_ep):
        s = far_first[i]
        wait_in(rdiag.at[s], rdr.at[s])
        if i % 2 == 0:
            part[ty, s] = (part[ty, s].astype(f32) + rdiag[s].astype(f32)).astype(bf16)
            ry_copy(s).start()
        else:
            part[tx, s] = (part[tx, s].astype(f32) + rdiag[s].astype(f32)).astype(bf16)
            rx_copy(s).start()
    relay_kv(1, lambda c: c.start(), True)
    relay_kv(2, lambda c: c.start(), True)
    last = jnp.where(z * 2 < chips, chips - 1, 0)
    first_chip = jnp.where(z * 2 < chips, 0, 1)
    scale = head_dim ** (-0.5)

    def scores_of(g, start, count):
        at = slice(g * head_dim, (g + 1) * head_dim)
        blocks = pl.ds(2 * start, 2 * count)
        keys = kv[blocks, 0, :, at].reshape(2 * count * tokens, head_dim)
        vals = kv[blocks, 1, :, at].reshape(2 * count * tokens, head_dim)
        q2 = qrot[g * group : (g + 1) * group].reshape(group * tokens, head_dim)
        s = lax.dot_general(q2, keys, (((1,), (1,)), ((), ())), preferred_element_type=f32)
        return s * scale, vals

    for k in range(chips - 1):
        block = 2 * (first_chip + k) + 1 - core
        wait_in(kv.at[block], kvr.at[block])
    for g in range(kv_here):
        scores, vals = scores_of(g, first_chip, chips - 1)
        peak = jnp.max(scores, axis=-1, keepdims=True)
        p = jnp.exp(scores - peak)
        amax[g] = peak
        atot[g] = jnp.sum(p, axis=-1, keepdims=True)
        asum[g] = jnp.dot(p.astype(bf16), vals, preferred_element_type=f32)

    def back_copy(s):
        return remote(back.at[s], ret.at[me], bs.at[s], br.at[me], ep=s)

    for i in range(n_ep):
        s = far_first[i]
        wait_in(rsx.at[s], rxr.at[s])
        wait_in(rsy.at[s], ryr.at[s])
        out = (part[t, s].astype(f32) + rsx[s].astype(f32) + rsy[s].astype(f32)).astype(bf16)
        if i < n_ep - 1:
            back[s] = out
            back_copy(s).start()
        else:
            ret[s] = out

    relay_kv(3, lambda c: c.start(), True)
    last_block = 2 * last + 1 - core
    wait_in(kv.at[last_block], kvr.at[last_block])
    for g in range(kv_here):
        scores, vals = scores_of(g, last, 1)
        peak = jnp.maximum(amax[g], jnp.max(scores, axis=-1, keepdims=True))
        p = jnp.exp(scores - peak)
        factor = jnp.exp(amax[g] - peak)
        total = atot[g] * factor + jnp.sum(p, axis=-1, keepdims=True)
        out = (asum[g] * factor + jnp.dot(p.astype(bf16), vals, preferred_element_type=f32)) / total
        for r in range(group):
            h = g * group + r
            att[:, h * head_dim : (h + 1) * head_dim] = out[r * tokens : (r + 1) * tokens].astype(bf16)
    loads[3].wait()
    share = tokens // 4
    width = wo.shape[1]
    chunk = width // 4

    def m_copy(i, c):
        to = (td, tx, ty)[i]
        return remote(mpart.at[c, to], mrecv.at[c, i], ms.at[c, i], mr.at[c, i], tp=to)

    for c in range(4):
        out = jnp.dot(att[...], wo[:, c * chunk : (c + 1) * chunk], preferred_element_type=f32)
        for j in range(4):
            mpart[c, j] = out[j * share : (j + 1) * share].astype(bf16)
        for i in range(3):
            m_copy(i, c).start()

    rank_lane = lane
    total_lane = lax.broadcasted_iota(jnp.int32, (tokens, rows), 1)

    def chosen(r):
        slot = jnp.sum(jnp.where(rank_lane == r, rank, 0.0), axis=-1, keepdims=True)
        target = r * cap + slot.astype(jnp.int32)
        return jnp.where(total_lane == target, 1.0, 0.0).astype(bf16)

    c0 = chosen(r0)
    c1 = chosen(r1)
    l0 = columns[:, 2:3]
    l1 = columns[:, 3:4]
    w0 = jax.nn.sigmoid(l0 - l1)
    w1 = jax.nn.sigmoid(l1 - l0)
    for d in range(1, n_ep):
        e = (me + d) % n_ep
        wait_in(ret.at[e], br.at[e])
    results = ret[...].astype(f32).reshape(rows, slab).astype(bf16)
    first = jnp.dot(c0, results, preferred_element_type=f32)
    second = jnp.dot(c1, results, preferred_element_type=f32)
    eout_hbm[...] = (w0 * first + w1 * second).astype(bf16)

    def m_store(c):
        at = slice(c * chunk, (c + 1) * chunk)
        return pltpu.make_async_copy(mixed_ref.at[c], mixed_hbm.at[:, at], wsem.at[10 + c])

    for c in range(4):
        summed = mpart[c, t].astype(f32)
        for i in range(3):
            wait_in(mrecv.at[c, i], mr.at[c, i])
            summed = summed + mrecv[c, i].astype(f32)
        mixed_hbm[:, c * chunk : (c + 1) * chunk] = summed.astype(bf16)

    for d in range(1, n_ep):
        z_copy(d).wait_send()
    own_kv(lambda c: c.wait_send())
    forward_kv(2, lambda c: c.wait_send(), False)
    for k in range(1, chips):
        relay_kv(k, lambda c: c.wait_send(), False)
    for i in range(n_ep):
        s = order[i]
        x_copy(s).wait_send()
        y_copy(s).wait_send()
        on_copy(s, tx if i % 2 == 0 else ty, ty if i % 2 == 0 else tx).wait_send()
        far_copy(i).wait_send()
        rx_copy(s).wait_send()
        ry_copy(s).wait_send()
        if i > 0:
            back_copy(s).wait_send()

    for c in range(4):
        for i in range(3):
            m_copy(i, c).wait_send()


def hand_over(a_ref, b_ref, a_out, b_out, sem):
    one = pltpu.make_async_copy(a_ref, a_out, sem.at[0])
    two = pltpu.make_async_copy(b_ref, b_out, sem.at[1])
    one.start()
    two.start()
    one.wait()
    two.wait()


def kernel_form(
    queries,
    keys,
    values,
    query_gain,
    key_gain,
    out_weight,
    expert_input,
    norm_gain,
    routes,
    route_logits,
    gate_weight,
    up_weight,
    down_weight,
):
    bf16, f32 = jnp.bfloat16, jnp.float32
    n_ep = lax.axis_size("ep")
    tokens = queries.shape[0]
    head_dim = query_gain.shape[0]
    heads = queries.shape[1] // head_dim
    kv_here = keys.shape[1] // head_dim
    width = expert_input.shape[1]
    n_tp = lax.axis_size("tp")
    slab = width // n_tp
    cap = tokens * routes.shape[1] // n_ep * 5 // 4
    rows = n_ep * cap
    ff = gate_weight.shape[2]
    share = tokens // n_tp
    table = jnp.asarray(rope_constants(tokens * n_ep, head_dim))
    vmem = pl.BlockSpec(memory_space=pltpu.VMEM)
    hbm = pl.BlockSpec(memory_space=pl.ANY)
    piece = (n_ep, cap, slab)
    dma = pltpu.SemaphoreType.DMA
    dims = (n_ep, cap, head_dim, kv_here, heads // kv_here)
    outs = pl.pallas_call(
        functools.partial(fused, dims),
        name="fused",
        out_shape=(
            pltpu.VMEM((share, out_weight.shape[1]), bf16),
            pltpu.VMEM((tokens, slab), bf16),
        ),
        in_specs=[hbm, hbm, hbm, vmem, vmem, hbm, hbm, vmem, vmem, vmem, hbm, hbm, hbm, hbm],
        out_specs=(vmem, vmem),
        scratch_shapes=[
            pltpu.VMEM((4, share, out_weight.shape[1] // 4), bf16),
            pltpu.VMEM((tokens, slab), bf16),
            pltpu.VMEM(queries.shape, bf16),
            pltpu.VMEM(keys.shape, bf16),
            pltpu.VMEM(expert_input.shape, bf16),
            pltpu.VMEM((kv_here, heads // kv_here * tokens, 1), f32),
            pltpu.VMEM((kv_here, heads // kv_here * tokens, 1), f32),
            pltpu.VMEM((kv_here, heads // kv_here * tokens, head_dim), f32),
            pltpu.VMEM(out_weight.shape, bf16),
            pltpu.VMEM((ff, width), bf16),
            pltpu.VMEM((ff, width), bf16),
            pltpu.VMEM(down_weight.shape[1:], bf16),
            pltpu.VMEM((2, tokens, head_dim), f32),
            pltpu.VMEM(piece, bf16),
            pltpu.VMEM((n_tp,) + piece, bf16),
            pltpu.VMEM((rows, ff), f32),
            pltpu.VMEM((rows, ff), f32),
            pltpu.VMEM((rows, ff), bf16),
            pltpu.VMEM((n_tp,) + piece, bf16),
            pltpu.VMEM(piece, bf16),
            pltpu.VMEM(piece, bf16),
            pltpu.VMEM(piece, bf16),
            pltpu.VMEM(piece, bf16),
            pltpu.VMEM(piece, bf16),
            pltpu.VMEM((n_ep, 2, tokens, kv_here * head_dim), bf16),
            pltpu.VMEM((heads, tokens, head_dim), bf16),
            pltpu.VMEM((tokens, heads * head_dim), bf16),
            pltpu.VMEM((4, n_tp, share, out_weight.shape[1] // 4), bf16),
            pltpu.VMEM((4, 3, share, out_weight.shape[1] // 4), bf16),
            dma((14,)),
        ]
        + [dma((n_ep,))] * 20
        + [dma((4, 3))] * 2,
        compiler_params=pltpu.CompilerParams(
            collective_id=0, has_side_effects=True, vmem_limit_bytes=60 * 1024 * 1024
        ),
    )(
        queries,
        keys,
        values,
        query_gain.reshape(1, -1),
        key_gain.reshape(1, -1),
        out_weight,
        expert_input,
        norm_gain.reshape(1, -1),
        routes.T,
        route_logits.T,
        jnp.swapaxes(gate_weight, 1, 2),
        jnp.swapaxes(up_weight, 1, 2),
        down_weight,
        table,
    )
    vm = lambda o: pltpu.with_memory_space_constraint(o, pltpu.VMEM)
    return pl.pallas_call(
        hand_over,
        name="hand_over",
        out_shape=tuple(jax.ShapeDtypeStruct(o.shape, o.dtype) for o in outs),
        in_specs=[vmem, vmem],
        out_specs=(hbm, hbm),
        scratch_shapes=[dma((2,))],
    )(*(vm(o) for o in outs))


def dispatch_form(mesh, *args):
    queries, routes = args[0], args[8]
    tokens = queries.shape[0]
    n_ep, n_tp = mesh.shape["ep"], mesh.shape["tp"]
    cap = tokens * routes.shape[1] // n_ep * 5 // 4
    same = args[6].shape[0] == tokens and tokens % 128 == 0
    fits = n_tp == 4 and n_ep == 8 and cap % 8 == 0
    if same and fits and routes.shape[1] == 2 and tokens == 128:
        return kernel_form(*args)
    return local(*args)


def solution(mesh):
    placed = (
        P("ep", "tp"),
        P("ep", "tp"),
        P("ep", "tp"),
        P(),
        P(),
        P("tp", None),
        P("ep", None),
        P(),
        P("ep", None),
        P("ep", None),
        P("ep", None, "tp"),
        P("ep", None, "tp"),
        P("ep", "tp", None),
    )
    return jax.shard_map(
        functools.partial(dispatch_form, mesh),
        mesh=mesh,
        in_specs=placed,
        out_specs=(P(("ep", "tp"), None), P("ep", "tp")),
        check_vma=False,
    )
```

```python
import functools
import jax
import jax.numpy as jnp
import numpy as np
from jax import lax
from jax.experimental import pallas as pl
from jax.experimental.pallas import tpu as pltpu
from jax.sharding import PartitionSpec as P

GRID_W = 64


def rope_tables(count, offset, head_dim):
    pos = offset + lax.iota(jnp.int32, count)
    grid_row = (pos // GRID_W).astype(jnp.float32)
    grid_col = (pos % GRID_W).astype(jnp.float32)
    quarter = head_dim // 4
    inverse = 10000.0 ** (-jnp.arange(quarter, dtype=jnp.float32) / quarter)
    angles = jnp.concatenate([grid_row[:, None] * inverse, grid_col[:, None] * inverse], axis=-1)
    return (jnp.cos(angles), jnp.sin(angles))


def norm_rotate(x, gain, cosine, sine):
    count, number, head_dim = x.shape
    y = x * lax.rsqrt(jnp.mean(x * x, axis=-1, keepdims=True) + 1e-06) * gain
    pairs = y.reshape(count, number, head_dim // 2, 2)
    first, second = (pairs[..., 0], pairs[..., 1])
    cos_b = cosine[:, None, :]
    sin_b = sine[:, None, :]
    turned = jnp.stack([first * cos_b - second * sin_b, first * sin_b + second * cos_b], axis=-1)
    return turned.reshape(count, number, head_dim).astype(jnp.bfloat16)


def key_block_size(length, shard_rows):
    if length <= 2048:
        return length
    shards = length // shard_rows
    most = max(1, 2048 // shard_rows)
    best = 1
    for count in range(1, most + 1):
        if shards % count == 0:
            best = count
    return best * shard_rows


def local(
    queries,
    keys,
    values,
    query_gain,
    key_gain,
    out_weight,
    expert_input,
    norm_gain,
    routes,
    route_logits,
    gate_weight,
    up_weight,
    down_weight,
):
    tokens_here = queries.shape[0]
    head_dim = query_gain.shape[0]
    heads_here = queries.shape[1] // head_dim
    kv_here = keys.shape[1] // head_dim
    group = heads_here // kv_here
    offset = lax.axis_index("ep") * tokens_here
    cosine, sine = rope_tables(tokens_here, offset, head_dim)
    q_rot = norm_rotate(
        queries.astype(jnp.float32).reshape(tokens_here, heads_here, head_dim),
        query_gain,
        cosine,
        sine,
    )
    k_rot = norm_rotate(
        keys.astype(jnp.float32).reshape(tokens_here, kv_here, head_dim), key_gain, cosine, sine
    ).reshape(tokens_here, kv_here * head_dim)
    q_grouped = q_rot.reshape(tokens_here, kv_here, group, head_dim).transpose(1, 2, 0, 3)
    q_grouped = q_grouped.reshape(kv_here, group * tokens_here, head_dim)
    query_rows = group * tokens_here
    scale = head_dim ** (-0.5)
    start_state = (
        jnp.full((kv_here, query_rows), -1e30, jnp.float32),
        jnp.zeros((kv_here, query_rows), jnp.float32),
        jnp.zeros((kv_here, query_rows, head_dim), jnp.float32),
    )
    key_piece = lax.all_gather(k_rot, "ep", axis=0, tiled=True)
    value_piece = lax.all_gather(values, "ep", axis=0, tiled=True)
    length = key_piece.shape[0]
    block = key_block_size(length, tokens_here)
    key_blocks = key_piece.reshape(length // block, block, kv_here, head_dim)
    value_blocks = value_piece.reshape(length // block, block, kv_here, head_dim)

    def step(state, blocks):
        running_max, running_total, running_sum = state
        key_block, value_block = blocks
        scores = (
            jnp.einsum("kqd,lkd->kql", q_grouped, key_block, preferred_element_type=jnp.float32)
            * scale
        )
        new_max = jnp.maximum(running_max, jnp.max(scores, axis=-1))
        factor = jnp.exp(running_max - new_max)
        weights = jnp.exp(scores - new_max[..., None])
        new_total = running_total * factor + jnp.sum(weights, axis=-1)
        new_sum = running_sum * factor[..., None] + jnp.einsum(
            "kql,lkd->kqd",
            weights.astype(jnp.bfloat16),
            value_block,
            preferred_element_type=jnp.float32,
        )
        return ((new_max, new_total, new_sum), None)

    result, _ = lax.scan(step, start_state, (key_blocks, value_blocks))
    final_max, final_total, final_sum = result
    attended = (final_sum / final_total[..., None]).astype(jnp.bfloat16)
    attended = attended.reshape(kv_here, group, tokens_here, head_dim).transpose(2, 0, 1, 3)
    attended = attended.reshape(tokens_here, heads_here * head_dim)
    summed = lax.psum_scatter(
        jnp.dot(attended, out_weight, preferred_element_type=jnp.float32).astype(jnp.bfloat16),
        "tp",
        scatter_dimension=0,
        tiled=True,
    ).astype(jnp.float32)
    mixed = summed.astype(jnp.bfloat16)
    expert_tokens_here, width = expert_input.shape
    n_ep = lax.axis_size("ep")
    top = routes.shape[1]
    capacity = expert_tokens_here * top // n_ep * 5 // 4
    x = expert_input.astype(jnp.float32)
    normed = (x * lax.rsqrt(jnp.mean(x * x, axis=-1, keepdims=True) + 1e-06) * norm_gain).astype(
        jnp.bfloat16
    )
    expert_ids = routes.reshape(-1)
    onehot = (expert_ids[:, None] == lax.iota(jnp.int32, n_ep)[None, :]).astype(jnp.int32)
    before = jnp.cumsum(onehot, axis=0) - onehot
    slot = jnp.sum(before * onehot, axis=1)
    target = expert_ids * capacity + slot
    owner_row = lax.iota(jnp.int32, expert_tokens_here * top) // top
    w_gate = gate_weight[0]
    w_up = up_weight[0]
    w_down = down_weight[0]
    columns = normed.shape[1]
    filled = jnp.zeros((n_ep * capacity, columns), jnp.bfloat16).at[target].set(normed[owner_row])
    arrived = lax.all_to_all(
        filled.reshape(n_ep, capacity, columns), "ep", split_axis=0, concat_axis=0, tiled=True
    )
    sources, slots, work_columns = arrived.shape
    flat = arrived.reshape(sources * slots, work_columns)
    gate = jnp.dot(flat, w_gate, preferred_element_type=jnp.float32)
    upper = jnp.dot(flat, w_up, preferred_element_type=jnp.float32)
    hidden = (jax.nn.silu(gate) * upper).astype(jnp.bfloat16)
    partial_out = jnp.dot(hidden, w_down, preferred_element_type=jnp.float32)
    summed = lax.psum_scatter(
        partial_out.reshape(sources, slots, width).astype(jnp.bfloat16),
        "tp",
        scatter_dimension=2,
        tiled=True,
    ).astype(jnp.float32)
    returned = lax.all_to_all(
        summed.astype(jnp.bfloat16), "ep", split_axis=0, concat_axis=0, tiled=True
    )
    picked = returned.reshape(n_ep * capacity, -1)[target].reshape(expert_tokens_here, top, -1)
    route_weight = jax.nn.sigmoid(route_logits - route_logits[:, ::-1])
    combined = jnp.sum(route_weight[..., None] * picked.astype(jnp.float32), axis=1)
    expert_out = combined.astype(jnp.bfloat16)
    return (mixed, expert_out)


MESH = pl.DeviceIdType.MESH


def rope_constants(length, head_dim):
    pos = np.arange(length)
    quarter = head_dim // 4
    inverse = (np.float32(10000.0) ** (-np.arange(quarter, dtype=np.float32) / np.float32(quarter))).astype(np.float32)
    grid_row = (pos // GRID_W).astype(np.float32)
    grid_col = (pos % GRID_W).astype(np.float32)
    angles = np.concatenate([grid_row[:, None] * inverse, grid_col[:, None] * inverse], axis=-1)
    cosine = np.repeat(np.cos(angles), 2, axis=-1).astype(np.float32)
    sine = np.repeat(np.sin(angles), 2, axis=-1).astype(np.float32)
    sine[:, 0::2] *= -1.0
    return np.stack([cosine, sine])


def fused(
    dims,
    q_hbm,
    k_hbm,
    v_hbm,
    qg_hbm,
    kg_hbm,
    wo_hbm,
    x_hbm,
    ng_hbm,
    rt_hbm,
    lg_hbm,
    wg_hbm,
    wu_hbm,
    wd_hbm,
    rope_hbm,
    mixed_ref,
    eout_ref,
    q_ref,
    k_ref,
    x_ref,
    qg_ref,
    kg_ref,
    ng_ref,
    rt_ref,
    lg_ref,
    wo,
    wg,
    wu,
    wd,
    rope,
    disp,
    xq,
    gacc,
    uacc,
    hid,
    part,
    rdiag,
    rs,
    back,
    ret,
    kv,
    qrot,
    qship,
    att,
    aship,
    macc,
    mpart,
    mrecv,
    wsem,
    ssem,
    zr,
    axr,
    ayr,
    afr,
    kvr,
    kvm,
    qsr,
    atr,
    rdr,
    rsr,
    br,
    mr,
):
    n_ep, cap, head_dim, kv_here, group = dims
    f32, bf16 = jnp.float32, jnp.bfloat16
    chips = n_ep // 2
    me = lax.axis_index("ep")
    t = lax.axis_index("tp")
    tx = t + 1 - 2 * (t % 2)
    ty = (t + 2) % 4
    td = 3 - t
    z = me // 2
    core = me % 2
    mate = 2 * z + 1 - core
    inner = (z == 1) | (z == 2)
    partner = z + 1 - 2 * (z % 2)
    other = 3 - z
    far_end = 3 - partner
    near = [partner, jnp.where(z < 2, 2, 1), jnp.where(z < 2, 3, 0)]
    order = [me, mate]
    for chip in near:
        order += [2 * chip + core, 2 * chip + 1 - core]
    far_first = order[::-1]
    first_to = []
    for chip in (partner, jnp.where(inner, other, far_end), jnp.where(inner, far_end, other)):
        first_to += [2 * chip + core, 2 * chip + 1 - core]
    tokens = x_ref.shape[0]
    slab = disp.shape[2]
    rows = n_ep * cap
    half = n_ep // 2

    loads = [
        (x_hbm, x_ref),
        (rt_hbm, rt_ref),
        (ng_hbm, ng_ref),
        (k_hbm, k_ref),
        (rope_hbm.at[:, pl.ds(pl.multiple_of(me * tokens, tokens), tokens), :], rope),
        (kg_hbm, kg_ref),
    ]
    for g in range(kv_here):
        loads.append((v_hbm.at[:, g * head_dim : (g + 1) * head_dim], kv.at[g, core, z, 1]))
    loads += [
        (q_hbm, q_ref),
        (qg_hbm, qg_ref),
        (lg_hbm, lg_ref),
        (wg_hbm.at[0], wg),
        (wu_hbm.at[0], wu),
        (wd_hbm.at[0], wd),
        (wo_hbm, wo),
    ]
    loads = [pltpu.make_async_copy(a, b, wsem.at[i]) for i, (a, b) in enumerate(loads)]
    x_load, rt_load, ng_load, k_load, rope_load, kg_load = loads[:6]
    v_loads = loads[6 : 6 + kv_here]
    q_load, qg_load, lg_load, wg_load, wu_load, wd_load, wo_load = loads[6 + kv_here :]
    x_load.start()
    rt_load.start()

    barrier = pltpu.get_barrier_semaphore()
    for d in range(1, n_ep):
        pl.semaphore_signal(barrier, inc=1, device_id={"ep": (me + d) % n_ep}, device_id_type=MESH)
    for peer in (tx, ty, td):
        pl.semaphore_signal(barrier, inc=1, device_id={"tp": peer}, device_id_type=MESH)
    for load in loads[2:]:
        load.start()

    rt_load.wait()
    wide = (tokens, tokens)
    lane = lax.broadcasted_iota(jnp.int32, wide, 1)
    sub = lax.broadcasted_iota(jnp.int32, wide, 0)
    routed = (sub == rt_ref[0:1, :]) | (sub == rt_ref[1:2, :])
    named_t = jnp.where(routed, 1.0, 0.0)
    upper = jnp.where(sub < lane, 1.0, 0.0).astype(bf16)
    rank_t = jnp.dot(named_t.astype(bf16), upper, preferred_element_type=f32)
    slot_iota = lax.broadcasted_iota(jnp.int32, (cap, tokens), 0).astype(f32)
    picks = [
        jnp.where((slot_iota == rank_t[e : e + 1, :]) & (named_t[e : e + 1, :] > 0.5), 1.0, 0.0)
        for e in range(n_ep)
    ]
    pick = jnp.concatenate(picks, axis=0).astype(bf16)

    ng_load.wait()
    x_load.wait()
    x = x_ref[...].astype(f32)
    inv = lax.rsqrt(jnp.mean(x * x, axis=-1, keepdims=True) + 1e-06)
    cols = pl.ds(pl.multiple_of(t * slab, slab), slab)
    normed = (x_ref[:, cols].astype(f32) * inv * ng_ref[:, cols]).astype(bf16)
    sent = jnp.dot(pick, normed, preferred_element_type=f32)
    for e in range(n_ep):
        disp[e] = sent[e * cap : (e + 1) * cap].astype(bf16)
    xq[t, me] = disp[me]

    pl.semaphore_wait(barrier, n_ep - 1 + 3)

    def remote(a, b, s, r, **where):
        return pltpu.make_async_remote_copy(
            src_ref=a, dst_ref=b, send_sem=s, recv_sem=r, device_id=where, device_id_type=MESH
        )

    def wait_in(ref, sem):
        remote(ref, ref, ssem.at[0], sem, tp=tx).wait_recv()

    def wait_out(ref, sem):
        remote(ref, ref, sem, zr.at[0], tp=tx).wait_send()

    for e in [mate] + first_to:
        remote(disp.at[e], xq.at[t, me], ssem.at[0], zr.at[me], ep=e).start()

    def spread(i):
        s = order[i]
        even = i % 2 == 0
        at_x, at_y = (i // 2, half) if even else (half, i // 2)
        remote(xq.at[t, s], xq.at[t, s], ssem.at[1], axr.at[at_x], tp=tx).start()
        remote(xq.at[t, s], xq.at[t, s], ssem.at[1], ayr.at[at_y], tp=ty).start()

    def forward(i):
        s = order[i]
        if i % 2 == 0:
            wait_in(xq.at[tx, s], axr.at[i // 2])
            remote(xq.at[tx, s], xq.at[tx, s], ssem.at[1], afr.at[0], tp=ty).start()
        else:
            wait_in(xq.at[ty, s], ayr.at[i // 2])
            remote(xq.at[ty, s], xq.at[ty, s], ssem.at[1], afr.at[0], tp=tx).start()

    spread(0)

    rope_load.wait()
    cos = rope[0]
    sin = rope[1]
    even = lax.broadcasted_iota(jnp.int32, (tokens, head_dim), 1) % 2 == 0

    def turn(piece, gain):
        a = piece.astype(f32)
        y = a * lax.rsqrt(jnp.mean(a * a, axis=-1, keepdims=True) + 1e-06) * gain
        other = jnp.where(even, pltpu.roll(y, head_dim - 1, 1), pltpu.roll(y, 1, 1))
        return (y * cos + other * sin).astype(bf16)

    kg_load.wait()
    k_load.wait()
    for g in range(kv_here):
        kv[g, core, z, 0] = turn(k_ref[:, g * head_dim : (g + 1) * head_dim], kg_ref[...])

    def kv_send(g, chip, to):
        block = kv.at[g, core, chip]
        remote(block, block, ssem.at[3], kvr.at[g, chip], ep=2 * to + core).start()

    def kv_mate(g, chip):
        block = kv.at[g, core, chip]
        remote(block, block, ssem.at[2], kvm.at[g], ep=mate).start()

    for v_load in v_loads:
        v_load.wait()

    def receive(i):
        wait_in(xq.at[t, order[i]], zr.at[order[i]])
        spread(i)

    receive(1)
    q_load.wait()
    qg_load.wait()
    for h in range(kv_here * group):
        qrot[h] = turn(q_ref[:, h * head_dim : (h + 1) * head_dim], qg_ref[...])
    q_of = lambda g: qrot.at[pl.ds(g * group, group)]

    lag = 4
    for i in range(2, n_ep):
        receive(i)
        if i == 3:

            @pl.when(~inner)
            def _():
                for g in range(kv_here):
                    kv_send(g, z, partner)
                    remote(q_of(g), qship.at[g], ssem.at[3], qsr.at[g], ep=2 * partner + core).start()

        if i >= lag:
            forward(i - lag)

    @pl.when(inner)
    def _():
        for g in range(kv_here):
            kv_send(g, z, other)
            kv_mate(g, z)

    def relay_kv(source, on):
        @pl.when(inner)
        def _():
            for g in range(kv_here):
                block = kv.at[g, core, source]
                wait_in(block, kvr.at[g, source])
                if on:
                    kv_send(g, source, other)
                kv_mate(g, source)

    wg_load.wait()
    wu_load.wait()

    def gate_up(q, first):
        block = xq[q].astype(f32).reshape(rows, slab).astype(bf16)
        at = pl.ds(pl.multiple_of(q * slab, slab), slab)
        g = lax.dot_general(block, wg[:, at], (((1,), (1,)), ((), ())), preferred_element_type=f32)
        u = lax.dot_general(block, wu[:, at], (((1,), (1,)), ((), ())), preferred_element_type=f32)
        if first:
            gacc[...] = g
            uacc[...] = u
        else:
            gacc[...] += g
            uacc[...] += u

    gate_up(t, True)
    for i in range(n_ep - lag, n_ep):
        forward(i)
    wait_in(xq.at[tx, pl.ds(0, half)], axr.at[half])
    wait_in(xq.at[ty, pl.ds(0, half)], ayr.at[half])
    gate_up(tx, False)
    gate_up(ty, False)
    relay_kv(partner, True)
    wait_in(xq.at[td], afr.at[0])
    gate_up(td, False)
    gate = gacc[...]
    hid[...] = (gate / (1.0 + jnp.exp(-gate)) * uacc[...]).astype(bf16)
    wd_load.wait()

    def down(q):
        at = pl.ds(pl.multiple_of(q * slab, slab), slab)
        out = jnp.dot(hid[...], wd[:, at], preferred_element_type=f32)
        for s in range(n_ep):
            part[q, s] = out[s * cap : (s + 1) * cap].astype(bf16)

    def rx_copy(s):
        remote(part.at[tx, s], rs.at[0, s], ssem.at[6], rsr.at[s], tp=tx).start()

    def ry_copy(s):
        remote(part.at[ty, s], rs.at[1, s], ssem.at[6], rsr.at[s], tp=ty).start()

    down(td)
    for i in range(n_ep):
        s = far_first[i]
        remote(part.at[td, s], rdiag.at[s], ssem.at[6], rdr.at[s], tp=tx if i % 2 == 0 else ty).start()
    down(tx)
    for i in range(0, n_ep, 2):
        rx_copy(far_first[i])
    down(ty)
    for i in range(1, n_ep, 2):
        ry_copy(far_first[i])
    down(t)
    relay_kv(other, False)
    relay_kv(far_end, False)
    scale = head_dim ** (-0.5) * 1.4426950408889634
    share = tokens // 4
    width = wo.shape[1]
    chunk = width // 4

    def attend_one(g, q2):
        keys = kv[g, :, :, 0].reshape(n_ep * tokens, head_dim)
        vals = kv[g, :, :, 1].reshape(n_ep * tokens, head_dim)
        q2 = q2.reshape(group * tokens, head_dim)
        s = lax.dot_general(q2, keys, (((1,), (1,)), ((), ())), preferred_element_type=f32)
        peak = jnp.max(s, axis=-1, keepdims=True)
        p = jnp.exp2((s - peak) * scale)
        total = jnp.sum(p, axis=-1, keepdims=True)
        out = jnp.dot(p.astype(bf16), vals, preferred_element_type=f32) / total
        return jnp.concatenate([out[r * tokens : (r + 1) * tokens] for r in range(group)], axis=1).astype(bf16)

    def attend(g):
        @pl.when(inner)
        def _():
            wait_in(qship.at[g], qsr.at[g])
            wait_in(kv.at[g, 1 - core], kvm.at[g])
            aship[g] = attend_one(g, qship[g])
            remote(aship.at[g], att.at[g], ssem.at[3], atr.at[g], ep=2 * partner + core).start()
            att[g] = attend_one(g, qrot[g * group : (g + 1) * group])

    def meet(i):
        s = far_first[i]
        wait_in(rdiag.at[s], rdr.at[s])
        if i % 2 == 0:
            part[ty, s] = (part[ty, s].astype(f32) + rdiag[s].astype(f32)).astype(bf16)
            ry_copy(s)
        else:
            part[tx, s] = (part[tx, s].astype(f32) + rdiag[s].astype(f32)).astype(bf16)
            rx_copy(s)

    def finish(i):
        s = far_first[i]
        wait_in(rs.at[0, pl.ds(0, 2)], rsr.at[s])
        out = (part[t, s].astype(f32) + rs[0, s].astype(f32) + rs[1, s].astype(f32)).astype(bf16)
        if i < n_ep - 1:
            back[s] = out
            remote(back.at[s], ret.at[me], ssem.at[7], br.at[0], ep=s).start()
        else:
            ret[s] = out

    attend(0)
    attend(1)
    for i in range(half):
        meet(i)
    attend(2)
    for i in range(half, n_ep):
        meet(i)
    attend(3)
    for i in range(n_ep):
        finish(i)

    @pl.when(~inner)
    def _():
        for g in range(kv_here):
            wait_in(att.at[g], atr.at[g])

    wo_load.wait()
    heads = jnp.concatenate([att[g] for g in range(kv_here)], axis=1)
    for c in range(4):
        at = slice(c * chunk, (c + 1) * chunk)
        out = jnp.dot(heads, wo[:, at], preferred_element_type=f32)
        for j in range(4):
            mpart[c, j] = out[j * share : (j + 1) * share].astype(bf16)
        for i, to in enumerate((td, tx, ty)):
            remote(mpart.at[c, to], mrecv.at[c, i], ssem.at[5], mr.at[c], tp=to).start()

    lg_load.wait()
    ids = rt_ref[...].astype(f32)
    logits = lg_ref[...]
    stacked = jnp.where(
        sub == 0,
        ids[0:1, :],
        jnp.where(sub == 1, ids[1:2, :], jnp.where(sub == 2, logits[0:1, :], logits[1:2, :])),
    )
    columns = stacked.T
    r0 = columns[:, 0:1].astype(jnp.int32)
    r1 = columns[:, 1:2].astype(jnp.int32)
    lower = jnp.where(lane < sub, 1.0, 0.0).astype(bf16)
    rank = jnp.dot(lower, named_t.T.astype(bf16), preferred_element_type=f32)
    total_lane = lax.broadcasted_iota(jnp.int32, (tokens, rows), 1)

    def chosen(r):
        slot = jnp.sum(jnp.where(lane == r, rank, 0.0), axis=-1, keepdims=True)
        target = r * cap + slot.astype(jnp.int32)
        return jnp.where(total_lane == target, 1.0, 0.0).astype(bf16)

    c0 = chosen(r0)
    c1 = chosen(r1)
    l0 = columns[:, 2:3]
    l1 = columns[:, 3:4]
    w0 = jax.nn.sigmoid(l0 - l1)
    w1 = jax.nn.sigmoid(l1 - l0)
    wait_in(ret.at[pl.ds(0, n_ep - 1)], br.at[0])
    results = ret[...].astype(f32).reshape(rows, slab).astype(bf16)
    first = jnp.dot(c0, results, preferred_element_type=f32)
    second = jnp.dot(c1, results, preferred_element_type=f32)
    eout_ref[...] = (w0 * first + w1 * second).astype(bf16)
    for c in range(4):
        wait_in(mrecv.at[c], mr.at[c])
        summed = mpart[c, t].astype(f32)
        for i in range(3):
            summed = summed + mrecv[c, i].astype(f32)
        mixed_ref[:, c * chunk : (c + 1) * chunk] = summed.astype(bf16)

    wait_out(disp.at[pl.ds(0, n_ep - 1)], ssem.at[0])
    wait_out(xq.at[pl.ds(0, 3)], ssem.at[1])

    @pl.when(inner)
    def _():
        wait_out(kv.at[:, 0], ssem.at[2])
        wait_out(kv.at[pl.ds(0, 3), 0], ssem.at[3])

    @pl.when(~inner)
    def _():
        wait_out(kv.at[pl.ds(0, 2), 0], ssem.at[3])

    wait_out(mrecv, ssem.at[5])
    wait_out(part.at[pl.ds(0, 3)], ssem.at[6])
    wait_out(back.at[pl.ds(0, n_ep - 1)], ssem.at[7])


def hand_over(a_ref, b_ref, a_out, b_out, sem):
    one = pltpu.make_async_copy(a_ref, a_out, sem.at[0])
    two = pltpu.make_async_copy(b_ref, b_out, sem.at[1])
    one.start()
    two.start()
    one.wait()
    two.wait()


def kernel_form(
    queries,
    keys,
    values,
    query_gain,
    key_gain,
    out_weight,
    expert_input,
    norm_gain,
    routes,
    route_logits,
    gate_weight,
    up_weight,
    down_weight,
):
    bf16, f32 = jnp.bfloat16, jnp.float32
    n_ep = lax.axis_size("ep")
    tokens = queries.shape[0]
    head_dim = query_gain.shape[0]
    heads = queries.shape[1] // head_dim
    kv_here = keys.shape[1] // head_dim
    width = expert_input.shape[1]
    n_tp = lax.axis_size("tp")
    slab = width // n_tp
    cap = tokens * routes.shape[1] // n_ep * 5 // 4
    rows = n_ep * cap
    ff = gate_weight.shape[2]
    share = tokens // n_tp
    chunk = out_weight.shape[1] // 4
    table = jnp.asarray(rope_constants(tokens * n_ep, head_dim))
    vmem = pl.BlockSpec(memory_space=pltpu.VMEM)
    hbm = pl.BlockSpec(memory_space=pl.ANY)
    piece = (n_ep, cap, slab)
    dma = pltpu.SemaphoreType.DMA
    dims = (n_ep, cap, head_dim, kv_here, heads // kv_here)
    outs = pl.pallas_call(
        functools.partial(fused, dims),
        name="fused",
        out_shape=(
            pltpu.VMEM((share, out_weight.shape[1]), bf16),
            pltpu.VMEM((tokens, slab), bf16),
        ),
        in_specs=[hbm] * 14,
        out_specs=(vmem, vmem),
        scratch_shapes=[
            pltpu.VMEM(queries.shape, bf16),
            pltpu.VMEM(keys.shape, bf16),
            pltpu.VMEM(expert_input.shape, bf16),
            pltpu.VMEM((1, head_dim), f32),
            pltpu.VMEM((1, head_dim), f32),
            pltpu.VMEM((1, width), f32),
            pltpu.VMEM((2, tokens), jnp.int32),
            pltpu.VMEM((2, tokens), f32),
            pltpu.VMEM(out_weight.shape, bf16),
            pltpu.VMEM((ff, width), bf16),
            pltpu.VMEM((ff, width), bf16),
            pltpu.VMEM(down_weight.shape[1:], bf16),
            pltpu.VMEM((2, tokens, head_dim), f32),
            pltpu.VMEM(piece, bf16),
            pltpu.VMEM((n_tp,) + piece, bf16),
            pltpu.VMEM((rows, ff), f32),
            pltpu.VMEM((rows, ff), f32),
            pltpu.VMEM((rows, ff), bf16),
            pltpu.VMEM((n_tp,) + piece, bf16),
            pltpu.VMEM(piece, bf16),
            pltpu.VMEM((2,) + piece, bf16),
            pltpu.VMEM(piece, bf16),
            pltpu.VMEM(piece, bf16),
            pltpu.VMEM((kv_here, 2, n_ep // 2, 2, tokens, head_dim), bf16),
            pltpu.VMEM((heads, tokens, head_dim), bf16),
            pltpu.VMEM((kv_here, heads // kv_here, tokens, head_dim), bf16),
            pltpu.VMEM((kv_here, tokens, heads // kv_here * head_dim), bf16),
            pltpu.VMEM((kv_here, tokens, heads // kv_here * head_dim), bf16),
            pltpu.VMEM((tokens, width), f32),
            pltpu.VMEM((4, n_tp, share, chunk), bf16),
            pltpu.VMEM((4, 3, share, chunk), bf16),
            dma((13 + kv_here,)),
            dma((8,)),
            dma((n_ep,)),
            dma((n_ep // 2 + 1,)),
            dma((n_ep // 2 + 1,)),
            dma((1,)),
            dma((kv_here, n_ep // 2)),
            dma((kv_here,)),
            dma((kv_here,)),
            dma((kv_here,)),
            dma((n_ep,)),
            dma((n_ep,)),
            dma((1,)),
            dma((4,)),
        ],
        compiler_params=pltpu.CompilerParams(
            collective_id=0, has_side_effects=True, vmem_limit_bytes=60 * 1024 * 1024
        ),
    )(
        queries,
        keys,
        values,
        query_gain.reshape(1, -1),
        key_gain.reshape(1, -1),
        out_weight,
        expert_input,
        norm_gain.reshape(1, -1),
        routes.T,
        route_logits.T,
        jnp.swapaxes(gate_weight, 1, 2),
        jnp.swapaxes(up_weight, 1, 2),
        down_weight,
        table,
    )
    return pl.pallas_call(
        hand_over,
        name="hand_over",
        out_shape=tuple(jax.ShapeDtypeStruct(o.shape, o.dtype) for o in outs),
        in_specs=[vmem, vmem],
        out_specs=(hbm, hbm),
        scratch_shapes=[dma((2,))],
    )(*(pltpu.with_memory_space_constraint(o, pltpu.VMEM) for o in outs))


def dispatch_form(mesh, *args):
    queries, routes = args[0], args[8]
    tokens = queries.shape[0]
    n_ep, n_tp = mesh.shape["ep"], mesh.shape["tp"]
    cap = tokens * routes.shape[1] // n_ep * 5 // 4
    same = args[6].shape[0] == tokens and tokens % 128 == 0
    fits = n_tp == 4 and n_ep == 8 and cap % 8 == 0
    if same and fits and routes.shape[1] == 2 and tokens == 128:
        return kernel_form(*args)
    return local(*args)


def solution(mesh):
    placed = (
        P("ep", "tp"),
        P("ep", "tp"),
        P("ep", "tp"),
        P(),
        P(),
        P("tp", None),
        P("ep", None),
        P(),
        P("ep", None),
        P("ep", None),
        P("ep", None, "tp"),
        P("ep", None, "tp"),
        P("ep", "tp", None),
    )
    return jax.shard_map(
        functools.partial(dispatch_form, mesh),
        mesh=mesh,
        in_specs=placed,
        out_specs=(P(("ep", "tp"), None), P("ep", "tp")),
        check_vma=False,
    )
```

```python
import functools
import jax
import jax.numpy as jnp
import numpy as np
from jax import lax
from jax.experimental import pallas as pl
from jax.experimental.pallas import tpu as pltpu
from jax.sharding import PartitionSpec as P

GRID_W = 64


def rope_tables(count, offset, head_dim):
    pos = offset + lax.iota(jnp.int32, count)
    grid_row = (pos // GRID_W).astype(jnp.float32)
    grid_col = (pos % GRID_W).astype(jnp.float32)
    quarter = head_dim // 4
    inverse = 10000.0 ** (-jnp.arange(quarter, dtype=jnp.float32) / quarter)
    angles = jnp.concatenate([grid_row[:, None] * inverse, grid_col[:, None] * inverse], axis=-1)
    return (jnp.cos(angles), jnp.sin(angles))


def norm_rotate(x, gain, cosine, sine):
    count, number, head_dim = x.shape
    y = x * lax.rsqrt(jnp.mean(x * x, axis=-1, keepdims=True) + 1e-06) * gain
    pairs = y.reshape(count, number, head_dim // 2, 2)
    first, second = (pairs[..., 0], pairs[..., 1])
    cos_b = cosine[:, None, :]
    sin_b = sine[:, None, :]
    turned = jnp.stack([first * cos_b - second * sin_b, first * sin_b + second * cos_b], axis=-1)
    return turned.reshape(count, number, head_dim).astype(jnp.bfloat16)


def key_block_size(length, shard_rows):
    if length <= 2048:
        return length
    shards = length // shard_rows
    most = max(1, 2048 // shard_rows)
    best = 1
    for count in range(1, most + 1):
        if shards % count == 0:
            best = count
    return best * shard_rows


def local(
    queries,
    keys,
    values,
    query_gain,
    key_gain,
    out_weight,
    expert_input,
    norm_gain,
    routes,
    route_logits,
    gate_weight,
    up_weight,
    down_weight,
):
    tokens_here = queries.shape[0]
    head_dim = query_gain.shape[0]
    heads_here = queries.shape[1] // head_dim
    kv_here = keys.shape[1] // head_dim
    group = heads_here // kv_here
    offset = lax.axis_index("ep") * tokens_here
    cosine, sine = rope_tables(tokens_here, offset, head_dim)
    q_rot = norm_rotate(
        queries.astype(jnp.float32).reshape(tokens_here, heads_here, head_dim),
        query_gain,
        cosine,
        sine,
    )
    k_rot = norm_rotate(
        keys.astype(jnp.float32).reshape(tokens_here, kv_here, head_dim), key_gain, cosine, sine
    ).reshape(tokens_here, kv_here * head_dim)
    q_grouped = q_rot.reshape(tokens_here, kv_here, group, head_dim).transpose(1, 2, 0, 3)
    q_grouped = q_grouped.reshape(kv_here, group * tokens_here, head_dim)
    query_rows = group * tokens_here
    scale = head_dim ** (-0.5)
    start_state = (
        jnp.full((kv_here, query_rows), -1e30, jnp.float32),
        jnp.zeros((kv_here, query_rows), jnp.float32),
        jnp.zeros((kv_here, query_rows, head_dim), jnp.float32),
    )
    key_piece = lax.all_gather(k_rot, "ep", axis=0, tiled=True)
    value_piece = lax.all_gather(values, "ep", axis=0, tiled=True)
    length = key_piece.shape[0]
    block = key_block_size(length, tokens_here)
    key_blocks = key_piece.reshape(length // block, block, kv_here, head_dim)
    value_blocks = value_piece.reshape(length // block, block, kv_here, head_dim)

    def step(state, blocks):
        running_max, running_total, running_sum = state
        key_block, value_block = blocks
        scores = (
            jnp.einsum("kqd,lkd->kql", q_grouped, key_block, preferred_element_type=jnp.float32)
            * scale
        )
        new_max = jnp.maximum(running_max, jnp.max(scores, axis=-1))
        factor = jnp.exp(running_max - new_max)
        weights = jnp.exp(scores - new_max[..., None])
        new_total = running_total * factor + jnp.sum(weights, axis=-1)
        new_sum = running_sum * factor[..., None] + jnp.einsum(
            "kql,lkd->kqd",
            weights.astype(jnp.bfloat16),
            value_block,
            preferred_element_type=jnp.float32,
        )
        return ((new_max, new_total, new_sum), None)

    result, _ = lax.scan(step, start_state, (key_blocks, value_blocks))
    final_max, final_total, final_sum = result
    attended = (final_sum / final_total[..., None]).astype(jnp.bfloat16)
    attended = attended.reshape(kv_here, group, tokens_here, head_dim).transpose(2, 0, 1, 3)
    attended = attended.reshape(tokens_here, heads_here * head_dim)
    summed = lax.psum_scatter(
        jnp.dot(attended, out_weight, preferred_element_type=jnp.float32).astype(jnp.bfloat16),
        "tp",
        scatter_dimension=0,
        tiled=True,
    ).astype(jnp.float32)
    mixed = summed.astype(jnp.bfloat16)
    expert_tokens_here, width = expert_input.shape
    n_ep = lax.axis_size("ep")
    top = routes.shape[1]
    capacity = expert_tokens_here * top // n_ep * 5 // 4
    x = expert_input.astype(jnp.float32)
    normed = (x * lax.rsqrt(jnp.mean(x * x, axis=-1, keepdims=True) + 1e-06) * norm_gain).astype(
        jnp.bfloat16
    )
    expert_ids = routes.reshape(-1)
    onehot = (expert_ids[:, None] == lax.iota(jnp.int32, n_ep)[None, :]).astype(jnp.int32)
    before = jnp.cumsum(onehot, axis=0) - onehot
    slot = jnp.sum(before * onehot, axis=1)
    target = expert_ids * capacity + slot
    owner_row = lax.iota(jnp.int32, expert_tokens_here * top) // top
    w_gate = gate_weight[0]
    w_up = up_weight[0]
    w_down = down_weight[0]
    columns = normed.shape[1]
    filled = jnp.zeros((n_ep * capacity, columns), jnp.bfloat16).at[target].set(normed[owner_row])
    arrived = lax.all_to_all(
        filled.reshape(n_ep, capacity, columns), "ep", split_axis=0, concat_axis=0, tiled=True
    )
    sources, slots, work_columns = arrived.shape
    flat = arrived.reshape(sources * slots, work_columns)
    gate = jnp.dot(flat, w_gate, preferred_element_type=jnp.float32)
    upper = jnp.dot(flat, w_up, preferred_element_type=jnp.float32)
    hidden = (jax.nn.silu(gate) * upper).astype(jnp.bfloat16)
    partial_out = jnp.dot(hidden, w_down, preferred_element_type=jnp.float32)
    summed = lax.psum_scatter(
        partial_out.reshape(sources, slots, width).astype(jnp.bfloat16),
        "tp",
        scatter_dimension=2,
        tiled=True,
    ).astype(jnp.float32)
    returned = lax.all_to_all(
        summed.astype(jnp.bfloat16), "ep", split_axis=0, concat_axis=0, tiled=True
    )
    picked = returned.reshape(n_ep * capacity, -1)[target].reshape(expert_tokens_here, top, -1)
    route_weight = jax.nn.sigmoid(route_logits - route_logits[:, ::-1])
    combined = jnp.sum(route_weight[..., None] * picked.astype(jnp.float32), axis=1)
    expert_out = combined.astype(jnp.bfloat16)
    return (mixed, expert_out)


MESH = pl.DeviceIdType.MESH


def rope_constants(length, head_dim):
    pos = np.arange(length)
    quarter = head_dim // 4
    inverse = (np.float32(10000.0) ** (-np.arange(quarter, dtype=np.float32) / np.float32(quarter))).astype(np.float32)
    grid_row = (pos // GRID_W).astype(np.float32)
    grid_col = (pos % GRID_W).astype(np.float32)
    angles = np.concatenate([grid_row[:, None] * inverse, grid_col[:, None] * inverse], axis=-1)
    cosine = np.repeat(np.cos(angles), 2, axis=-1).astype(np.float32)
    sine = np.repeat(np.sin(angles), 2, axis=-1).astype(np.float32)
    sine[:, 0::2] *= -1.0
    return np.stack([cosine, sine])


def fused(
    dims,
    q_hbm,
    k_hbm,
    v_hbm,
    qg_hbm,
    kg_hbm,
    wo_hbm,
    x_hbm,
    ng_hbm,
    rt_hbm,
    lg_hbm,
    wg_hbm,
    wu_hbm,
    wd_hbm,
    rope_hbm,
    mixed_ref,
    eout_ref,
    q_ref,
    k_ref,
    x_ref,
    qg_ref,
    kg_ref,
    ng_ref,
    rt_ref,
    lg_ref,
    wo,
    wg,
    wu,
    wd,
    rope,
    disp,
    xq,
    gacc,
    uacc,
    hid,
    part,
    rdiag,
    rs,
    back,
    ret,
    kv,
    qrot,
    qship,
    att,
    aship,
    macc,
    mpart,
    mrecv,
    wsem,
    ssem,
    zr,
    axr,
    ayr,
    afr,
    kvr,
    kvm,
    qsr,
    atr,
    rdr,
    rsr,
    br,
    mr,
):
    n_ep, cap, head_dim, kv_here, group = dims
    f32, bf16 = jnp.float32, jnp.bfloat16
    chips = n_ep // 2
    me = lax.axis_index("ep")
    t = lax.axis_index("tp")
    tx = t + 1 - 2 * (t % 2)
    ty = (t + 2) % 4
    td = 3 - t
    z = me // 2
    core = me % 2
    mate = 2 * z + 1 - core
    inner = (z == 1) | (z == 2)
    partner = z + 1 - 2 * (z % 2)
    other = 3 - z
    far_end = 3 - partner
    near = [partner, jnp.where(z < 2, 2, 1), jnp.where(z < 2, 3, 0)]
    order = [me, mate]
    for chip in near:
        order += [2 * chip + core, 2 * chip + 1 - core]
    far_first = order[::-1]
    first_to = []
    for chip in (partner, other, far_end):
        first_to += [2 * chip + core, 2 * chip + 1 - core]
    tokens = x_ref.shape[0]
    slab = disp.shape[2]
    rows = n_ep * cap
    half = n_ep // 2

    loads = [
        (x_hbm, x_ref),
        (rt_hbm, rt_ref),
        (ng_hbm, ng_ref),
        (k_hbm, k_ref),
        (rope_hbm.at[:, pl.ds(pl.multiple_of(me * tokens, tokens), tokens), :], rope),
        (kg_hbm, kg_ref),
    ]
    for g in range(kv_here):
        loads.append((v_hbm.at[:, g * head_dim : (g + 1) * head_dim], kv.at[g, core, z, 1]))
    loads += [
        (q_hbm, q_ref),
        (qg_hbm, qg_ref),
        (lg_hbm, lg_ref),
        (wg_hbm.at[0], wg),
        (wu_hbm.at[0], wu),
        (wd_hbm.at[0], wd),
        (wo_hbm, wo),
    ]
    loads = [pltpu.make_async_copy(a, b, wsem.at[i]) for i, (a, b) in enumerate(loads)]
    x_load, rt_load, ng_load, k_load, rope_load, kg_load = loads[:6]
    v_loads = loads[6 : 6 + kv_here]
    q_load, qg_load, lg_load, wg_load, wu_load, wd_load, wo_load = loads[6 + kv_here :]
    x_load.start()
    rt_load.start()

    barrier = pltpu.get_barrier_semaphore()
    for d in range(1, n_ep):
        pl.semaphore_signal(barrier, inc=1, device_id={"ep": (me + d) % n_ep}, device_id_type=MESH)
    for peer in (tx, ty, td):
        pl.semaphore_signal(barrier, inc=1, device_id={"tp": peer}, device_id_type=MESH)
    for load in loads[2:]:
        load.start()

    rt_load.wait()
    wide = (tokens, tokens)
    lane = lax.broadcasted_iota(jnp.int32, wide, 1)
    sub = lax.broadcasted_iota(jnp.int32, wide, 0)
    routed = (sub == rt_ref[0:1, :]) | (sub == rt_ref[1:2, :])
    named_t = jnp.where(routed, 1.0, 0.0)
    upper = jnp.where(sub < lane, 1.0, 0.0).astype(bf16)
    rank_t = jnp.dot(named_t.astype(bf16), upper, preferred_element_type=f32)
    slot_iota = lax.broadcasted_iota(jnp.int32, (cap, tokens), 0).astype(f32)
    picks = [
        jnp.where((slot_iota == rank_t[e : e + 1, :]) & (named_t[e : e + 1, :] > 0.5), 1.0, 0.0)
        for e in range(n_ep)
    ]
    pick = jnp.concatenate(picks, axis=0).astype(bf16)

    ng_load.wait()
    x_load.wait()
    x = x_ref[...].astype(f32)
    inv = lax.rsqrt(jnp.mean(x * x, axis=-1, keepdims=True) + 1e-06)
    cols = pl.ds(pl.multiple_of(t * slab, slab), slab)
    normed = (x_ref[:, cols].astype(f32) * inv * ng_ref[:, cols]).astype(bf16)
    sent = jnp.dot(pick, normed, preferred_element_type=f32)
    for e in range(n_ep):
        disp[e] = sent[e * cap : (e + 1) * cap].astype(bf16)
    xq[t, me] = disp[me]

    pl.semaphore_wait(barrier, n_ep - 1 + 3)

    def remote(a, b, s, r, **where):
        return pltpu.make_async_remote_copy(
            src_ref=a, dst_ref=b, send_sem=s, recv_sem=r, device_id=where, device_id_type=MESH
        )

    def wait_in(ref, sem):
        remote(ref, ref, ssem.at[0], sem, tp=tx).wait_recv()

    def wait_out(ref, sem):
        remote(ref, ref, sem, zr.at[0], tp=tx).wait_send()

    for e in [mate] + first_to:
        remote(disp.at[e], xq.at[t, me], ssem.at[0], zr.at[me], ep=e).start()

    def spread(i):
        s = order[i]
        even = i % 2 == 0
        at_x, at_y = (i // 2, half) if even else (half, i // 2)
        remote(xq.at[t, s], xq.at[t, s], ssem.at[1], axr.at[at_x], tp=tx).start()
        remote(xq.at[t, s], xq.at[t, s], ssem.at[1], ayr.at[at_y], tp=ty).start()

    def forward(i):
        s = order[i]
        if i % 2 == 0:
            wait_in(xq.at[tx, s], axr.at[i // 2])
            remote(xq.at[tx, s], xq.at[tx, s], ssem.at[1], afr.at[0], tp=ty).start()
        else:
            wait_in(xq.at[ty, s], ayr.at[i // 2])
            remote(xq.at[ty, s], xq.at[ty, s], ssem.at[1], afr.at[0], tp=tx).start()

    spread(0)

    rope_load.wait()
    cos = rope[0]
    sin = rope[1]
    even = lax.broadcasted_iota(jnp.int32, (tokens, head_dim), 1) % 2 == 0

    def turn(piece, gain):
        a = piece.astype(f32)
        y = a * lax.rsqrt(jnp.mean(a * a, axis=-1, keepdims=True) + 1e-06) * gain
        other = jnp.where(even, pltpu.roll(y, head_dim - 1, 1), pltpu.roll(y, 1, 1))
        return (y * cos + other * sin).astype(bf16)

    kg_load.wait()
    k_load.wait()
    for g in range(kv_here):
        kv[g, core, z, 0] = turn(k_ref[:, g * head_dim : (g + 1) * head_dim], kg_ref[...])

    def kv_send(g, chip, to):
        block = kv.at[g, core, chip]
        remote(block, block, ssem.at[3], kvr.at[g, chip], ep=2 * to + core).start()

    def kv_mate(g, chip):
        block = kv.at[g, core, chip]
        remote(block, block, ssem.at[2], kvm.at[g], ep=mate).start()

    for v_load in v_loads:
        v_load.wait()

    def receive(i):
        wait_in(xq.at[t, order[i]], zr.at[order[i]])
        spread(i)

    receive(1)
    q_load.wait()
    qg_load.wait()
    for h in range(kv_here * group):
        qrot[h] = turn(q_ref[:, h * head_dim : (h + 1) * head_dim], qg_ref[...])
    q_of = lambda g: qrot.at[pl.ds(g * group, group)]

    receive(2)
    receive(3)

    @pl.when(~inner)
    def _():
        for g in range(kv_here):
            kv_send(g, z, partner)
        for g in range(kv_here):
            remote(q_of(g), qship.at[g], ssem.at[3], qsr.at[g], ep=2 * partner + core).start()

    forward(0)
    forward(1)

    @pl.when(~inner)
    def _():
        forward(2)
        forward(3)

    receive(4)
    receive(5)

    @pl.when(inner)
    def _():
        forward(2)
        forward(3)

    receive(6)
    receive(7)

    @pl.when(inner)
    def _():
        for g in range(kv_here):
            kv_send(g, z, other)
            kv_mate(g, z)

    def relay_kv(g, source, on):
        block = kv.at[g, core, source]
        wait_in(block, kvr.at[g, source])
        if on:
            kv_send(g, source, other)
        kv_mate(g, source)

    def relay_all(heads, source, on):
        @pl.when(inner)
        def _():
            for g in heads:
                relay_kv(g, source, on)

    wg_load.wait()
    wu_load.wait()

    def gate_up(q, first):
        block = xq[q].astype(f32).reshape(rows, slab).astype(bf16)
        at = pl.ds(pl.multiple_of(q * slab, slab), slab)
        g = lax.dot_general(block, wg[:, at], (((1,), (1,)), ((), ())), preferred_element_type=f32)
        u = lax.dot_general(block, wu[:, at], (((1,), (1,)), ((), ())), preferred_element_type=f32)
        if first:
            gacc[...] = g
            uacc[...] = u
        else:
            gacc[...] += g
            uacc[...] += u

    gate_up(t, True)
    forward(4)
    forward(5)
    relay_all((0, 1), partner, True)
    forward(6)
    forward(7)
    wait_in(xq.at[tx, pl.ds(0, half)], axr.at[half])
    wait_in(xq.at[ty, pl.ds(0, half)], ayr.at[half])
    gate_up(tx, False)
    gate_up(ty, False)
    relay_all((2, 3), partner, True)
    wait_in(xq.at[td], afr.at[0])
    gate_up(td, False)
    gate = gacc[...]
    hid[...] = (gate / (1.0 + jnp.exp(-gate)) * uacc[...]).astype(bf16)
    wd_load.wait()

    def down(q):
        at = pl.ds(pl.multiple_of(q * slab, slab), slab)
        out = jnp.dot(hid[...], wd[:, at], preferred_element_type=f32)
        for s in range(n_ep):
            part[q, s] = out[s * cap : (s + 1) * cap].astype(bf16)

    def rx_copy(s):
        remote(part.at[tx, s], rs.at[0, s], ssem.at[6], rsr.at[s], tp=tx).start()

    def ry_copy(s):
        remote(part.at[ty, s], rs.at[1, s], ssem.at[6], rsr.at[s], tp=ty).start()

    down(td)
    for i in range(n_ep):
        s = far_first[i]
        remote(part.at[td, s], rdiag.at[s], ssem.at[6], rdr.at[s], tp=tx if i % 2 == 0 else ty).start()
    down(tx)
    for i in range(0, n_ep, 2):
        rx_copy(far_first[i])
    down(ty)
    for i in range(1, n_ep, 2):
        ry_copy(far_first[i])
    down(t)
    relay_all(range(kv_here), other, False)
    scale = head_dim ** (-0.5) * 1.4426950408889634
    share = tokens // 4
    width = wo.shape[1]
    chunk = width // 4

    def attend_one(g, q2):
        keys = kv[g, :, :, 0].reshape(n_ep * tokens, head_dim)
        vals = kv[g, :, :, 1].reshape(n_ep * tokens, head_dim)
        q2 = q2.reshape(group * tokens, head_dim)
        s = lax.dot_general(q2, keys, (((1,), (1,)), ((), ())), preferred_element_type=f32)
        peak = jnp.max(s, axis=-1, keepdims=True)
        p = jnp.exp2((s - peak) * scale)
        total = jnp.sum(p, axis=-1, keepdims=True)
        out = jnp.dot(p.astype(bf16), vals, preferred_element_type=f32) / total
        return jnp.concatenate([out[r * tokens : (r + 1) * tokens] for r in range(group)], axis=1).astype(bf16)

    def attend_ship(g):
        relay_kv(g, far_end, False)
        wait_in(qship.at[g], qsr.at[g])
        wait_in(kv.at[g, 1 - core], kvm.at[g])
        aship[g] = attend_one(g, qship[g])
        remote(aship.at[g], att.at[g], ssem.at[3], atr.at[g], ep=2 * partner + core).start()

    def meet(i):
        s = far_first[i]
        wait_in(rdiag.at[s], rdr.at[s])
        if i % 2 == 0:
            part[ty, s] = (part[ty, s].astype(f32) + rdiag[s].astype(f32)).astype(bf16)
            ry_copy(s)
        else:
            part[tx, s] = (part[tx, s].astype(f32) + rdiag[s].astype(f32)).astype(bf16)
            rx_copy(s)

    def finish(i):
        s = far_first[i]
        wait_in(rs.at[0, pl.ds(0, 2)], rsr.at[s])
        out = (part[t, s].astype(f32) + rs[0, s].astype(f32) + rs[1, s].astype(f32)).astype(bf16)
        if i < n_ep - 1:
            back[s] = out
            remote(back.at[s], ret.at[me], ssem.at[7], br.at[0], ep=s).start()
        else:
            ret[s] = out


    @pl.when(inner)
    def _():
        for g in range(kv_here):
            attend_ship(g)

    for i in range(n_ep):
        meet(i)

    @pl.when(inner)
    def _():
        for g in range(kv_here):
            att[g] = attend_one(g, qrot[g * group : (g + 1) * group])

    @pl.when(~inner)
    def _():
        for g in range(kv_here):
            wait_in(att.at[g], atr.at[g])

    wo_load.wait()
    heads = jnp.concatenate([att[g] for g in range(kv_here)], axis=1)
    for c in range(4):
        at = slice(c * chunk, (c + 1) * chunk)
        out = jnp.dot(heads, wo[:, at], preferred_element_type=f32)
        for j in range(4):
            mpart[c, j] = out[j * share : (j + 1) * share].astype(bf16)
        for i, to in enumerate((td, tx, ty)):
            remote(mpart.at[c, to], mrecv.at[c, i], ssem.at[5], mr.at[c], tp=to).start()

    for i in range(n_ep):
        finish(i)
    lg_load.wait()
    ids = rt_ref[...].astype(f32)
    logits = lg_ref[...]
    stacked = jnp.where(
        sub == 0,
        ids[0:1, :],
        jnp.where(sub == 1, ids[1:2, :], jnp.where(sub == 2, logits[0:1, :], logits[1:2, :])),
    )
    columns = stacked.T
    r0 = columns[:, 0:1].astype(jnp.int32)
    r1 = columns[:, 1:2].astype(jnp.int32)
    lower = jnp.where(lane < sub, 1.0, 0.0).astype(bf16)
    rank = jnp.dot(lower, named_t.T.astype(bf16), preferred_element_type=f32)
    total_lane = lax.broadcasted_iota(jnp.int32, (tokens, rows), 1)

    def chosen(r):
        slot = jnp.sum(jnp.where(lane == r, rank, 0.0), axis=-1, keepdims=True)
        target = r * cap + slot.astype(jnp.int32)
        return jnp.where(total_lane == target, 1.0, 0.0).astype(bf16)

    c0 = chosen(r0)
    c1 = chosen(r1)
    l0 = columns[:, 2:3]
    l1 = columns[:, 3:4]
    w0 = jax.nn.sigmoid(l0 - l1)
    w1 = jax.nn.sigmoid(l1 - l0)
    wait_in(ret.at[pl.ds(0, n_ep - 1)], br.at[0])
    results = ret[...].astype(f32).reshape(rows, slab).astype(bf16)
    first = jnp.dot(c0, results, preferred_element_type=f32)
    second = jnp.dot(c1, results, preferred_element_type=f32)
    eout_ref[...] = (w0 * first + w1 * second).astype(bf16)
    for c in range(4):
        wait_in(mrecv.at[c], mr.at[c])
        summed = mpart[c, t].astype(f32)
        for i in range(3):
            summed = summed + mrecv[c, i].astype(f32)
        mixed_ref[:, c * chunk : (c + 1) * chunk] = summed.astype(bf16)

    wait_out(disp.at[pl.ds(0, n_ep - 1)], ssem.at[0])
    wait_out(xq.at[pl.ds(0, 3)], ssem.at[1])

    @pl.when(inner)
    def _():
        wait_out(kv.at[:, 0], ssem.at[2])
        wait_out(kv.at[pl.ds(0, 3), 0], ssem.at[3])

    @pl.when(~inner)
    def _():
        wait_out(kv.at[pl.ds(0, 2), 0], ssem.at[3])

    wait_out(mrecv, ssem.at[5])
    wait_out(part.at[pl.ds(0, 3)], ssem.at[6])
    wait_out(back.at[pl.ds(0, n_ep - 1)], ssem.at[7])


def hand_over(a_ref, b_ref, a_out, b_out, sem):
    one = pltpu.make_async_copy(a_ref, a_out, sem.at[0])
    two = pltpu.make_async_copy(b_ref, b_out, sem.at[1])
    one.start()
    two.start()
    one.wait()
    two.wait()


def kernel_form(
    queries,
    keys,
    values,
    query_gain,
    key_gain,
    out_weight,
    expert_input,
    norm_gain,
    routes,
    route_logits,
    gate_weight,
    up_weight,
    down_weight,
):
    bf16, f32 = jnp.bfloat16, jnp.float32
    n_ep = lax.axis_size("ep")
    tokens = queries.shape[0]
    head_dim = query_gain.shape[0]
    heads = queries.shape[1] // head_dim
    kv_here = keys.shape[1] // head_dim
    width = expert_input.shape[1]
    n_tp = lax.axis_size("tp")
    slab = width // n_tp
    cap = tokens * routes.shape[1] // n_ep * 5 // 4
    rows = n_ep * cap
    ff = gate_weight.shape[2]
    share = tokens // n_tp
    chunk = out_weight.shape[1] // 4
    table = jnp.asarray(rope_constants(tokens * n_ep, head_dim))
    vmem = pl.BlockSpec(memory_space=pltpu.VMEM)
    hbm = pl.BlockSpec(memory_space=pl.ANY)
    piece = (n_ep, cap, slab)
    dma = pltpu.SemaphoreType.DMA
    dims = (n_ep, cap, head_dim, kv_here, heads // kv_here)
    outs = pl.pallas_call(
        functools.partial(fused, dims),
        name="fused",
        out_shape=(
            pltpu.VMEM((share, out_weight.shape[1]), bf16),
            pltpu.VMEM((tokens, slab), bf16),
        ),
        in_specs=[hbm] * 14,
        out_specs=(vmem, vmem),
        scratch_shapes=[
            pltpu.VMEM(queries.shape, bf16),
            pltpu.VMEM(keys.shape, bf16),
            pltpu.VMEM(expert_input.shape, bf16),
            pltpu.VMEM((1, head_dim), f32),
            pltpu.VMEM((1, head_dim), f32),
            pltpu.VMEM((1, width), f32),
            pltpu.VMEM((2, tokens), jnp.int32),
            pltpu.VMEM((2, tokens), f32),
            pltpu.VMEM(out_weight.shape, bf16),
            pltpu.VMEM((ff, width), bf16),
            pltpu.VMEM((ff, width), bf16),
            pltpu.VMEM(down_weight.shape[1:], bf16),
            pltpu.VMEM((2, tokens, head_dim), f32),
            pltpu.VMEM(piece, bf16),
            pltpu.VMEM((n_tp,) + piece, bf16),
            pltpu.VMEM((rows, ff), f32),
            pltpu.VMEM((rows, ff), f32),
            pltpu.VMEM((rows, ff), bf16),
            pltpu.VMEM((n_tp,) + piece, bf16),
            pltpu.VMEM(piece, bf16),
            pltpu.VMEM((2,) + piece, bf16),
            pltpu.VMEM(piece, bf16),
            pltpu.VMEM(piece, bf16),
            pltpu.VMEM((kv_here, 2, n_ep // 2, 2, tokens, head_dim), bf16),
            pltpu.VMEM((heads, tokens, head_dim), bf16),
            pltpu.VMEM((kv_here, heads // kv_here, tokens, head_dim), bf16),
            pltpu.VMEM((kv_here, tokens, heads // kv_here * head_dim), bf16),
            pltpu.VMEM((kv_here, tokens, heads // kv_here * head_dim), bf16),
            pltpu.VMEM((tokens, width), f32),
            pltpu.VMEM((4, n_tp, share, chunk), bf16),
            pltpu.VMEM((4, 3, share, chunk), bf16),
            dma((13 + kv_here,)),
            dma((8,)),
            dma((n_ep,)),
            dma((n_ep // 2 + 1,)),
            dma((n_ep // 2 + 1,)),
            dma((1,)),
            dma((kv_here, n_ep // 2)),
            dma((kv_here,)),
            dma((kv_here,)),
            dma((kv_here,)),
            dma((n_ep,)),
            dma((n_ep,)),
            dma((1,)),
            dma((4,)),
        ],
        compiler_params=pltpu.CompilerParams(
            collective_id=0, has_side_effects=True, vmem_limit_bytes=60 * 1024 * 1024
        ),
    )(
        queries,
        keys,
        values,
        query_gain.reshape(1, -1),
        key_gain.reshape(1, -1),
        out_weight,
        expert_input,
        norm_gain.reshape(1, -1),
        routes.T,
        route_logits.T,
        jnp.swapaxes(gate_weight, 1, 2),
        jnp.swapaxes(up_weight, 1, 2),
        down_weight,
        table,
    )
    return pl.pallas_call(
        hand_over,
        name="hand_over",
        out_shape=tuple(jax.ShapeDtypeStruct(o.shape, o.dtype) for o in outs),
        in_specs=[vmem, vmem],
        out_specs=(hbm, hbm),
        scratch_shapes=[dma((2,))],
    )(*(pltpu.with_memory_space_constraint(o, pltpu.VMEM) for o in outs))


def dispatch_form(mesh, *args):
    queries, routes = args[0], args[8]
    tokens = queries.shape[0]
    n_ep, n_tp = mesh.shape["ep"], mesh.shape["tp"]
    cap = tokens * routes.shape[1] // n_ep * 5 // 4
    same = args[6].shape[0] == tokens and tokens % 128 == 0
    fits = n_tp == 4 and n_ep == 8 and cap % 8 == 0
    if same and fits and routes.shape[1] == 2 and tokens == 128:
        return kernel_form(*args)
    return local(*args)


def solution(mesh):
    placed = (
        P("ep", "tp"),
        P("ep", "tp"),
        P("ep", "tp"),
        P(),
        P(),
        P("tp", None),
        P("ep", None),
        P(),
        P("ep", None),
        P("ep", None),
        P("ep", None, "tp"),
        P("ep", None, "tp"),
        P("ep", "tp", None),
    )
    return jax.shard_map(
        functools.partial(dispatch_form, mesh),
        mesh=mesh,
        in_specs=placed,
        out_specs=(P(("ep", "tp"), None), P("ep", "tp")),
        check_vma=False,
    )
```

```python
import functools
import jax
import jax.numpy as jnp
import numpy as np
from jax import lax
from jax.experimental import pallas as pl
from jax.experimental.pallas import tpu as pltpu
from jax.sharding import PartitionSpec as P

GRID_W = 64


def rope_tables(count, offset, head_dim):
    pos = offset + lax.iota(jnp.int32, count)
    grid_row = (pos // GRID_W).astype(jnp.float32)
    grid_col = (pos % GRID_W).astype(jnp.float32)
    quarter = head_dim // 4
    inverse = 10000.0 ** (-jnp.arange(quarter, dtype=jnp.float32) / quarter)
    angles = jnp.concatenate([grid_row[:, None] * inverse, grid_col[:, None] * inverse], axis=-1)
    return (jnp.cos(angles), jnp.sin(angles))


def norm_rotate(x, gain, cosine, sine):
    count, number, head_dim = x.shape
    y = x * lax.rsqrt(jnp.mean(x * x, axis=-1, keepdims=True) + 1e-06) * gain
    pairs = y.reshape(count, number, head_dim // 2, 2)
    first, second = (pairs[..., 0], pairs[..., 1])
    cos_b = cosine[:, None, :]
    sin_b = sine[:, None, :]
    turned = jnp.stack([first * cos_b - second * sin_b, first * sin_b + second * cos_b], axis=-1)
    return turned.reshape(count, number, head_dim).astype(jnp.bfloat16)


def key_block_size(length, shard_rows):
    if length <= 2048:
        return length
    shards = length // shard_rows
    most = max(1, 2048 // shard_rows)
    best = 1
    for count in range(1, most + 1):
        if shards % count == 0:
            best = count
    return best * shard_rows


def local(
    queries,
    keys,
    values,
    query_gain,
    key_gain,
    out_weight,
    expert_input,
    norm_gain,
    routes,
    route_logits,
    gate_weight,
    up_weight,
    down_weight,
):
    tokens_here = queries.shape[0]
    head_dim = query_gain.shape[0]
    heads_here = queries.shape[1] // head_dim
    kv_here = keys.shape[1] // head_dim
    group = heads_here // kv_here
    offset = lax.axis_index("ep") * tokens_here
    cosine, sine = rope_tables(tokens_here, offset, head_dim)
    q_rot = norm_rotate(
        queries.astype(jnp.float32).reshape(tokens_here, heads_here, head_dim),
        query_gain,
        cosine,
        sine,
    )
    k_rot = norm_rotate(
        keys.astype(jnp.float32).reshape(tokens_here, kv_here, head_dim), key_gain, cosine, sine
    ).reshape(tokens_here, kv_here * head_dim)
    q_grouped = q_rot.reshape(tokens_here, kv_here, group, head_dim).transpose(1, 2, 0, 3)
    q_grouped = q_grouped.reshape(kv_here, group * tokens_here, head_dim)
    query_rows = group * tokens_here
    scale = head_dim ** (-0.5)
    start_state = (
        jnp.full((kv_here, query_rows), -1e30, jnp.float32),
        jnp.zeros((kv_here, query_rows), jnp.float32),
        jnp.zeros((kv_here, query_rows, head_dim), jnp.float32),
    )
    key_piece = lax.all_gather(k_rot, "ep", axis=0, tiled=True)
    value_piece = lax.all_gather(values, "ep", axis=0, tiled=True)
    length = key_piece.shape[0]
    block = key_block_size(length, tokens_here)
    key_blocks = key_piece.reshape(length // block, block, kv_here, head_dim)
    value_blocks = value_piece.reshape(length // block, block, kv_here, head_dim)

    def step(state, blocks):
        running_max, running_total, running_sum = state
        key_block, value_block = blocks
        scores = (
            jnp.einsum("kqd,lkd->kql", q_grouped, key_block, preferred_element_type=jnp.float32)
            * scale
        )
        new_max = jnp.maximum(running_max, jnp.max(scores, axis=-1))
        factor = jnp.exp(running_max - new_max)
        weights = jnp.exp(scores - new_max[..., None])
        new_total = running_total * factor + jnp.sum(weights, axis=-1)
        new_sum = running_sum * factor[..., None] + jnp.einsum(
            "kql,lkd->kqd",
            weights.astype(jnp.bfloat16),
            value_block,
            preferred_element_type=jnp.float32,
        )
        return ((new_max, new_total, new_sum), None)

    result, _ = lax.scan(step, start_state, (key_blocks, value_blocks))
    final_max, final_total, final_sum = result
    attended = (final_sum / final_total[..., None]).astype(jnp.bfloat16)
    attended = attended.reshape(kv_here, group, tokens_here, head_dim).transpose(2, 0, 1, 3)
    attended = attended.reshape(tokens_here, heads_here * head_dim)
    summed = lax.psum_scatter(
        jnp.dot(attended, out_weight, preferred_element_type=jnp.float32).astype(jnp.bfloat16),
        "tp",
        scatter_dimension=0,
        tiled=True,
    ).astype(jnp.float32)
    mixed = summed.astype(jnp.bfloat16)
    expert_tokens_here, width = expert_input.shape
    n_ep = lax.axis_size("ep")
    top = routes.shape[1]
    capacity = expert_tokens_here * top // n_ep * 5 // 4
    x = expert_input.astype(jnp.float32)
    normed = (x * lax.rsqrt(jnp.mean(x * x, axis=-1, keepdims=True) + 1e-06) * norm_gain).astype(
        jnp.bfloat16
    )
    expert_ids = routes.reshape(-1)
    onehot = (expert_ids[:, None] == lax.iota(jnp.int32, n_ep)[None, :]).astype(jnp.int32)
    before = jnp.cumsum(onehot, axis=0) - onehot
    slot = jnp.sum(before * onehot, axis=1)
    target = expert_ids * capacity + slot
    owner_row = lax.iota(jnp.int32, expert_tokens_here * top) // top
    w_gate = gate_weight[0]
    w_up = up_weight[0]
    w_down = down_weight[0]
    columns = normed.shape[1]
    filled = jnp.zeros((n_ep * capacity, columns), jnp.bfloat16).at[target].set(normed[owner_row])
    arrived = lax.all_to_all(
        filled.reshape(n_ep, capacity, columns), "ep", split_axis=0, concat_axis=0, tiled=True
    )
    sources, slots, work_columns = arrived.shape
    flat = arrived.reshape(sources * slots, work_columns)
    gate = jnp.dot(flat, w_gate, preferred_element_type=jnp.float32)
    upper = jnp.dot(flat, w_up, preferred_element_type=jnp.float32)
    hidden = (jax.nn.silu(gate) * upper).astype(jnp.bfloat16)
    partial_out = jnp.dot(hidden, w_down, preferred_element_type=jnp.float32)
    summed = lax.psum_scatter(
        partial_out.reshape(sources, slots, width).astype(jnp.bfloat16),
        "tp",
        scatter_dimension=2,
        tiled=True,
    ).astype(jnp.float32)
    returned = lax.all_to_all(
        summed.astype(jnp.bfloat16), "ep", split_axis=0, concat_axis=0, tiled=True
    )
    picked = returned.reshape(n_ep * capacity, -1)[target].reshape(expert_tokens_here, top, -1)
    route_weight = jax.nn.sigmoid(route_logits - route_logits[:, ::-1])
    combined = jnp.sum(route_weight[..., None] * picked.astype(jnp.float32), axis=1)
    expert_out = combined.astype(jnp.bfloat16)
    return (mixed, expert_out)


MESH = pl.DeviceIdType.MESH


def rope_constants(length, head_dim):
    pos = np.arange(length)
    quarter = head_dim // 4
    inverse = (np.float32(10000.0) ** (-np.arange(quarter, dtype=np.float32) / np.float32(quarter))).astype(np.float32)
    grid_row = (pos // GRID_W).astype(np.float32)
    grid_col = (pos % GRID_W).astype(np.float32)
    angles = np.concatenate([grid_row[:, None] * inverse, grid_col[:, None] * inverse], axis=-1)
    cosine = np.repeat(np.cos(angles), 2, axis=-1).astype(np.float32)
    sine = np.repeat(np.sin(angles), 2, axis=-1).astype(np.float32)
    sine[:, 0::2] *= -1.0
    return np.stack([cosine, sine])


def fused(
    dims,
    q_hbm,
    k_hbm,
    v_hbm,
    qg_hbm,
    kg_hbm,
    wo_hbm,
    x_hbm,
    ng_hbm,
    rt_hbm,
    lg_hbm,
    wg_hbm,
    wu_hbm,
    wd_hbm,
    rope_hbm,
    mixed_ref,
    eout_ref,
    q_ref,
    k_ref,
    x_ref,
    qg_ref,
    kg_ref,
    ng_ref,
    rt_ref,
    lg_ref,
    wo,
    wg,
    wu,
    wd,
    rope,
    disp,
    xq,
    gacc,
    uacc,
    hid,
    part,
    rdiag,
    rs,
    back,
    ret,
    kv,
    qrot,
    qship,
    att,
    aship,
    macc,
    mpart,
    mrecv,
    wsem,
    ssem,
    zr,
    axr,
    ayr,
    afr,
    kvr,
    kvm,
    qsr,
    atr,
    rdr,
    rsr,
    br,
    mr,
):
    n_ep, cap, head_dim, kv_here, group = dims
    f32, bf16 = jnp.float32, jnp.bfloat16
    chips = n_ep // 2
    me = lax.axis_index("ep")
    t = lax.axis_index("tp")
    tx = t + 1 - 2 * (t % 2)
    ty = (t + 2) % 4
    td = 3 - t
    z = me // 2
    core = me % 2
    mate = 2 * z + 1 - core
    inner = (z == 1) | (z == 2)
    partner = z + 1 - 2 * (z % 2)
    other = 3 - z
    far_end = 3 - partner
    near = [partner, jnp.where(z < 2, 2, 1), jnp.where(z < 2, 3, 0)]
    half = n_ep // 2
    order = [me, mate]
    for chip in near:
        order += [2 * chip + core, 2 * chip + 1 - core]
    base = [half * (z // 2), half * (1 - z // 2)]
    turns = [order[:half][::-1], order[half:][::-1]]
    first_to = []
    for chip in (partner, other, far_end):
        first_to += [2 * chip + core, 2 * chip + 1 - core]
    tokens = x_ref.shape[0]
    slab = disp.shape[2]
    rows = n_ep * cap

    loads = [
        (x_hbm, x_ref),
        (rt_hbm, rt_ref),
        (ng_hbm, ng_ref),
        (k_hbm, k_ref),
        (rope_hbm.at[:, pl.ds(pl.multiple_of(me * tokens, tokens), tokens), :], rope),
        (kg_hbm, kg_ref),
    ]
    for g in range(kv_here):
        loads.append((v_hbm.at[:, g * head_dim : (g + 1) * head_dim], kv.at[g, core, z, 1]))
    loads += [
        (q_hbm, q_ref),
        (qg_hbm, qg_ref),
        (lg_hbm, lg_ref),
        (wg_hbm.at[0], wg),
        (wu_hbm.at[0], wu),
        (wd_hbm.at[0], wd),
        (wo_hbm, wo),
    ]
    loads = [pltpu.make_async_copy(a, b, wsem.at[i]) for i, (a, b) in enumerate(loads)]
    x_load, rt_load, ng_load, k_load, rope_load, kg_load = loads[:6]
    v_loads = loads[6 : 6 + kv_here]
    q_load, qg_load, lg_load, wg_load, wu_load, wd_load, wo_load = loads[6 + kv_here :]
    x_load.start()
    rt_load.start()

    barrier = pltpu.get_barrier_semaphore()
    for d in range(1, n_ep):
        pl.semaphore_signal(barrier, inc=1, device_id={"ep": (me + d) % n_ep}, device_id_type=MESH)
    for peer in (tx, ty, td):
        pl.semaphore_signal(barrier, inc=1, device_id={"tp": peer}, device_id_type=MESH)
    for load in loads[2:]:
        load.start()

    rt_load.wait()
    wide = (tokens, tokens)
    lane = lax.broadcasted_iota(jnp.int32, wide, 1)
    sub = lax.broadcasted_iota(jnp.int32, wide, 0)
    routed = (sub == rt_ref[0:1, :]) | (sub == rt_ref[1:2, :])
    named_t = jnp.where(routed, 1.0, 0.0)
    upper = jnp.where(sub < lane, 1.0, 0.0).astype(bf16)
    rank_t = jnp.dot(named_t.astype(bf16), upper, preferred_element_type=f32)
    slot_iota = lax.broadcasted_iota(jnp.int32, (cap, tokens), 0).astype(f32)
    picks = [
        jnp.where((slot_iota == rank_t[e : e + 1, :]) & (named_t[e : e + 1, :] > 0.5), 1.0, 0.0)
        for e in range(n_ep)
    ]
    pick = jnp.concatenate(picks, axis=0).astype(bf16)

    ng_load.wait()
    x_load.wait()
    x = x_ref[...].astype(f32)
    inv = lax.rsqrt(jnp.mean(x * x, axis=-1, keepdims=True) + 1e-06)
    cols = pl.ds(pl.multiple_of(t * slab, slab), slab)
    normed = (x_ref[:, cols].astype(f32) * inv * ng_ref[:, cols]).astype(bf16)
    sent = jnp.dot(pick, normed, preferred_element_type=f32)
    for e in range(n_ep):
        disp[e] = sent[e * cap : (e + 1) * cap].astype(bf16)
    xq[t, me] = disp[me]

    pl.semaphore_wait(barrier, n_ep - 1 + 3)

    def remote(a, b, s, r, **where):
        return pltpu.make_async_remote_copy(
            src_ref=a, dst_ref=b, send_sem=s, recv_sem=r, device_id=where, device_id_type=MESH
        )

    def wait_in(ref, sem):
        remote(ref, ref, ssem.at[0], sem, tp=tx).wait_recv()

    def wait_out(ref, sem):
        remote(ref, ref, sem, zr.at[0], tp=tx).wait_send()

    for e in [mate] + first_to:
        remote(disp.at[e], xq.at[t, me], ssem.at[0], zr.at[me], ep=e).start()

    def spread(i):
        s = order[i]
        rest = half + i // half
        at_x, at_y = (i // 2, rest) if i % 2 == 0 else (rest, i // 2)
        remote(xq.at[t, s], xq.at[t, s], ssem.at[1], axr.at[at_x], tp=tx).start()
        remote(xq.at[t, s], xq.at[t, s], ssem.at[1], ayr.at[at_y], tp=ty).start()

    def forward(i):
        s = order[i]
        if i % 2 == 0:
            wait_in(xq.at[tx, s], axr.at[i // 2])
            remote(xq.at[tx, s], xq.at[tx, s], ssem.at[1], afr.at[i // half], tp=ty).start()
        else:
            wait_in(xq.at[ty, s], ayr.at[i // 2])
            remote(xq.at[ty, s], xq.at[ty, s], ssem.at[1], afr.at[i // half], tp=tx).start()

    spread(0)

    rope_load.wait()
    cos = rope[0]
    sin = rope[1]
    even = lax.broadcasted_iota(jnp.int32, (tokens, head_dim), 1) % 2 == 0

    def turn(piece, gain):
        a = piece.astype(f32)
        y = a * lax.rsqrt(jnp.mean(a * a, axis=-1, keepdims=True) + 1e-06) * gain
        other = jnp.where(even, pltpu.roll(y, head_dim - 1, 1), pltpu.roll(y, 1, 1))
        return (y * cos + other * sin).astype(bf16)

    kg_load.wait()
    k_load.wait()
    for g in range(kv_here):
        kv[g, core, z, 0] = turn(k_ref[:, g * head_dim : (g + 1) * head_dim], kg_ref[...])

    def kv_send(g, chip, to):
        block = kv.at[g, core, chip]
        remote(block, block, ssem.at[3], kvr.at[g, chip], ep=2 * to + core).start()

    def kv_mate(g, chip):
        block = kv.at[g, core, chip]
        remote(block, block, ssem.at[2], kvm.at[g], ep=mate).start()

    for v_load in v_loads:
        v_load.wait()

    def receive(i):
        wait_in(xq.at[t, order[i]], zr.at[order[i]])
        spread(i)

    receive(1)
    q_load.wait()
    qg_load.wait()
    for h in range(kv_here * group):
        qrot[h] = turn(q_ref[:, h * head_dim : (h + 1) * head_dim], qg_ref[...])
    q_of = lambda g: qrot.at[pl.ds(g * group, group)]

    def gate_up(q, k, first=False):
        block = xq[q, pl.ds(base[k], half)].astype(f32).reshape(half * cap, slab).astype(bf16)
        at = pl.ds(pl.multiple_of(q * slab, slab), slab)
        g = lax.dot_general(block, wg[:, at], (((1,), (1,)), ((), ())), preferred_element_type=f32)
        u = lax.dot_general(block, wu[:, at], (((1,), (1,)), ((), ())), preferred_element_type=f32)
        if first:
            gacc[k] = g
            uacc[k] = u
        else:
            gacc[k] += g
            uacc[k] += u

    def sides(k):
        wait_in(xq.at[tx, pl.ds(0, half // 2)], axr.at[half + k])
        wait_in(xq.at[ty, pl.ds(0, half // 2)], ayr.at[half + k])

    def corner(k):
        wait_in(xq.at[td, pl.ds(0, half)], afr.at[k])

    def activate(k):
        gate = gacc[k]
        hid[k] = (gate / (1.0 + jnp.exp(-gate)) * uacc[k]).astype(bf16)

    def down(q, k):
        at = pl.ds(pl.multiple_of(q * slab, slab), slab)
        out = jnp.dot(hid[k], wd[:, at], preferred_element_type=f32)
        for s in range(half):
            part[q, base[k] + s] = out[s * cap : (s + 1) * cap].astype(bf16)

    def rx_copy(s):
        remote(part.at[tx, s], rs.at[0, s], ssem.at[6], rsr.at[s], tp=tx).start()

    def ry_copy(s):
        remote(part.at[ty, s], rs.at[1, s], ssem.at[6], rsr.at[s], tp=ty).start()

    def send_far(k):
        for j, s in enumerate(turns[k]):
            remote(part.at[td, s], rdiag.at[s], ssem.at[6], rdr.at[s], tp=tx if j % 2 == 0 else ty).start()

    def send_near(k):
        for s in turns[k][0::2]:
            rx_copy(s)
        for s in turns[k][1::2]:
            ry_copy(s)

    def corner_far(k):
        corner(k)
        gate_up(td, k)
        activate(k)
        down(td, k)

    def down_rest(k):
        down(tx, k)
        down(ty, k)
        down(t, k)

    receive(2)
    receive(3)

    @pl.when(~inner)
    def _():
        for g in range(kv_here):
            kv_send(g, z, partner)
        for g in range(kv_here):
            remote(q_of(g), qship.at[g], ssem.at[3], qsr.at[g], ep=2 * partner + core).start()

    forward(0)
    forward(1)

    wg_load.wait()
    wu_load.wait()

    @pl.when(~inner)
    def _():
        forward(2)
        forward(3)
        gate_up(t, 0, True)

    receive(4)
    receive(5)

    @pl.when(inner)
    def _():
        kv_send(0, z, other)
        kv_mate(0, z)
        gate_up(t, 0, True)
        forward(2)
        forward(3)

    receive(6)
    receive(7)

    def own_kv(heads):
        @pl.when(inner)
        def _():
            for g in heads:
                kv_send(g, z, other)
                kv_mate(g, z)

    def relay_kv(heads, source, on):
        @pl.when(inner)
        def _():
            for g in heads:
                block = kv.at[g, core, source]
                wait_in(block, kvr.at[g, source])
                if on:
                    kv_send(g, source, other)
                kv_mate(g, source)

    own_kv((1,))
    scale = head_dim ** (-0.5) * 1.4426950408889634
    share = tokens // 4
    width = wo.shape[1]
    chunk = width // 4

    def attend_one(g, q2):
        keys = kv[g, :, :, 0].reshape(n_ep * tokens, head_dim)
        vals = kv[g, :, :, 1].reshape(n_ep * tokens, head_dim)
        q2 = q2.reshape(group * tokens, head_dim)
        s = lax.dot_general(q2, keys, (((1,), (1,)), ((), ())), preferred_element_type=f32)
        peak = jnp.max(s, axis=-1, keepdims=True)
        p = jnp.exp2((s - peak) * scale)
        total = jnp.sum(p, axis=-1, keepdims=True)
        out = jnp.dot(p.astype(bf16), vals, preferred_element_type=f32) / total
        return jnp.concatenate([out[r * tokens : (r + 1) * tokens] for r in range(group)], axis=1).astype(bf16)

    def attend_ship(heads):
        @pl.when(inner)
        def _():
            for g in heads:
                wait_in(qship.at[g], qsr.at[g])
                wait_in(kv.at[g, 1 - core], kvm.at[g])
                aship[g] = attend_one(g, qship[g])
                remote(aship.at[g], att.at[g], ssem.at[3], atr.at[g], ep=2 * partner + core).start()

    def meet(k):
        for j, s in enumerate(turns[k]):
            wait_in(rdiag.at[s], rdr.at[s])
            if j % 2 == 0:
                part[ty, s] = (part[ty, s].astype(f32) + rdiag[s].astype(f32)).astype(bf16)
                ry_copy(s)
            else:
                part[tx, s] = (part[tx, s].astype(f32) + rdiag[s].astype(f32)).astype(bf16)
                rx_copy(s)

    def finish(k):
        for j, s in enumerate(turns[k]):
            wait_in(rs.at[0, pl.ds(0, 2)], rsr.at[s])
            out = (part[t, s].astype(f32) + rs[0, s].astype(f32) + rs[1, s].astype(f32)).astype(bf16)
            if k == 0 and j == half - 1:
                ret[s] = out
            else:
                back[s] = out
                remote(back.at[s], ret.at[me], ssem.at[7], br.at[0], ep=s).start()

    share = tokens // 4
    width = wo.shape[1]
    chunk = width // 4

    wd_load.wait()
    sides(0)
    gate_up(tx, 0)
    gate_up(ty, 0)

    @pl.when(~inner)
    def _():
        corner_far(0)
        down_rest(0)

    forward(4)
    forward(5)
    relay_kv((0,), partner, True)
    own_kv((2,))

    @pl.when(inner)
    def _():
        corner_far(0)

    send_far(0)
    forward(6)
    forward(7)
    relay_kv((1,), partner, True)
    own_kv((3,))
    relay_kv((0, 1), other, False)

    @pl.when(inner)
    def _():
        down_rest(0)

    send_near(0)
    relay_kv((2, 3), partner, True)
    relay_kv((0,), far_end, False)
    gate_up(t, 1, True)
    sides(1)
    gate_up(tx, 1)
    gate_up(ty, 1)
    attend_ship((0,))
    relay_kv((2,), other, False)
    relay_kv((1,), far_end, False)
    corner_far(1)
    send_far(1)
    down_rest(1)
    send_near(1)
    meet(0)
    attend_ship((1,))
    relay_kv((3,), other, False)
    relay_kv((2,), far_end, False)
    relay_kv((3,), far_end, False)
    attend_ship((2, 3))
    meet(1)

    @pl.when(inner)
    def _():
        for g in range(kv_here):
            att[g] = attend_one(g, qrot[g * group : (g + 1) * group])

    finish(0)
    finish(1)


    def attended(heads):
        @pl.when(~inner)
        def _():
            for g in heads:
                wait_in(att.at[g], atr.at[g])

    attended(range(kv_here - 1))
    wo_load.wait()
    cut = (kv_here - 1) * group * head_dim
    early = jnp.concatenate([att[g] for g in range(kv_here - 1)], axis=1)
    macc[...] = jnp.dot(early, wo[:cut, :], preferred_element_type=f32)
    attended((kv_here - 1,))
    for c in range(4):
        at = slice(c * chunk, (c + 1) * chunk)
        out = macc[:, at] + jnp.dot(att[kv_here - 1], wo[cut:, at], preferred_element_type=f32)
        for j in range(4):
            mpart[c, j] = out[j * share : (j + 1) * share].astype(bf16)
        for i, to in enumerate((td, tx, ty)):
            remote(mpart.at[c, to], mrecv.at[c, i], ssem.at[5], mr.at[c], tp=to).start()

    lg_load.wait()
    ids = rt_ref[...].astype(f32)
    logits = lg_ref[...]
    stacked = jnp.where(
        sub == 0,
        ids[0:1, :],
        jnp.where(sub == 1, ids[1:2, :], jnp.where(sub == 2, logits[0:1, :], logits[1:2, :])),
    )
    columns = stacked.T
    r0 = columns[:, 0:1].astype(jnp.int32)
    r1 = columns[:, 1:2].astype(jnp.int32)
    lower = jnp.where(lane < sub, 1.0, 0.0).astype(bf16)
    rank = jnp.dot(lower, named_t.T.astype(bf16), preferred_element_type=f32)
    total_lane = lax.broadcasted_iota(jnp.int32, (tokens, rows), 1)

    def chosen(r):
        slot = jnp.sum(jnp.where(lane == r, rank, 0.0), axis=-1, keepdims=True)
        target = r * cap + slot.astype(jnp.int32)
        return jnp.where(total_lane == target, 1.0, 0.0).astype(bf16)

    c0 = chosen(r0)
    c1 = chosen(r1)
    l0 = columns[:, 2:3]
    l1 = columns[:, 3:4]
    w0 = jax.nn.sigmoid(l0 - l1)
    w1 = jax.nn.sigmoid(l1 - l0)
    wait_in(ret.at[pl.ds(0, n_ep - 1)], br.at[0])
    results = ret[...].astype(f32).reshape(rows, slab).astype(bf16)
    first = jnp.dot(c0, results, preferred_element_type=f32)
    second = jnp.dot(c1, results, preferred_element_type=f32)
    eout_ref[...] = (w0 * first + w1 * second).astype(bf16)
    for c in range(4):
        wait_in(mrecv.at[c], mr.at[c])
        summed = mpart[c, t].astype(f32)
        for i in range(3):
            summed = summed + mrecv[c, i].astype(f32)
        mixed_ref[:, c * chunk : (c + 1) * chunk] = summed.astype(bf16)

    wait_out(disp.at[pl.ds(0, n_ep - 1)], ssem.at[0])
    wait_out(xq.at[pl.ds(0, 3)], ssem.at[1])

    @pl.when(inner)
    def _():
        wait_out(kv.at[:, 0], ssem.at[2])
        wait_out(kv.at[pl.ds(0, 3), 0], ssem.at[3])

    @pl.when(~inner)
    def _():
        wait_out(kv.at[pl.ds(0, 2), 0], ssem.at[3])

    wait_out(mrecv, ssem.at[5])
    wait_out(part.at[pl.ds(0, 3)], ssem.at[6])
    wait_out(back.at[pl.ds(0, n_ep - 1)], ssem.at[7])


def hand_over(a_ref, b_ref, a_out, b_out, sem):
    one = pltpu.make_async_copy(a_ref, a_out, sem.at[0])
    two = pltpu.make_async_copy(b_ref, b_out, sem.at[1])
    one.start()
    two.start()
    one.wait()
    two.wait()


def kernel_form(
    queries,
    keys,
    values,
    query_gain,
    key_gain,
    out_weight,
    expert_input,
    norm_gain,
    routes,
    route_logits,
    gate_weight,
    up_weight,
    down_weight,
):
    bf16, f32 = jnp.bfloat16, jnp.float32
    n_ep = lax.axis_size("ep")
    tokens = queries.shape[0]
    head_dim = query_gain.shape[0]
    heads = queries.shape[1] // head_dim
    kv_here = keys.shape[1] // head_dim
    width = expert_input.shape[1]
    n_tp = lax.axis_size("tp")
    slab = width // n_tp
    cap = tokens * routes.shape[1] // n_ep * 5 // 4
    rows = n_ep * cap
    ff = gate_weight.shape[2]
    share = tokens // n_tp
    chunk = out_weight.shape[1] // 4
    table = jnp.asarray(rope_constants(tokens * n_ep, head_dim))
    vmem = pl.BlockSpec(memory_space=pltpu.VMEM)
    hbm = pl.BlockSpec(memory_space=pl.ANY)
    piece = (n_ep, cap, slab)
    dma = pltpu.SemaphoreType.DMA
    dims = (n_ep, cap, head_dim, kv_here, heads // kv_here)
    outs = pl.pallas_call(
        functools.partial(fused, dims),
        name="fused",
        out_shape=(
            pltpu.VMEM((share, out_weight.shape[1]), bf16),
            pltpu.VMEM((tokens, slab), bf16),
        ),
        in_specs=[hbm] * 14,
        out_specs=(vmem, vmem),
        scratch_shapes=[
            pltpu.VMEM(queries.shape, bf16),
            pltpu.VMEM(keys.shape, bf16),
            pltpu.VMEM(expert_input.shape, bf16),
            pltpu.VMEM((1, head_dim), f32),
            pltpu.VMEM((1, head_dim), f32),
            pltpu.VMEM((1, width), f32),
            pltpu.VMEM((2, tokens), jnp.int32),
            pltpu.VMEM((2, tokens), f32),
            pltpu.VMEM(out_weight.shape, bf16),
            pltpu.VMEM((ff, width), bf16),
            pltpu.VMEM((ff, width), bf16),
            pltpu.VMEM(down_weight.shape[1:], bf16),
            pltpu.VMEM((2, tokens, head_dim), f32),
            pltpu.VMEM(piece, bf16),
            pltpu.VMEM((n_tp,) + piece, bf16),
            pltpu.VMEM((2, rows // 2, ff), f32),
            pltpu.VMEM((2, rows // 2, ff), f32),
            pltpu.VMEM((2, rows // 2, ff), bf16),
            pltpu.VMEM((n_tp,) + piece, bf16),
            pltpu.VMEM(piece, bf16),
            pltpu.VMEM((2,) + piece, bf16),
            pltpu.VMEM(piece, bf16),
            pltpu.VMEM(piece, bf16),
            pltpu.VMEM((kv_here, 2, n_ep // 2, 2, tokens, head_dim), bf16),
            pltpu.VMEM((heads, tokens, head_dim), bf16),
            pltpu.VMEM((kv_here, heads // kv_here, tokens, head_dim), bf16),
            pltpu.VMEM((kv_here, tokens, heads // kv_here * head_dim), bf16),
            pltpu.VMEM((kv_here, tokens, heads // kv_here * head_dim), bf16),
            pltpu.VMEM((tokens, width), f32),
            pltpu.VMEM((4, n_tp, share, chunk), bf16),
            pltpu.VMEM((4, 3, share, chunk), bf16),
            dma((13 + kv_here,)),
            dma((8,)),
            dma((n_ep,)),
            dma((n_ep // 2 + 2,)),
            dma((n_ep // 2 + 2,)),
            dma((2,)),
            dma((kv_here, n_ep // 2)),
            dma((kv_here,)),
            dma((kv_here,)),
            dma((kv_here,)),
            dma((n_ep,)),
            dma((n_ep,)),
            dma((1,)),
            dma((4,)),
        ],
        compiler_params=pltpu.CompilerParams(
            collective_id=0, has_side_effects=True, vmem_limit_bytes=60 * 1024 * 1024
        ),
    )(
        queries,
        keys,
        values,
        query_gain.reshape(1, -1),
        key_gain.reshape(1, -1),
        out_weight,
        expert_input,
        norm_gain.reshape(1, -1),
        routes.T,
        route_logits.T,
        jnp.swapaxes(gate_weight, 1, 2),
        jnp.swapaxes(up_weight, 1, 2),
        down_weight,
        table,
    )
    return pl.pallas_call(
        hand_over,
        name="hand_over",
        out_shape=tuple(jax.ShapeDtypeStruct(o.shape, o.dtype) for o in outs),
        in_specs=[vmem, vmem],
        out_specs=(hbm, hbm),
        scratch_shapes=[dma((2,))],
    )(*(pltpu.with_memory_space_constraint(o, pltpu.VMEM) for o in outs))


def dispatch_form(mesh, *args):
    queries, routes = args[0], args[8]
    tokens = queries.shape[0]
    n_ep, n_tp = mesh.shape["ep"], mesh.shape["tp"]
    cap = tokens * routes.shape[1] // n_ep * 5 // 4
    same = args[6].shape[0] == tokens and tokens % 128 == 0
    fits = n_tp == 4 and n_ep == 8 and cap % 8 == 0
    if same and fits and routes.shape[1] == 2 and tokens == 128:
        return kernel_form(*args)
    return local(*args)


def solution(mesh):
    placed = (
        P("ep", "tp"),
        P("ep", "tp"),
        P("ep", "tp"),
        P(),
        P(),
        P("tp", None),
        P("ep", None),
        P(),
        P("ep", None),
        P("ep", None),
        P("ep", None, "tp"),
        P("ep", None, "tp"),
        P("ep", "tp", None),
    )
    return jax.shard_map(
        functools.partial(dispatch_form, mesh),
        mesh=mesh,
        in_specs=placed,
        out_specs=(P(("ep", "tp"), None), P("ep", "tp")),
        check_vma=False,
    )
```

```python
import functools
import jax
import jax.numpy as jnp
import numpy as np
from jax import lax
from jax.experimental import pallas as pl
from jax.experimental.pallas import tpu as pltpu
from jax.sharding import PartitionSpec as P

GRID_W = 64


def rope_tables(count, offset, head_dim):
    pos = offset + lax.iota(jnp.int32, count)
    grid_row = (pos // GRID_W).astype(jnp.float32)
    grid_col = (pos % GRID_W).astype(jnp.float32)
    quarter = head_dim // 4
    inverse = 10000.0 ** (-jnp.arange(quarter, dtype=jnp.float32) / quarter)
    angles = jnp.concatenate([grid_row[:, None] * inverse, grid_col[:, None] * inverse], axis=-1)
    return (jnp.cos(angles), jnp.sin(angles))


def norm_rotate(x, gain, cosine, sine):
    count, number, head_dim = x.shape
    y = x * lax.rsqrt(jnp.mean(x * x, axis=-1, keepdims=True) + 1e-06) * gain
    pairs = y.reshape(count, number, head_dim // 2, 2)
    first, second = (pairs[..., 0], pairs[..., 1])
    cos_b = cosine[:, None, :]
    sin_b = sine[:, None, :]
    turned = jnp.stack([first * cos_b - second * sin_b, first * sin_b + second * cos_b], axis=-1)
    return turned.reshape(count, number, head_dim).astype(jnp.bfloat16)


def key_block_size(length, shard_rows):
    if length <= 2048:
        return length
    shards = length // shard_rows
    most = max(1, 2048 // shard_rows)
    best = 1
    for count in range(1, most + 1):
        if shards % count == 0:
            best = count
    return best * shard_rows


def local(
    queries,
    keys,
    values,
    query_gain,
    key_gain,
    out_weight,
    expert_input,
    norm_gain,
    routes,
    route_logits,
    gate_weight,
    up_weight,
    down_weight,
):
    tokens_here = queries.shape[0]
    head_dim = query_gain.shape[0]
    heads_here = queries.shape[1] // head_dim
    kv_here = keys.shape[1] // head_dim
    group = heads_here // kv_here
    offset = lax.axis_index("ep") * tokens_here
    cosine, sine = rope_tables(tokens_here, offset, head_dim)
    q_rot = norm_rotate(
        queries.astype(jnp.float32).reshape(tokens_here, heads_here, head_dim),
        query_gain,
        cosine,
        sine,
    )
    k_rot = norm_rotate(
        keys.astype(jnp.float32).reshape(tokens_here, kv_here, head_dim), key_gain, cosine, sine
    ).reshape(tokens_here, kv_here * head_dim)
    q_grouped = q_rot.reshape(tokens_here, kv_here, group, head_dim).transpose(1, 2, 0, 3)
    q_grouped = q_grouped.reshape(kv_here, group * tokens_here, head_dim)
    query_rows = group * tokens_here
    scale = head_dim ** (-0.5)
    start_state = (
        jnp.full((kv_here, query_rows), -1e30, jnp.float32),
        jnp.zeros((kv_here, query_rows), jnp.float32),
        jnp.zeros((kv_here, query_rows, head_dim), jnp.float32),
    )
    key_piece = lax.all_gather(k_rot, "ep", axis=0, tiled=True)
    value_piece = lax.all_gather(values, "ep", axis=0, tiled=True)
    length = key_piece.shape[0]
    block = key_block_size(length, tokens_here)
    key_blocks = key_piece.reshape(length // block, block, kv_here, head_dim)
    value_blocks = value_piece.reshape(length // block, block, kv_here, head_dim)

    def step(state, blocks):
        running_max, running_total, running_sum = state
        key_block, value_block = blocks
        scores = (
            jnp.einsum("kqd,lkd->kql", q_grouped, key_block, preferred_element_type=jnp.float32)
            * scale
        )
        new_max = jnp.maximum(running_max, jnp.max(scores, axis=-1))
        factor = jnp.exp(running_max - new_max)
        weights = jnp.exp(scores - new_max[..., None])
        new_total = running_total * factor + jnp.sum(weights, axis=-1)
        new_sum = running_sum * factor[..., None] + jnp.einsum(
            "kql,lkd->kqd",
            weights.astype(jnp.bfloat16),
            value_block,
            preferred_element_type=jnp.float32,
        )
        return ((new_max, new_total, new_sum), None)

    result, _ = lax.scan(step, start_state, (key_blocks, value_blocks))
    final_max, final_total, final_sum = result
    attended = (final_sum / final_total[..., None]).astype(jnp.bfloat16)
    attended = attended.reshape(kv_here, group, tokens_here, head_dim).transpose(2, 0, 1, 3)
    attended = attended.reshape(tokens_here, heads_here * head_dim)
    summed = lax.psum_scatter(
        jnp.dot(attended, out_weight, preferred_element_type=jnp.float32).astype(jnp.bfloat16),
        "tp",
        scatter_dimension=0,
        tiled=True,
    ).astype(jnp.float32)
    mixed = summed.astype(jnp.bfloat16)
    expert_tokens_here, width = expert_input.shape
    n_ep = lax.axis_size("ep")
    top = routes.shape[1]
    capacity = expert_tokens_here * top // n_ep * 5 // 4
    x = expert_input.astype(jnp.float32)
    normed = (x * lax.rsqrt(jnp.mean(x * x, axis=-1, keepdims=True) + 1e-06) * norm_gain).astype(
        jnp.bfloat16
    )
    expert_ids = routes.reshape(-1)
    onehot = (expert_ids[:, None] == lax.iota(jnp.int32, n_ep)[None, :]).astype(jnp.int32)
    before = jnp.cumsum(onehot, axis=0) - onehot
    slot = jnp.sum(before * onehot, axis=1)
    target = expert_ids * capacity + slot
    owner_row = lax.iota(jnp.int32, expert_tokens_here * top) // top
    w_gate = gate_weight[0]
    w_up = up_weight[0]
    w_down = down_weight[0]
    columns = normed.shape[1]
    filled = jnp.zeros((n_ep * capacity, columns), jnp.bfloat16).at[target].set(normed[owner_row])
    arrived = lax.all_to_all(
        filled.reshape(n_ep, capacity, columns), "ep", split_axis=0, concat_axis=0, tiled=True
    )
    sources, slots, work_columns = arrived.shape
    flat = arrived.reshape(sources * slots, work_columns)
    gate = jnp.dot(flat, w_gate, preferred_element_type=jnp.float32)
    upper = jnp.dot(flat, w_up, preferred_element_type=jnp.float32)
    hidden = (jax.nn.silu(gate) * upper).astype(jnp.bfloat16)
    partial_out = jnp.dot(hidden, w_down, preferred_element_type=jnp.float32)
    summed = lax.psum_scatter(
        partial_out.reshape(sources, slots, width).astype(jnp.bfloat16),
        "tp",
        scatter_dimension=2,
        tiled=True,
    ).astype(jnp.float32)
    returned = lax.all_to_all(
        summed.astype(jnp.bfloat16), "ep", split_axis=0, concat_axis=0, tiled=True
    )
    picked = returned.reshape(n_ep * capacity, -1)[target].reshape(expert_tokens_here, top, -1)
    route_weight = jax.nn.sigmoid(route_logits - route_logits[:, ::-1])
    combined = jnp.sum(route_weight[..., None] * picked.astype(jnp.float32), axis=1)
    expert_out = combined.astype(jnp.bfloat16)
    return (mixed, expert_out)


MESH = pl.DeviceIdType.MESH


def rope_constants(length, head_dim):
    pos = np.arange(length)
    quarter = head_dim // 4
    inverse = (np.float32(10000.0) ** (-np.arange(quarter, dtype=np.float32) / np.float32(quarter))).astype(np.float32)
    grid_row = (pos // GRID_W).astype(np.float32)
    grid_col = (pos % GRID_W).astype(np.float32)
    angles = np.concatenate([grid_row[:, None] * inverse, grid_col[:, None] * inverse], axis=-1)
    cosine = np.repeat(np.cos(angles), 2, axis=-1).astype(np.float32)
    sine = np.repeat(np.sin(angles), 2, axis=-1).astype(np.float32)
    sine[:, 0::2] *= -1.0
    return np.stack([cosine, sine])


def fused(
    dims,
    q_hbm,
    k_hbm,
    v_hbm,
    qg_hbm,
    kg_hbm,
    wo_hbm,
    x_hbm,
    ng_hbm,
    rt_hbm,
    lg_hbm,
    wg_hbm,
    wu_hbm,
    wd_hbm,
    rope_hbm,
    mixed_ref,
    eout_ref,
    q_ref,
    k_ref,
    x_ref,
    gains,
    rt_ref,
    lg_ref,
    wo,
    wgu,
    wd,
    rope,
    disp,
    xq,
    gacc,
    uacc,
    hid,
    part,
    rdiag,
    rs,
    back,
    ret,
    kv,
    qrot,
    qship,
    att,
    aship,
    macc,
    mpart,
    mrecv,
    wsem,
    ssem,
    zr,
    axr,
    ayr,
    afr,
    kvr,
    kvm,
    qar,
    rdr,
    rsr,
    br,
    mr,
):
    n_ep, cap, head_dim, kv_here, group = dims
    f32, bf16 = jnp.float32, jnp.bfloat16
    chips = n_ep // 2
    me = lax.axis_index("ep")
    t = lax.axis_index("tp")
    tx = t + 1 - 2 * (t % 2)
    ty = (t + 2) % 4
    td = 3 - t
    z = me // 2
    core = me % 2
    mate = 2 * z + 1 - core
    inner = (z == 1) | (z == 2)
    partner = z + 1 - 2 * (z % 2)
    other = 3 - z
    far_end = 3 - partner
    near = [jnp.where(inner, a, b) for a, b in ((other, partner), (partner, far_end), (far_end, other))]
    half = n_ep // 2
    order = [me, mate]
    for chip in near:
        order += [2 * chip + core, 2 * chip + 1 - core]
    sides_of = [(z, near[0]), (near[1], near[2])]
    turns = [order[:half][::-1], order[half:][::-1]]
    first_to = []
    for chip in (partner, other, far_end):
        first_to += [2 * chip + core, 2 * chip + 1 - core]
    tokens = x_ref.shape[0]
    slab = disp.shape[2]
    rows = n_ep * cap

    width = x_ref.shape[1]
    ends = (0, width, width + head_dim, width + 2 * head_dim)
    ng_ref, kg_ref, qg_ref = [gains.at[:, ends[i] : ends[i + 1]] for i in range(3)]

    def load(i, a, b):
        return pltpu.make_async_copy(a, b, wsem.at[i])

    def loaded(i, ref):
        load(i, ref, ref).wait()

    load(0, x_hbm, x_ref).start()
    load(1, rt_hbm, rt_ref).start()

    barrier = pltpu.get_barrier_semaphore()
    for d in range(1, n_ep):
        pl.semaphore_signal(barrier, inc=1, device_id={"ep": (me + d) % n_ep}, device_id_type=MESH)
    for peer in (tx, ty, td):
        pl.semaphore_signal(barrier, inc=1, device_id={"tp": peer}, device_id_type=MESH)
    load(2, ng_hbm, ng_ref).start()
    load(2, kg_hbm, kg_ref).start()
    load(2, qg_hbm, qg_ref).start()
    load(3, k_hbm, k_ref).start()
    load(4, rope_hbm.at[:, pl.ds(pl.multiple_of(me * tokens, tokens), tokens), :], rope).start()
    for g in range(kv_here):
        load(5, v_hbm.at[:, g * head_dim : (g + 1) * head_dim], kv.at[g, core, z, 1]).start()
    load(6, q_hbm, q_ref).start()
    load(7, lg_hbm, lg_ref).start()
    load(8, wg_hbm.at[0], wgu.at[0]).start()
    load(8, wu_hbm.at[0], wgu.at[1]).start()
    load(9, wd_hbm.at[0], wd).start()
    load(10, wo_hbm, wo).start()

    loaded(1, rt_ref)
    wide = (tokens, tokens)
    lane = lax.broadcasted_iota(jnp.int32, wide, 1)
    sub = lax.broadcasted_iota(jnp.int32, wide, 0)
    routed = (sub == rt_ref[0:1, :]) | (sub == rt_ref[1:2, :])
    named_t = jnp.where(routed, 1.0, 0.0)
    upper = jnp.where(sub < lane, 1.0, 0.0).astype(bf16)
    rank_t = jnp.dot(named_t.astype(bf16), upper, preferred_element_type=f32)
    slot_iota = lax.broadcasted_iota(jnp.int32, (cap, tokens), 0).astype(f32)
    picks = [
        jnp.where((slot_iota == rank_t[e : e + 1, :]) & (named_t[e : e + 1, :] > 0.5), 1.0, 0.0)
        for e in range(n_ep)
    ]
    pick = jnp.concatenate(picks, axis=0).astype(bf16)

    loaded(2, gains)
    loaded(0, x_ref)
    x = x_ref[...].astype(f32)
    inv = lax.rsqrt(jnp.mean(x * x, axis=-1, keepdims=True) + 1e-06)
    cols = pl.ds(pl.multiple_of(t * slab, slab), slab)
    normed = (x_ref[:, cols].astype(f32) * inv * ng_ref[:, cols]).astype(bf16)
    sent = jnp.dot(pick, normed, preferred_element_type=f32)
    for e in range(n_ep):
        disp[e] = sent[e * cap : (e + 1) * cap].astype(bf16)
    xq[t, me] = disp[me]

    pl.semaphore_wait(barrier, n_ep - 1 + 3)

    def remote(a, b, s, r, **where):
        return pltpu.make_async_remote_copy(
            src_ref=a, dst_ref=b, send_sem=s, recv_sem=r, device_id=where, device_id_type=MESH
        )

    def wait_in(ref, sem):
        remote(ref, ref, ssem.at[0], sem, tp=tx).wait_recv()

    def wait_out(ref, sem):
        remote(ref, ref, sem, zr.at[0], tp=tx).wait_send()

    for e, i in zip([mate] + first_to, range(n_ep - 1)):
        remote(disp.at[e], xq.at[t, me], ssem.at[0], zr.at[i], ep=e).start()

    def spread(i):
        s = order[i]
        rest = half + i // half
        at_x, at_y = (i // 2, rest) if i % 2 == 0 else (rest, i // 2)
        remote(xq.at[t, s], xq.at[t, s], ssem.at[1], axr.at[at_x], tp=tx).start()
        remote(xq.at[t, s], xq.at[t, s], ssem.at[1], ayr.at[at_y], tp=ty).start()

    def forward(i):
        s = order[i]
        if i % 2 == 0:
            wait_in(xq.at[tx, s], axr.at[i // 2])
            remote(xq.at[tx, s], xq.at[tx, s], ssem.at[1], afr.at[i // half], tp=ty).start()
        else:
            wait_in(xq.at[ty, s], ayr.at[i // 2])
            remote(xq.at[ty, s], xq.at[ty, s], ssem.at[1], afr.at[i // half], tp=tx).start()

    spread(0)

    loaded(4, rope)
    cos = rope[0]
    sin = rope[1]
    even = lax.broadcasted_iota(jnp.int32, (tokens, head_dim), 1) % 2 == 0

    def turn(piece, gain):
        a = piece.astype(f32)
        y = a * lax.rsqrt(jnp.mean(a * a, axis=-1, keepdims=True) + 1e-06) * gain
        other = jnp.where(even, pltpu.roll(y, head_dim - 1, 1), pltpu.roll(y, 1, 1))
        return (y * cos + other * sin).astype(bf16)

    loaded(3, k_ref)
    for g in range(kv_here):
        kv[g, core, z, 0] = turn(k_ref[:, g * head_dim : (g + 1) * head_dim], kg_ref[...])

    def kv_send(g, chip, to, kind):
        block = kv.at[g, core, chip]
        remote(block, block, ssem.at[3], kvr.at[g, kind], ep=2 * to + core).start()

    def kv_mate(g, chip):
        block = kv.at[g, core, chip]
        remote(block, block, ssem.at[2], kvm.at[g], ep=mate).start()

    loaded(5, kv.at[0, 0, pl.ds(0, kv_here // 2)])

    def receive(i):
        kind = 0
        if i > 1:
            for_inner, for_end = ((3, 1), (4, 2), (1, 5), (2, 6), (5, 3), (6, 4))[i - 2]
            kind = jnp.where(inner, for_inner, for_end)
        wait_in(xq.at[t, order[i]], zr.at[kind])
        spread(i)

    receive(1)
    loaded(6, q_ref)
    for h in range(kv_here * group):
        qrot[h] = turn(q_ref[:, h * head_dim : (h + 1) * head_dim], qg_ref[...])
    q_of = lambda g: qrot.at[pl.ds(g * group, group)]

    def gate_up(q, k, first=False):
        pieces = [xq[q, pl.ds(2 * chip, 2)].astype(f32).reshape(2 * cap, slab) for chip in sides_of[k]]
        block = jnp.concatenate(pieces, axis=0).astype(bf16)
        at = pl.ds(pl.multiple_of(q * slab, slab), slab)
        g = lax.dot_general(block, wgu[0, :, at], (((1,), (1,)), ((), ())), preferred_element_type=f32)
        u = lax.dot_general(block, wgu[1, :, at], (((1,), (1,)), ((), ())), preferred_element_type=f32)
        if first:
            gacc[k] = g
            uacc[k] = u
        else:
            gacc[k] += g
            uacc[k] += u

    def sides(k):
        wait_in(xq.at[tx, pl.ds(0, half // 2)], axr.at[half + k])
        wait_in(xq.at[ty, pl.ds(0, half // 2)], ayr.at[half + k])

    def corner(k):
        wait_in(xq.at[td, pl.ds(0, half)], afr.at[k])

    def activate(k):
        gate = gacc[k]
        hid[k] = (gate / (1.0 + jnp.exp(-gate)) * uacc[k]).astype(bf16)

    def down(q, k):
        at = pl.ds(pl.multiple_of(q * slab, slab), slab)
        out = jnp.dot(hid[k], wd[:, at], preferred_element_type=f32)
        for s in range(half):
            part[q, 2 * sides_of[k][s // 2] + s % 2] = out[s * cap : (s + 1) * cap].astype(bf16)

    def rx_copy(k, j):
        s = turns[k][j]
        remote(part.at[tx, s], rs.at[0, s], ssem.at[6], rsr.at[k, j // 2], tp=tx).start()

    def ry_copy(k, j):
        s = turns[k][j]
        remote(part.at[ty, s], rs.at[1, s], ssem.at[6], rsr.at[k, j // 2], tp=ty).start()

    def send_far(k):
        for j, s in enumerate(turns[k]):
            to = tx if j % 2 == 0 else ty
            remote(part.at[td, s], rdiag.at[s], ssem.at[6], rdr.at[k, j // 2], tp=to).start()

    def send_near(k):
        for j in range(0, half, 2):
            rx_copy(k, j)
            ry_copy(k, j + 1)

    def corner_far(k):
        corner(k)
        gate_up(td, k)
        activate(k)
        down(td, k)

    def down_rest(k):
        down(tx, k)
        down(ty, k)
        down(t, k)

    receive(2)
    receive(3)

    @pl.when(~inner)
    def _():
        for g in range(kv_here):
            kv_send(g, z, partner, 0)
        for g in range(kv_here):
            remote(q_of(g), qship.at[g], ssem.at[3], qar.at[g], ep=2 * partner + core).start()

    forward(0)
    forward(1)

    loaded(8, wgu)

    @pl.when(~inner)
    def _():
        forward(2)
        forward(3)
        gate_up(t, 0, True)

    receive(4)
    receive(5)

    @pl.when(inner)
    def _():
        kv_send(0, z, other, 1)
        kv_mate(0, z)
        gate_up(t, 0, True)
        forward(2)
        forward(3)

    receive(6)
    receive(7)

    def own_kv(heads):
        @pl.when(inner)
        def _():
            for g in heads:
                kv_send(g, z, other, 1)
                kv_mate(g, z)

    def relay_kv(heads, source, kind):
        @pl.when(inner)
        def _():
            for g in heads:
                block = kv.at[g, core, source]
                wait_in(block, kvr.at[g, kind])
                if kind == 0:
                    kv_send(g, source, other, 2)
                kv_mate(g, source)

    own_kv((1,))
    scale = head_dim ** (-0.5) * 1.4426950408889634

    def attend_one(g, q2):
        keys = kv[g, :, :, 0].reshape(n_ep * tokens, head_dim)
        vals = kv[g, :, :, 1].reshape(n_ep * tokens, head_dim)
        q2 = q2.reshape(group * tokens, head_dim)
        s = lax.dot_general(q2, keys, (((1,), (1,)), ((), ())), preferred_element_type=f32)
        peak = jnp.max(s, axis=-1, keepdims=True)
        p = jnp.exp2((s - peak) * scale)
        total = jnp.sum(p, axis=-1, keepdims=True)
        out = jnp.dot(p.astype(bf16), vals, preferred_element_type=f32) / total
        return jnp.concatenate([out[r * tokens : (r + 1) * tokens] for r in range(group)], axis=1).astype(bf16)

    def attend_ship(heads):
        @pl.when(inner)
        def _():
            for g in heads:
                wait_in(qship.at[g], qar.at[g])
                wait_in(kv.at[g, 1 - core], kvm.at[g])
                aship[g] = attend_one(g, qship[g])
                remote(aship.at[g], att.at[g], ssem.at[3], qar.at[kv_here - 1 if g == kv_here - 1 else 0], ep=2 * partner + core).start()

    def meet(k):
        for j, s in enumerate(turns[k]):
            if j % 2 == 0:
                wait_in(rdiag.at[pl.ds(0, 2)], rdr.at[k, j // 2])
                part[ty, s] = (part[ty, s].astype(f32) + rdiag[s].astype(f32)).astype(bf16)
                ry_copy(k, j)
            else:
                part[tx, s] = (part[tx, s].astype(f32) + rdiag[s].astype(f32)).astype(bf16)
                rx_copy(k, j)

    def finish(k):
        for j, s in enumerate(turns[k]):
            if j % 2 == 0:
                wait_in(rs.at[0, pl.ds(0, 4)], rsr.at[k, j // 2])
            out = (part[t, s].astype(f32) + rs[0, s].astype(f32) + rs[1, s].astype(f32)).astype(bf16)
            if k == 0 and j == half - 1:
                ret[s] = out
            else:
                back[s] = out
                remote(back.at[s], ret.at[me], ssem.at[7], br.at[0], ep=s).start()

    share = tokens // 4
    chunk = width // 4

    loaded(9, wd)
    sides(0)
    gate_up(tx, 0)
    gate_up(ty, 0)

    @pl.when(~inner)
    def _():
        corner_far(0)
        down_rest(0)
        send_far(0)

    forward(4)
    forward(5)
    relay_kv((0,), partner, 0)
    own_kv((2,))

    @pl.when(inner)
    def _():
        corner_far(0)
        send_far(0)

    forward(6)
    forward(7)
    relay_kv((1,), partner, 0)
    own_kv((3,))
    relay_kv((0, 1), other, 1)

    @pl.when(inner)
    def _():
        down_rest(0)

    send_near(0)
    relay_kv((2, 3), partner, 0)
    relay_kv((0,), far_end, 2)
    gate_up(t, 1, True)
    sides(1)
    gate_up(tx, 1)
    gate_up(ty, 1)
    meet(0)
    attend_ship((0,))
    relay_kv((2,), other, 1)
    relay_kv((1,), far_end, 2)
    corner_far(1)
    send_far(1)
    down_rest(1)
    send_near(1)
    attend_ship((1,))
    relay_kv((3,), other, 1)
    relay_kv((2,), far_end, 2)
    relay_kv((3,), far_end, 2)
    attend_ship((2, 3))
    finish(0)
    meet(1)

    @pl.when(inner)
    def _():
        for g in range(kv_here):
            att[g] = attend_one(g, qrot[g * group : (g + 1) * group])


    @pl.when(inner)
    def _():
        finish(1)


    def attended(first, count, i):
        @pl.when(~inner)
        def _():
            wait_in(att.at[pl.ds(first, count)], qar.at[i])

    attended(0, kv_here - 1, 0)
    loaded(10, wo)
    cut = (kv_here - 1) * group * head_dim
    early = jnp.concatenate([att[g] for g in range(kv_here - 1)], axis=1)
    macc[...] = jnp.dot(early, wo[:cut, :], preferred_element_type=f32)
    attended(kv_here - 1, 1, kv_here - 1)
    for c in range(4):
        at = slice(c * chunk, (c + 1) * chunk)
        out = macc[:, at] + jnp.dot(att[kv_here - 1], wo[cut:, at], preferred_element_type=f32)
        for j in range(4):
            mpart[c, j] = out[j * share : (j + 1) * share].astype(bf16)
        for i, to in enumerate((td, tx, ty)):
            remote(mpart.at[c, to], mrecv.at[c, i], ssem.at[5], mr.at[c], tp=to).start()

    @pl.when(~inner)
    def _():
        finish(1)

    loaded(7, lg_ref)
    ids = rt_ref[...].astype(f32)
    logits = lg_ref[...]
    stacked = jnp.where(
        sub == 0,
        ids[0:1, :],
        jnp.where(sub == 1, ids[1:2, :], jnp.where(sub == 2, logits[0:1, :], logits[1:2, :])),
    )
    columns = stacked.T
    r0 = columns[:, 0:1].astype(jnp.int32)
    r1 = columns[:, 1:2].astype(jnp.int32)
    lower = jnp.where(lane < sub, 1.0, 0.0).astype(bf16)
    rank = jnp.dot(lower, named_t.T.astype(bf16), preferred_element_type=f32)
    total_lane = lax.broadcasted_iota(jnp.int32, (tokens, rows), 1)

    def chosen(r):
        slot = jnp.sum(jnp.where(lane == r, rank, 0.0), axis=-1, keepdims=True)
        target = r * cap + slot.astype(jnp.int32)
        return jnp.where(total_lane == target, 1.0, 0.0).astype(bf16)

    c0 = chosen(r0)
    c1 = chosen(r1)
    l0 = columns[:, 2:3]
    l1 = columns[:, 3:4]
    w0 = jax.nn.sigmoid(l0 - l1)
    w1 = jax.nn.sigmoid(l1 - l0)
    wait_in(ret.at[pl.ds(0, n_ep - 1)], br.at[0])
    results = ret[...].astype(f32).reshape(rows, slab).astype(bf16)
    first = jnp.dot(c0, results, preferred_element_type=f32)
    second = jnp.dot(c1, results, preferred_element_type=f32)
    eout_ref[...] = (w0 * first + w1 * second).astype(bf16)
    for c in range(4):
        wait_in(mrecv.at[c], mr.at[c])
        summed = mpart[c, t].astype(f32)
        for i in range(3):
            summed = summed + mrecv[c, i].astype(f32)
        mixed_ref[:, c * chunk : (c + 1) * chunk] = summed.astype(bf16)

    wait_out(disp.at[pl.ds(0, n_ep - 1)], ssem.at[0])
    wait_out(xq.at[pl.ds(0, 3)], ssem.at[1])

    @pl.when(inner)
    def _():
        wait_out(kv.at[:, 0], ssem.at[2])
        wait_out(kv.at[pl.ds(0, 3), 0], ssem.at[3])

    @pl.when(~inner)
    def _():
        wait_out(kv.at[pl.ds(0, 2), 0], ssem.at[3])

    wait_out(mrecv, ssem.at[5])
    wait_out(part.at[pl.ds(0, 3)], ssem.at[6])
    wait_out(back.at[pl.ds(0, n_ep - 1)], ssem.at[7])


def hand_over(a_ref, b_ref, a_out, b_out, sem):
    one = pltpu.make_async_copy(a_ref, a_out, sem.at[0])
    two = pltpu.make_async_copy(b_ref, b_out, sem.at[1])
    one.start()
    two.start()
    one.wait()
    two.wait()


def kernel_form(
    queries,
    keys,
    values,
    query_gain,
    key_gain,
    out_weight,
    expert_input,
    norm_gain,
    routes,
    route_logits,
    gate_weight,
    up_weight,
    down_weight,
):
    bf16, f32 = jnp.bfloat16, jnp.float32
    n_ep = lax.axis_size("ep")
    tokens = queries.shape[0]
    head_dim = query_gain.shape[0]
    heads = queries.shape[1] // head_dim
    kv_here = keys.shape[1] // head_dim
    width = expert_input.shape[1]
    n_tp = lax.axis_size("tp")
    slab = width // n_tp
    cap = tokens * routes.shape[1] // n_ep * 5 // 4
    rows = n_ep * cap
    ff = gate_weight.shape[2]
    share = tokens // n_tp
    chunk = out_weight.shape[1] // 4
    table = jnp.asarray(rope_constants(tokens * n_ep, head_dim))
    vmem = pl.BlockSpec(memory_space=pltpu.VMEM)
    hbm = pl.BlockSpec(memory_space=pl.ANY)
    piece = (n_ep, cap, slab)
    dma = pltpu.SemaphoreType.DMA
    dims = (n_ep, cap, head_dim, kv_here, heads // kv_here)
    outs = pl.pallas_call(
        functools.partial(fused, dims),
        name="fused",
        out_shape=(
            pltpu.VMEM((share, out_weight.shape[1]), bf16),
            pltpu.VMEM((tokens, slab), bf16),
        ),
        in_specs=[hbm] * 14,
        out_specs=(vmem, vmem),
        scratch_shapes=[
            pltpu.VMEM(queries.shape, bf16),
            pltpu.VMEM(keys.shape, bf16),
            pltpu.VMEM(expert_input.shape, bf16),
            pltpu.VMEM((1, width + 2 * head_dim), f32),
            pltpu.VMEM((2, tokens), jnp.int32),
            pltpu.VMEM((2, tokens), f32),
            pltpu.VMEM(out_weight.shape, bf16),
            pltpu.VMEM((2, ff, width), bf16),
            pltpu.VMEM(down_weight.shape[1:], bf16),
            pltpu.VMEM((2, tokens, head_dim), f32),
            pltpu.VMEM(piece, bf16),
            pltpu.VMEM((n_tp,) + piece, bf16),
            pltpu.VMEM((2, rows // 2, ff), f32),
            pltpu.VMEM((2, rows // 2, ff), f32),
            pltpu.VMEM((2, rows // 2, ff), bf16),
            pltpu.VMEM((n_tp,) + piece, bf16),
            pltpu.VMEM(piece, bf16),
            pltpu.VMEM((2,) + piece, bf16),
            pltpu.VMEM(piece, bf16),
            pltpu.VMEM(piece, bf16),
            pltpu.VMEM((kv_here, 2, n_ep // 2, 2, tokens, head_dim), bf16),
            pltpu.VMEM((heads, tokens, head_dim), bf16),
            pltpu.VMEM((kv_here, heads // kv_here, tokens, head_dim), bf16),
            pltpu.VMEM((kv_here, tokens, heads // kv_here * head_dim), bf16),
            pltpu.VMEM((kv_here, tokens, heads // kv_here * head_dim), bf16),
            pltpu.VMEM((tokens, width), f32),
            pltpu.VMEM((4, n_tp, share, chunk), bf16),
            pltpu.VMEM((4, 3, share, chunk), bf16),
            dma((11,)),
            dma((8,)),
            dma((7,)),
            dma((n_ep // 2 + 2,)),
            dma((n_ep // 2 + 2,)),
            dma((2,)),
            dma((kv_here, 3)),
            dma((kv_here,)),
            dma((kv_here,)),
            dma((2, 2)),
            dma((2, 2)),
            dma((1,)),
            dma((4,)),
        ],
        compiler_params=pltpu.CompilerParams(
            collective_id=0, has_side_effects=True, vmem_limit_bytes=60 * 1024 * 1024
        ),
    )(
        queries,
        keys,
        values,
        query_gain.reshape(1, -1),
        key_gain.reshape(1, -1),
        out_weight,
        expert_input,
        norm_gain.reshape(1, -1),
        routes.T,
        route_logits.T,
        jnp.swapaxes(gate_weight, 1, 2),
        jnp.swapaxes(up_weight, 1, 2),
        down_weight,
        table,
    )
    return pl.pallas_call(
        hand_over,
        name="hand_over",
        out_shape=tuple(jax.ShapeDtypeStruct(o.shape, o.dtype) for o in outs),
        in_specs=[vmem, vmem],
        out_specs=(hbm, hbm),
        scratch_shapes=[dma((2,))],
    )(*(pltpu.with_memory_space_constraint(o, pltpu.VMEM) for o in outs))


def dispatch_form(mesh, *args):
    queries, routes = args[0], args[8]
    tokens = queries.shape[0]
    n_ep, n_tp = mesh.shape["ep"], mesh.shape["tp"]
    cap = tokens * routes.shape[1] // n_ep * 5 // 4
    same = args[6].shape[0] == tokens and tokens % 128 == 0
    fits = n_tp == 4 and n_ep == 8 and cap % 8 == 0
    if same and fits and routes.shape[1] == 2 and tokens == 128:
        return kernel_form(*args)
    return local(*args)


def solution(mesh):
    placed = (
        P("ep", "tp"),
        P("ep", "tp"),
        P("ep", "tp"),
        P(),
        P(),
        P("tp", None),
        P("ep", None),
        P(),
        P("ep", None),
        P("ep", None),
        P("ep", None, "tp"),
        P("ep", None, "tp"),
        P("ep", "tp", None),
    )
    return jax.shard_map(
        functools.partial(dispatch_form, mesh),
        mesh=mesh,
        in_specs=placed,
        out_specs=(P(("ep", "tp"), None), P("ep", "tp")),
        check_vma=False,
    )
```

```python
import functools
import jax
import jax.numpy as jnp
import numpy as np
from jax import lax
from jax.experimental import pallas as pl
from jax.experimental.pallas import tpu as pltpu
from jax.sharding import PartitionSpec as P

GRID_W = 64


def rope_tables(count, offset, head_dim):
    pos = offset + lax.iota(jnp.int32, count)
    grid_row = (pos // GRID_W).astype(jnp.float32)
    grid_col = (pos % GRID_W).astype(jnp.float32)
    quarter = head_dim // 4
    inverse = 10000.0 ** (-jnp.arange(quarter, dtype=jnp.float32) / quarter)
    angles = jnp.concatenate([grid_row[:, None] * inverse, grid_col[:, None] * inverse], axis=-1)
    return (jnp.cos(angles), jnp.sin(angles))


def norm_rotate(x, gain, cosine, sine):
    count, number, head_dim = x.shape
    y = x * lax.rsqrt(jnp.mean(x * x, axis=-1, keepdims=True) + 1e-06) * gain
    pairs = y.reshape(count, number, head_dim // 2, 2)
    first, second = (pairs[..., 0], pairs[..., 1])
    cos_b = cosine[:, None, :]
    sin_b = sine[:, None, :]
    turned = jnp.stack([first * cos_b - second * sin_b, first * sin_b + second * cos_b], axis=-1)
    return turned.reshape(count, number, head_dim).astype(jnp.bfloat16)


def key_block_size(length, shard_rows):
    if length <= 2048:
        return length
    shards = length // shard_rows
    most = max(1, 2048 // shard_rows)
    best = 1
    for count in range(1, most + 1):
        if shards % count == 0:
            best = count
    return best * shard_rows


def local(
    queries,
    keys,
    values,
    query_gain,
    key_gain,
    out_weight,
    expert_input,
    norm_gain,
    routes,
    route_logits,
    gate_weight,
    up_weight,
    down_weight,
):
    tokens_here = queries.shape[0]
    head_dim = query_gain.shape[0]
    heads_here = queries.shape[1] // head_dim
    kv_here = keys.shape[1] // head_dim
    group = heads_here // kv_here
    offset = lax.axis_index("ep") * tokens_here
    cosine, sine = rope_tables(tokens_here, offset, head_dim)
    q_rot = norm_rotate(
        queries.astype(jnp.float32).reshape(tokens_here, heads_here, head_dim),
        query_gain,
        cosine,
        sine,
    )
    k_rot = norm_rotate(
        keys.astype(jnp.float32).reshape(tokens_here, kv_here, head_dim), key_gain, cosine, sine
    ).reshape(tokens_here, kv_here * head_dim)
    q_grouped = q_rot.reshape(tokens_here, kv_here, group, head_dim).transpose(1, 2, 0, 3)
    q_grouped = q_grouped.reshape(kv_here, group * tokens_here, head_dim)
    query_rows = group * tokens_here
    scale = head_dim ** (-0.5)
    start_state = (
        jnp.full((kv_here, query_rows), -1e30, jnp.float32),
        jnp.zeros((kv_here, query_rows), jnp.float32),
        jnp.zeros((kv_here, query_rows, head_dim), jnp.float32),
    )
    key_piece = lax.all_gather(k_rot, "ep", axis=0, tiled=True)
    value_piece = lax.all_gather(values, "ep", axis=0, tiled=True)
    length = key_piece.shape[0]
    block = key_block_size(length, tokens_here)
    key_blocks = key_piece.reshape(length // block, block, kv_here, head_dim)
    value_blocks = value_piece.reshape(length // block, block, kv_here, head_dim)

    def step(state, blocks):
        running_max, running_total, running_sum = state
        key_block, value_block = blocks
        scores = (
            jnp.einsum("kqd,lkd->kql", q_grouped, key_block, preferred_element_type=jnp.float32)
            * scale
        )
        new_max = jnp.maximum(running_max, jnp.max(scores, axis=-1))
        factor = jnp.exp(running_max - new_max)
        weights = jnp.exp(scores - new_max[..., None])
        new_total = running_total * factor + jnp.sum(weights, axis=-1)
        new_sum = running_sum * factor[..., None] + jnp.einsum(
            "kql,lkd->kqd",
            weights.astype(jnp.bfloat16),
            value_block,
            preferred_element_type=jnp.float32,
        )
        return ((new_max, new_total, new_sum), None)

    result, _ = lax.scan(step, start_state, (key_blocks, value_blocks))
    final_max, final_total, final_sum = result
    attended = (final_sum / final_total[..., None]).astype(jnp.bfloat16)
    attended = attended.reshape(kv_here, group, tokens_here, head_dim).transpose(2, 0, 1, 3)
    attended = attended.reshape(tokens_here, heads_here * head_dim)
    summed = lax.psum_scatter(
        jnp.dot(attended, out_weight, preferred_element_type=jnp.float32).astype(jnp.bfloat16),
        "tp",
        scatter_dimension=0,
        tiled=True,
    ).astype(jnp.float32)
    mixed = summed.astype(jnp.bfloat16)
    expert_tokens_here, width = expert_input.shape
    n_ep = lax.axis_size("ep")
    top = routes.shape[1]
    capacity = expert_tokens_here * top // n_ep * 5 // 4
    x = expert_input.astype(jnp.float32)
    normed = (x * lax.rsqrt(jnp.mean(x * x, axis=-1, keepdims=True) + 1e-06) * norm_gain).astype(
        jnp.bfloat16
    )
    expert_ids = routes.reshape(-1)
    onehot = (expert_ids[:, None] == lax.iota(jnp.int32, n_ep)[None, :]).astype(jnp.int32)
    before = jnp.cumsum(onehot, axis=0) - onehot
    slot = jnp.sum(before * onehot, axis=1)
    target = expert_ids * capacity + slot
    owner_row = lax.iota(jnp.int32, expert_tokens_here * top) // top
    w_gate = gate_weight[0]
    w_up = up_weight[0]
    w_down = down_weight[0]
    columns = normed.shape[1]
    filled = jnp.zeros((n_ep * capacity, columns), jnp.bfloat16).at[target].set(normed[owner_row])
    arrived = lax.all_to_all(
        filled.reshape(n_ep, capacity, columns), "ep", split_axis=0, concat_axis=0, tiled=True
    )
    sources, slots, work_columns = arrived.shape
    flat = arrived.reshape(sources * slots, work_columns)
    gate = jnp.dot(flat, w_gate, preferred_element_type=jnp.float32)
    upper = jnp.dot(flat, w_up, preferred_element_type=jnp.float32)
    hidden = (jax.nn.silu(gate) * upper).astype(jnp.bfloat16)
    partial_out = jnp.dot(hidden, w_down, preferred_element_type=jnp.float32)
    summed = lax.psum_scatter(
        partial_out.reshape(sources, slots, width).astype(jnp.bfloat16),
        "tp",
        scatter_dimension=2,
        tiled=True,
    ).astype(jnp.float32)
    returned = lax.all_to_all(
        summed.astype(jnp.bfloat16), "ep", split_axis=0, concat_axis=0, tiled=True
    )
    picked = returned.reshape(n_ep * capacity, -1)[target].reshape(expert_tokens_here, top, -1)
    route_weight = jax.nn.sigmoid(route_logits - route_logits[:, ::-1])
    combined = jnp.sum(route_weight[..., None] * picked.astype(jnp.float32), axis=1)
    expert_out = combined.astype(jnp.bfloat16)
    return (mixed, expert_out)


MESH = pl.DeviceIdType.MESH


def rope_constants(length, head_dim):
    pos = np.arange(length)
    quarter = head_dim // 4
    inverse = (np.float32(10000.0) ** (-np.arange(quarter, dtype=np.float32) / np.float32(quarter))).astype(np.float32)
    grid_row = (pos // GRID_W).astype(np.float32)
    grid_col = (pos % GRID_W).astype(np.float32)
    angles = np.concatenate([grid_row[:, None] * inverse, grid_col[:, None] * inverse], axis=-1)
    cosine = np.repeat(np.cos(angles), 2, axis=-1).astype(np.float32)
    sine = np.repeat(np.sin(angles), 2, axis=-1).astype(np.float32)
    sine[:, 0::2] *= -1.0
    return np.stack([cosine, sine])


def fused(
    dims,
    q_hbm,
    k_hbm,
    v_hbm,
    qg_hbm,
    kg_hbm,
    wo_hbm,
    x_hbm,
    ng_hbm,
    rt_hbm,
    lg_hbm,
    wg_hbm,
    wu_hbm,
    wd_hbm,
    rope_hbm,
    mixed_ref,
    eout_ref,
    q_ref,
    k_ref,
    x_ref,
    gains,
    rt_ref,
    lg_ref,
    wo,
    wgu,
    wd,
    rope,
    disp,
    xq,
    gacc,
    uacc,
    hid,
    part,
    rdiag,
    rs,
    back,
    ret,
    kv,
    qrot,
    qship,
    att,
    aship,
    macc,
    mpart,
    mfar,
    mrecv,
    wsem,
    ssem,
    zr,
    axr,
    ayr,
    afr,
    kvr,
    kvm,
    qar,
    rdr,
    rsr,
    br,
    mf,
    mr,
):
    n_ep, cap, head_dim, kv_here, group = dims
    f32, bf16 = jnp.float32, jnp.bfloat16
    chips = n_ep // 2
    me = lax.axis_index("ep")
    t = lax.axis_index("tp")
    tx = t + 1 - 2 * (t % 2)
    ty = (t + 2) % 4
    td = 3 - t
    z = me // 2
    core = me % 2
    mate = 2 * z + 1 - core
    inner = (z == 1) | (z == 2)
    partner = z + 1 - 2 * (z % 2)
    other = 3 - z
    far_end = 3 - partner
    near = [jnp.where(inner, a, b) for a, b in ((other, partner), (partner, far_end), (far_end, other))]
    half = n_ep // 2
    order = [me, mate]
    for chip in near:
        order += [2 * chip + core, 2 * chip + 1 - core]
    sides_of = [(z, near[0]), (near[1], near[2])]
    turns = [order[:half][::-1], order[half:][::-1]]
    first_to = []
    for chip in (partner, other, far_end):
        first_to += [2 * chip + core, 2 * chip + 1 - core]
    tokens = x_ref.shape[0]
    slab = disp.shape[2]
    rows = n_ep * cap

    width = x_ref.shape[1]
    ends = (0, width, width + head_dim, width + 2 * head_dim)
    ng_ref, kg_ref, qg_ref = [gains.at[:, ends[i] : ends[i + 1]] for i in range(3)]

    def load(i, a, b):
        return pltpu.make_async_copy(a, b, wsem.at[i])

    def loaded(i, ref):
        load(i, ref, ref).wait()

    load(0, x_hbm, x_ref).start()
    load(1, rt_hbm, rt_ref).start()

    barrier = pltpu.get_barrier_semaphore()
    for d in range(1, n_ep):
        pl.semaphore_signal(barrier, inc=1, device_id={"ep": (me + d) % n_ep}, device_id_type=MESH)
    for peer in (tx, ty, td):
        pl.semaphore_signal(barrier, inc=1, device_id={"tp": peer}, device_id_type=MESH)
    load(2, ng_hbm, ng_ref).start()
    load(2, kg_hbm, kg_ref).start()
    load(2, qg_hbm, qg_ref).start()
    load(3, k_hbm, k_ref).start()
    load(4, rope_hbm.at[:, pl.ds(pl.multiple_of(me * tokens, tokens), tokens), :], rope).start()
    for g in range(kv_here):
        load(5, v_hbm.at[:, g * head_dim : (g + 1) * head_dim], kv.at[g, core, z, 1]).start()
    load(6, q_hbm, q_ref).start()
    load(7, lg_hbm, lg_ref).start()
    load(8, wg_hbm.at[0], wgu.at[0]).start()
    load(8, wu_hbm.at[0], wgu.at[1]).start()
    load(9, wd_hbm.at[0], wd).start()
    load(10, wo_hbm, wo).start()

    loaded(1, rt_ref)
    wide = (tokens, tokens)
    lane = lax.broadcasted_iota(jnp.int32, wide, 1)
    sub = lax.broadcasted_iota(jnp.int32, wide, 0)
    routed = (sub == rt_ref[0:1, :]) | (sub == rt_ref[1:2, :])
    named_t = jnp.where(routed, 1.0, 0.0)
    upper = jnp.where(sub < lane, 1.0, 0.0).astype(bf16)
    rank_t = jnp.dot(named_t.astype(bf16), upper, preferred_element_type=f32)
    slot_iota = lax.broadcasted_iota(jnp.int32, (cap, tokens), 0).astype(f32)
    picks = [
        jnp.where((slot_iota == rank_t[e : e + 1, :]) & (named_t[e : e + 1, :] > 0.5), 1.0, 0.0)
        for e in range(n_ep)
    ]
    pick = jnp.concatenate(picks, axis=0).astype(bf16)

    loaded(2, gains)
    loaded(0, x_ref)
    x = x_ref[...].astype(f32)
    inv = lax.rsqrt(jnp.mean(x * x, axis=-1, keepdims=True) + 1e-06)
    cols = pl.ds(pl.multiple_of(t * slab, slab), slab)
    normed = (x_ref[:, cols].astype(f32) * inv * ng_ref[:, cols]).astype(bf16)
    sent = jnp.dot(pick, normed, preferred_element_type=f32)
    for e in range(n_ep):
        disp[e] = sent[e * cap : (e + 1) * cap].astype(bf16)
    xq[t, me] = disp[me]

    pl.semaphore_wait(barrier, n_ep - 1 + 3)

    def remote(a, b, s, r, **where):
        return pltpu.make_async_remote_copy(
            src_ref=a, dst_ref=b, send_sem=s, recv_sem=r, device_id=where, device_id_type=MESH
        )

    def wait_in(ref, sem):
        remote(ref, ref, ssem.at[0], sem, tp=tx).wait_recv()

    def wait_out(ref, sem):
        remote(ref, ref, sem, zr.at[0], tp=tx).wait_send()

    for e, i in zip([mate] + first_to, range(n_ep - 1)):
        remote(disp.at[e], xq.at[t, me], ssem.at[0], zr.at[i], ep=e).start()

    def spread(i):
        s = order[i]
        rest = half + i // half
        at_x, at_y = (i // 2, rest) if i % 2 == 0 else (rest, i // 2)
        remote(xq.at[t, s], xq.at[t, s], ssem.at[1], axr.at[at_x], tp=tx).start()
        remote(xq.at[t, s], xq.at[t, s], ssem.at[1], ayr.at[at_y], tp=ty).start()

    def forward(i):
        s = order[i]
        if i % 2 == 0:
            wait_in(xq.at[tx, s], axr.at[i // 2])
            remote(xq.at[tx, s], xq.at[tx, s], ssem.at[1], afr.at[i // half], tp=ty).start()
        else:
            wait_in(xq.at[ty, s], ayr.at[i // 2])
            remote(xq.at[ty, s], xq.at[ty, s], ssem.at[1], afr.at[i // half], tp=tx).start()

    spread(0)

    loaded(4, rope)
    cos = rope[0]
    sin = rope[1]
    even = lax.broadcasted_iota(jnp.int32, (tokens, head_dim), 1) % 2 == 0

    def turn(piece, gain):
        a = piece.astype(f32)
        y = a * lax.rsqrt(jnp.mean(a * a, axis=-1, keepdims=True) + 1e-06) * gain
        other = jnp.where(even, pltpu.roll(y, head_dim - 1, 1), pltpu.roll(y, 1, 1))
        return (y * cos + other * sin).astype(bf16)

    loaded(3, k_ref)
    for g in range(kv_here):
        kv[g, core, z, 0] = turn(k_ref[:, g * head_dim : (g + 1) * head_dim], kg_ref[...])

    def kv_send(g, chip, to, kind):
        block = kv.at[g, core, chip]
        remote(block, block, ssem.at[3], kvr.at[g, kind], ep=2 * to + core).start()

    def kv_mate(g, chip):
        block = kv.at[g, core, chip]
        remote(block, block, ssem.at[2], kvm.at[g], ep=mate).start()

    loaded(5, kv.at[0, 0, pl.ds(0, kv_here // 2)])

    def receive(i):
        kind = 0
        if i > 1:
            for_inner, for_end = ((3, 1), (4, 2), (1, 5), (2, 6), (5, 3), (6, 4))[i - 2]
            kind = jnp.where(inner, for_inner, for_end)
        wait_in(xq.at[t, order[i]], zr.at[kind])
        spread(i)

    receive(1)
    loaded(6, q_ref)
    for h in range(kv_here * group):
        qrot[h] = turn(q_ref[:, h * head_dim : (h + 1) * head_dim], qg_ref[...])
    q_of = lambda g: qrot.at[pl.ds(g * group, group)]

    def gate_up(q, k, first=False):
        pieces = [xq[q, pl.ds(2 * chip, 2)].astype(f32).reshape(2 * cap, slab) for chip in sides_of[k]]
        block = jnp.concatenate(pieces, axis=0).astype(bf16)
        at = pl.ds(pl.multiple_of(q * slab, slab), slab)
        g = lax.dot_general(block, wgu[0, :, at], (((1,), (1,)), ((), ())), preferred_element_type=f32)
        u = lax.dot_general(block, wgu[1, :, at], (((1,), (1,)), ((), ())), preferred_element_type=f32)
        if first:
            gacc[k] = g
            uacc[k] = u
        else:
            gacc[k] += g
            uacc[k] += u

    def sides(k):
        wait_in(xq.at[tx, pl.ds(0, half // 2)], axr.at[half + k])
        wait_in(xq.at[ty, pl.ds(0, half // 2)], ayr.at[half + k])

    def corner(k):
        wait_in(xq.at[td, pl.ds(0, half)], afr.at[k])

    def activate(k):
        gate = gacc[k]
        hid[k] = (gate / (1.0 + jnp.exp(-gate)) * uacc[k]).astype(bf16)

    def down(q, k):
        at = pl.ds(pl.multiple_of(q * slab, slab), slab)
        out = jnp.dot(hid[k], wd[:, at], preferred_element_type=f32)
        for s in range(half):
            part[q, 2 * sides_of[k][s // 2] + s % 2] = out[s * cap : (s + 1) * cap].astype(bf16)

    def rx_copy(k, j):
        s = turns[k][j]
        remote(part.at[tx, s], rs.at[0, s], ssem.at[6], rsr.at[k, j // 2], tp=tx).start()

    def ry_copy(k, j):
        s = turns[k][j]
        remote(part.at[ty, s], rs.at[1, s], ssem.at[6], rsr.at[k, j // 2], tp=ty).start()

    def send_far(k):
        for j, s in enumerate(turns[k]):
            to = tx if j % 2 == 0 else ty
            remote(part.at[td, s], rdiag.at[s], ssem.at[6], rdr.at[k, j // 2], tp=to).start()

    def send_near(k):
        for j in range(0, half, 2):
            rx_copy(k, j)
            ry_copy(k, j + 1)

    def corner_far(k):
        corner(k)
        gate_up(td, k)
        activate(k)
        down(td, k)

    def down_rest(k):
        down(tx, k)
        down(ty, k)
        down(t, k)

    receive(2)
    receive(3)

    @pl.when(~inner)
    def _():
        for g in range(kv_here):
            kv_send(g, z, partner, 0)
        for g in range(kv_here):
            remote(q_of(g), qship.at[g], ssem.at[3], qar.at[g], ep=2 * partner + core).start()

    forward(0)
    forward(1)

    loaded(8, wgu)

    @pl.when(~inner)
    def _():
        forward(2)
        forward(3)
        gate_up(t, 0, True)

    receive(4)
    receive(5)

    @pl.when(inner)
    def _():
        kv_send(0, z, other, 1)
        kv_mate(0, z)
        gate_up(t, 0, True)
        forward(2)
        forward(3)

    receive(6)
    receive(7)

    def own_kv(heads):
        @pl.when(inner)
        def _():
            for g in heads:
                kv_send(g, z, other, 1)
                kv_mate(g, z)

    def relay_kv(heads, source, kind):
        @pl.when(inner)
        def _():
            for g in heads:
                block = kv.at[g, core, source]
                wait_in(block, kvr.at[g, kind])
                if kind == 0:
                    kv_send(g, source, other, 2)
                kv_mate(g, source)

    own_kv((1,))
    scale = head_dim ** (-0.5) * 1.4426950408889634

    def attend_one(g, q2):
        keys = kv[g, :, :, 0].reshape(n_ep * tokens, head_dim)
        vals = kv[g, :, :, 1].reshape(n_ep * tokens, head_dim)
        q2 = q2.reshape(group * tokens, head_dim)
        s = lax.dot_general(q2, keys, (((1,), (1,)), ((), ())), preferred_element_type=f32)
        peak = jnp.max(s, axis=-1, keepdims=True)
        p = jnp.exp2((s - peak) * scale)
        total = jnp.sum(p, axis=-1, keepdims=True)
        out = jnp.dot(p.astype(bf16), vals, preferred_element_type=f32) / total
        return jnp.concatenate([out[r * tokens : (r + 1) * tokens] for r in range(group)], axis=1).astype(bf16)

    def attend_ship(heads):
        @pl.when(inner)
        def _():
            for g in heads:
                wait_in(qship.at[g], qar.at[g])
                wait_in(kv.at[g, 1 - core], kvm.at[g])
                aship[g] = attend_one(g, qship[g])
                remote(aship.at[g], att.at[g], ssem.at[3], qar.at[kv_here - 1 if g == kv_here - 1 else 0], ep=2 * partner + core).start()

    def meet(k):
        for j, s in enumerate(turns[k]):
            if j % 2 == 0:
                wait_in(rdiag.at[pl.ds(0, 2)], rdr.at[k, j // 2])
                part[ty, s] = (part[ty, s].astype(f32) + rdiag[s].astype(f32)).astype(bf16)
                ry_copy(k, j)
            else:
                part[tx, s] = (part[tx, s].astype(f32) + rdiag[s].astype(f32)).astype(bf16)
                rx_copy(k, j)

    def finish(k):
        for j, s in enumerate(turns[k]):
            if j % 2 == 0:
                wait_in(rs.at[0, pl.ds(0, 4)], rsr.at[k, j // 2])
            out = (part[t, s].astype(f32) + rs[0, s].astype(f32) + rs[1, s].astype(f32)).astype(bf16)
            if k == 0 and j == half - 1:
                ret[s] = out
            else:
                back[s] = out
                remote(back.at[s], ret.at[me], ssem.at[7], br.at[0], ep=s).start()

    share = tokens // 4
    chunk = width // 4

    loaded(9, wd)
    sides(0)
    gate_up(tx, 0)
    gate_up(ty, 0)

    @pl.when(~inner)
    def _():
        corner_far(0)
        down_rest(0)
        send_far(0)

    forward(4)
    forward(5)
    relay_kv((0,), partner, 0)
    own_kv((2,))

    @pl.when(inner)
    def _():
        corner_far(0)
        send_far(0)

    forward(6)
    forward(7)
    relay_kv((1,), partner, 0)
    own_kv((3,))
    relay_kv((0, 1), other, 1)

    @pl.when(inner)
    def _():
        down_rest(0)

    send_near(0)
    relay_kv((2, 3), partner, 0)
    relay_kv((0,), far_end, 2)
    gate_up(t, 1, True)
    sides(1)
    gate_up(tx, 1)
    gate_up(ty, 1)
    meet(0)
    attend_ship((0,))
    relay_kv((2,), other, 1)
    relay_kv((1,), far_end, 2)
    corner_far(1)
    send_far(1)
    down_rest(1)
    send_near(1)
    attend_ship((1,))
    relay_kv((3,), other, 1)
    relay_kv((2,), far_end, 2)
    relay_kv((3,), far_end, 2)
    attend_ship((2, 3))
    finish(0)
    meet(1)

    @pl.when(inner)
    def _():
        for g in range(kv_here):
            att[g] = attend_one(g, qrot[g * group : (g + 1) * group])


    @pl.when(inner)
    def _():
        finish(1)


    def attended(first, count, i):
        @pl.when(~inner)
        def _():
            wait_in(att.at[pl.ds(first, count)], qar.at[i])

    attended(0, kv_here - 1, 0)
    loaded(10, wo)
    cut = (kv_here - 1) * group * head_dim
    early = jnp.concatenate([att[g] for g in range(kv_here - 1)], axis=1)
    macc[...] = jnp.dot(early, wo[:cut, :], preferred_element_type=f32)
    attended(kv_here - 1, 1, kv_here - 1)
    def m_send(a, b, sem, to):
        remote(a, b, ssem.at[5], sem, tp=to).start()

    for c in (0, 2, 1, 3):
        at = slice(c * chunk, (c + 1) * chunk)
        out = macc[:, at] + jnp.dot(att[kv_here - 1], wo[cut:, at], preferred_element_type=f32)
        for j in range(4):
            mpart[c, j] = out[j * share : (j + 1) * share].astype(bf16)
        if c % 2 == 0:
            to = tx if c == 0 else ty
            m_send(mpart.at[c, td], mfar.at[c // 2], mf.at[c // 2], to)
            m_send(mpart.at[c, to], mrecv.at[c, c // 2], mr.at[c], to)
        else:
            for i, to in ((2, td), (0, tx), (1, ty)):
                m_send(mpart.at[c, to], mrecv.at[c, i], mr.at[c], to)

    @pl.when(~inner)
    def _():
        finish(1)

    loaded(7, lg_ref)
    ids = rt_ref[...].astype(f32)
    logits = lg_ref[...]
    stacked = jnp.where(
        sub == 0,
        ids[0:1, :],
        jnp.where(sub == 1, ids[1:2, :], jnp.where(sub == 2, logits[0:1, :], logits[1:2, :])),
    )
    columns = stacked.T
    r0 = columns[:, 0:1].astype(jnp.int32)
    r1 = columns[:, 1:2].astype(jnp.int32)
    lower = jnp.where(lane < sub, 1.0, 0.0).astype(bf16)
    rank = jnp.dot(lower, named_t.T.astype(bf16), preferred_element_type=f32)
    total_lane = lax.broadcasted_iota(jnp.int32, (tokens, rows), 1)

    def chosen(r):
        slot = jnp.sum(jnp.where(lane == r, rank, 0.0), axis=-1, keepdims=True)
        target = r * cap + slot.astype(jnp.int32)
        return jnp.where(total_lane == target, 1.0, 0.0).astype(bf16)

    c0 = chosen(r0)
    c1 = chosen(r1)
    l0 = columns[:, 2:3]
    l1 = columns[:, 3:4]
    w0 = jax.nn.sigmoid(l0 - l1)
    w1 = jax.nn.sigmoid(l1 - l0)
    for c in (0, 2):
        to = ty if c == 0 else tx
        wait_in(mfar.at[c // 2], mf.at[c // 2])
        mpart[c, to] = (mpart[c, to].astype(f32) + mfar[c // 2].astype(f32)).astype(bf16)
        m_send(mpart.at[c, to], mrecv.at[c, 1 - c // 2], mr.at[c], to)

    wait_in(ret.at[pl.ds(0, n_ep - 1)], br.at[0])
    results = ret[...].astype(f32).reshape(rows, slab).astype(bf16)
    first = jnp.dot(c0, results, preferred_element_type=f32)
    second = jnp.dot(c1, results, preferred_element_type=f32)
    eout_ref[...] = (w0 * first + w1 * second).astype(bf16)
    for c in (1, 3, 0, 2):
        count = 2 + c % 2
        wait_in(mrecv.at[c, pl.ds(0, count)], mr.at[c])
        summed = mpart[c, t].astype(f32)
        for i in range(count):
            summed = summed + mrecv[c, i].astype(f32)
        mixed_ref[:, c * chunk : (c + 1) * chunk] = summed.astype(bf16)

    wait_out(disp.at[pl.ds(0, n_ep - 1)], ssem.at[0])
    wait_out(xq.at[pl.ds(0, 3)], ssem.at[1])

    @pl.when(inner)
    def _():
        wait_out(kv.at[:, 0], ssem.at[2])
        wait_out(kv.at[pl.ds(0, 3), 0], ssem.at[3])

    @pl.when(~inner)
    def _():
        wait_out(kv.at[pl.ds(0, 2), 0], ssem.at[3])

    wait_out(mrecv, ssem.at[5])
    wait_out(part.at[pl.ds(0, 3)], ssem.at[6])
    wait_out(back.at[pl.ds(0, n_ep - 1)], ssem.at[7])


def hand_over(a_ref, b_ref, a_out, b_out, sem):
    one = pltpu.make_async_copy(a_ref, a_out, sem.at[0])
    two = pltpu.make_async_copy(b_ref, b_out, sem.at[1])
    one.start()
    two.start()
    one.wait()
    two.wait()


def kernel_form(
    queries,
    keys,
    values,
    query_gain,
    key_gain,
    out_weight,
    expert_input,
    norm_gain,
    routes,
    route_logits,
    gate_weight,
    up_weight,
    down_weight,
):
    bf16, f32 = jnp.bfloat16, jnp.float32
    n_ep = lax.axis_size("ep")
    tokens = queries.shape[0]
    head_dim = query_gain.shape[0]
    heads = queries.shape[1] // head_dim
    kv_here = keys.shape[1] // head_dim
    width = expert_input.shape[1]
    n_tp = lax.axis_size("tp")
    slab = width // n_tp
    cap = tokens * routes.shape[1] // n_ep * 5 // 4
    rows = n_ep * cap
    ff = gate_weight.shape[2]
    share = tokens // n_tp
    chunk = out_weight.shape[1] // 4
    table = jnp.asarray(rope_constants(tokens * n_ep, head_dim))
    vmem = pl.BlockSpec(memory_space=pltpu.VMEM)
    hbm = pl.BlockSpec(memory_space=pl.ANY)
    piece = (n_ep, cap, slab)
    dma = pltpu.SemaphoreType.DMA
    dims = (n_ep, cap, head_dim, kv_here, heads // kv_here)
    outs = pl.pallas_call(
        functools.partial(fused, dims),
        name="fused",
        out_shape=(
            pltpu.VMEM((share, out_weight.shape[1]), bf16),
            pltpu.VMEM((tokens, slab), bf16),
        ),
        in_specs=[hbm] * 14,
        out_specs=(vmem, vmem),
        scratch_shapes=[
            pltpu.VMEM(queries.shape, bf16),
            pltpu.VMEM(keys.shape, bf16),
            pltpu.VMEM(expert_input.shape, bf16),
            pltpu.VMEM((1, width + 2 * head_dim), f32),
            pltpu.VMEM((2, tokens), jnp.int32),
            pltpu.VMEM((2, tokens), f32),
            pltpu.VMEM(out_weight.shape, bf16),
            pltpu.VMEM((2, ff, width), bf16),
            pltpu.VMEM(down_weight.shape[1:], bf16),
            pltpu.VMEM((2, tokens, head_dim), f32),
            pltpu.VMEM(piece, bf16),
            pltpu.VMEM((n_tp,) + piece, bf16),
            pltpu.VMEM((2, rows // 2, ff), f32),
            pltpu.VMEM((2, rows // 2, ff), f32),
            pltpu.VMEM((2, rows // 2, ff), bf16),
            pltpu.VMEM((n_tp,) + piece, bf16),
            pltpu.VMEM(piece, bf16),
            pltpu.VMEM((2,) + piece, bf16),
            pltpu.VMEM(piece, bf16),
            pltpu.VMEM(piece, bf16),
            pltpu.VMEM((kv_here, 2, n_ep // 2, 2, tokens, head_dim), bf16),
            pltpu.VMEM((heads, tokens, head_dim), bf16),
            pltpu.VMEM((kv_here, heads // kv_here, tokens, head_dim), bf16),
            pltpu.VMEM((kv_here, tokens, heads // kv_here * head_dim), bf16),
            pltpu.VMEM((kv_here, tokens, heads // kv_here * head_dim), bf16),
            pltpu.VMEM((tokens, width), f32),
            pltpu.VMEM((4, n_tp, share, chunk), bf16),
            pltpu.VMEM((2, share, chunk), bf16),
            pltpu.VMEM((4, 3, share, chunk), bf16),
            dma((11,)),
            dma((8,)),
            dma((7,)),
            dma((n_ep // 2 + 2,)),
            dma((n_ep // 2 + 2,)),
            dma((2,)),
            dma((kv_here, 3)),
            dma((kv_here,)),
            dma((kv_here,)),
            dma((2, 2)),
            dma((2, 2)),
            dma((1,)),
            dma((2,)),
            dma((4,)),
        ],
        compiler_params=pltpu.CompilerParams(
            collective_id=0, has_side_effects=True, vmem_limit_bytes=60 * 1024 * 1024
        ),
    )(
        queries,
        keys,
        values,
        query_gain.reshape(1, -1),
        key_gain.reshape(1, -1),
        out_weight,
        expert_input,
        norm_gain.reshape(1, -1),
        routes.T,
        route_logits.T,
        jnp.swapaxes(gate_weight, 1, 2),
        jnp.swapaxes(up_weight, 1, 2),
        down_weight,
        table,
    )
    return pl.pallas_call(
        hand_over,
        name="hand_over",
        out_shape=tuple(jax.ShapeDtypeStruct(o.shape, o.dtype) for o in outs),
        in_specs=[vmem, vmem],
        out_specs=(hbm, hbm),
        scratch_shapes=[dma((2,))],
    )(*(pltpu.with_memory_space_constraint(o, pltpu.VMEM) for o in outs))


def dispatch_form(mesh, *args):
    queries, routes = args[0], args[8]
    tokens = queries.shape[0]
    n_ep, n_tp = mesh.shape["ep"], mesh.shape["tp"]
    cap = tokens * routes.shape[1] // n_ep * 5 // 4
    same = args[6].shape[0] == tokens and tokens % 128 == 0
    fits = n_tp == 4 and n_ep == 8 and cap % 8 == 0
    if same and fits and routes.shape[1] == 2 and tokens == 128:
        return kernel_form(*args)
    return local(*args)


def solution(mesh):
    placed = (
        P("ep", "tp"),
        P("ep", "tp"),
        P("ep", "tp"),
        P(),
        P(),
        P("tp", None),
        P("ep", None),
        P(),
        P("ep", None),
        P("ep", None),
        P("ep", None, "tp"),
        P("ep", None, "tp"),
        P("ep", "tp", None),
    )
    return jax.shard_map(
        functools.partial(dispatch_form, mesh),
        mesh=mesh,
        in_specs=placed,
        out_specs=(P(("ep", "tp"), None), P("ep", "tp")),
        check_vma=False,
    )
```

```python
import functools
import jax
import jax.numpy as jnp
import numpy as np
from jax import lax
from jax.experimental import pallas as pl
from jax.experimental.pallas import tpu as pltpu
from jax.sharding import PartitionSpec as P

GRID_W = 64


def rope_tables(count, offset, head_dim):
    pos = offset + lax.iota(jnp.int32, count)
    grid_row = (pos // GRID_W).astype(jnp.float32)
    grid_col = (pos % GRID_W).astype(jnp.float32)
    quarter = head_dim // 4
    inverse = 10000.0 ** (-jnp.arange(quarter, dtype=jnp.float32) / quarter)
    angles = jnp.concatenate([grid_row[:, None] * inverse, grid_col[:, None] * inverse], axis=-1)
    return (jnp.cos(angles), jnp.sin(angles))


def norm_rotate(x, gain, cosine, sine):
    count, number, head_dim = x.shape
    y = x * lax.rsqrt(jnp.mean(x * x, axis=-1, keepdims=True) + 1e-06) * gain
    pairs = y.reshape(count, number, head_dim // 2, 2)
    first, second = (pairs[..., 0], pairs[..., 1])
    cos_b = cosine[:, None, :]
    sin_b = sine[:, None, :]
    turned = jnp.stack([first * cos_b - second * sin_b, first * sin_b + second * cos_b], axis=-1)
    return turned.reshape(count, number, head_dim).astype(jnp.bfloat16)


def key_block_size(length, shard_rows):
    if length <= 2048:
        return length
    shards = length // shard_rows
    most = max(1, 2048 // shard_rows)
    best = 1
    for count in range(1, most + 1):
        if shards % count == 0:
            best = count
    return best * shard_rows


def local(
    queries,
    keys,
    values,
    query_gain,
    key_gain,
    out_weight,
    expert_input,
    norm_gain,
    routes,
    route_logits,
    gate_weight,
    up_weight,
    down_weight,
):
    tokens_here = queries.shape[0]
    head_dim = query_gain.shape[0]
    heads_here = queries.shape[1] // head_dim
    kv_here = keys.shape[1] // head_dim
    group = heads_here // kv_here
    offset = lax.axis_index("ep") * tokens_here
    cosine, sine = rope_tables(tokens_here, offset, head_dim)
    q_rot = norm_rotate(
        queries.astype(jnp.float32).reshape(tokens_here, heads_here, head_dim),
        query_gain,
        cosine,
        sine,
    )
    k_rot = norm_rotate(
        keys.astype(jnp.float32).reshape(tokens_here, kv_here, head_dim), key_gain, cosine, sine
    ).reshape(tokens_here, kv_here * head_dim)
    q_grouped = q_rot.reshape(tokens_here, kv_here, group, head_dim).transpose(1, 2, 0, 3)
    q_grouped = q_grouped.reshape(kv_here, group * tokens_here, head_dim)
    query_rows = group * tokens_here
    scale = head_dim ** (-0.5)
    start_state = (
        jnp.full((kv_here, query_rows), -1e30, jnp.float32),
        jnp.zeros((kv_here, query_rows), jnp.float32),
        jnp.zeros((kv_here, query_rows, head_dim), jnp.float32),
    )
    key_piece = lax.all_gather(k_rot, "ep", axis=0, tiled=True)
    value_piece = lax.all_gather(values, "ep", axis=0, tiled=True)
    length = key_piece.shape[0]
    block = key_block_size(length, tokens_here)
    key_blocks = key_piece.reshape(length // block, block, kv_here, head_dim)
    value_blocks = value_piece.reshape(length // block, block, kv_here, head_dim)

    def step(state, blocks):
        running_max, running_total, running_sum = state
        key_block, value_block = blocks
        scores = (
            jnp.einsum("kqd,lkd->kql", q_grouped, key_block, preferred_element_type=jnp.float32)
            * scale
        )
        new_max = jnp.maximum(running_max, jnp.max(scores, axis=-1))
        factor = jnp.exp(running_max - new_max)
        weights = jnp.exp(scores - new_max[..., None])
        new_total = running_total * factor + jnp.sum(weights, axis=-1)
        new_sum = running_sum * factor[..., None] + jnp.einsum(
            "kql,lkd->kqd",
            weights.astype(jnp.bfloat16),
            value_block,
            preferred_element_type=jnp.float32,
        )
        return ((new_max, new_total, new_sum), None)

    result, _ = lax.scan(step, start_state, (key_blocks, value_blocks))
    final_max, final_total, final_sum = result
    attended = (final_sum / final_total[..., None]).astype(jnp.bfloat16)
    attended = attended.reshape(kv_here, group, tokens_here, head_dim).transpose(2, 0, 1, 3)
    attended = attended.reshape(tokens_here, heads_here * head_dim)
    summed = lax.psum_scatter(
        jnp.dot(attended, out_weight, preferred_element_type=jnp.float32).astype(jnp.bfloat16),
        "tp",
        scatter_dimension=0,
        tiled=True,
    ).astype(jnp.float32)
    mixed = summed.astype(jnp.bfloat16)
    expert_tokens_here, width = expert_input.shape
    n_ep = lax.axis_size("ep")
    top = routes.shape[1]
    capacity = expert_tokens_here * top // n_ep * 5 // 4
    x = expert_input.astype(jnp.float32)
    normed = (x * lax.rsqrt(jnp.mean(x * x, axis=-1, keepdims=True) + 1e-06) * norm_gain).astype(
        jnp.bfloat16
    )
    expert_ids = routes.reshape(-1)
    onehot = (expert_ids[:, None] == lax.iota(jnp.int32, n_ep)[None, :]).astype(jnp.int32)
    before = jnp.cumsum(onehot, axis=0) - onehot
    slot = jnp.sum(before * onehot, axis=1)
    target = expert_ids * capacity + slot
    owner_row = lax.iota(jnp.int32, expert_tokens_here * top) // top
    w_gate = gate_weight[0]
    w_up = up_weight[0]
    w_down = down_weight[0]
    columns = normed.shape[1]
    filled = jnp.zeros((n_ep * capacity, columns), jnp.bfloat16).at[target].set(normed[owner_row])
    arrived = lax.all_to_all(
        filled.reshape(n_ep, capacity, columns), "ep", split_axis=0, concat_axis=0, tiled=True
    )
    sources, slots, work_columns = arrived.shape
    flat = arrived.reshape(sources * slots, work_columns)
    gate = jnp.dot(flat, w_gate, preferred_element_type=jnp.float32)
    upper = jnp.dot(flat, w_up, preferred_element_type=jnp.float32)
    hidden = (jax.nn.silu(gate) * upper).astype(jnp.bfloat16)
    partial_out = jnp.dot(hidden, w_down, preferred_element_type=jnp.float32)
    summed = lax.psum_scatter(
        partial_out.reshape(sources, slots, width).astype(jnp.bfloat16),
        "tp",
        scatter_dimension=2,
        tiled=True,
    ).astype(jnp.float32)
    returned = lax.all_to_all(
        summed.astype(jnp.bfloat16), "ep", split_axis=0, concat_axis=0, tiled=True
    )
    picked = returned.reshape(n_ep * capacity, -1)[target].reshape(expert_tokens_here, top, -1)
    route_weight = jax.nn.sigmoid(route_logits - route_logits[:, ::-1])
    combined = jnp.sum(route_weight[..., None] * picked.astype(jnp.float32), axis=1)
    expert_out = combined.astype(jnp.bfloat16)
    return (mixed, expert_out)


MESH = pl.DeviceIdType.MESH


def rope_constants(length, head_dim):
    pos = np.arange(length)
    quarter = head_dim // 4
    inverse = (np.float32(10000.0) ** (-np.arange(quarter, dtype=np.float32) / np.float32(quarter))).astype(np.float32)
    grid_row = (pos // GRID_W).astype(np.float32)
    grid_col = (pos % GRID_W).astype(np.float32)
    angles = np.concatenate([grid_row[:, None] * inverse, grid_col[:, None] * inverse], axis=-1)
    cosine = np.repeat(np.cos(angles), 2, axis=-1).astype(np.float32)
    sine = np.repeat(np.sin(angles), 2, axis=-1).astype(np.float32)
    sine[:, 0::2] *= -1.0
    return np.stack([cosine, sine])


def fused(
    dims,
    q_hbm,
    k_hbm,
    v_hbm,
    qg_hbm,
    kg_hbm,
    wo_hbm,
    x_hbm,
    ng_hbm,
    rt_hbm,
    lg_hbm,
    wg_hbm,
    wu_hbm,
    wd_hbm,
    rope_hbm,
    mixed_ref,
    eout_ref,
    q_ref,
    k_ref,
    x_ref,
    gains,
    rt_ref,
    lg_ref,
    wo,
    wgu,
    wd,
    rope,
    disp,
    xq,
    gacc,
    uacc,
    hid,
    part,
    rdiag,
    rs,
    back,
    ret,
    kv,
    qrot,
    qship,
    att,
    aship,
    macc,
    mpart,
    mfar,
    mrecv,
    wsem,
    ssem,
    zr,
    axr,
    ayr,
    afr,
    kvr,
    kvm,
    qar,
    rdr,
    rsr,
    br,
    mf,
    mr,
):
    n_ep, cap, head_dim, kv_here, group = dims
    f32, bf16 = jnp.float32, jnp.bfloat16
    chips = n_ep // 2
    me = lax.axis_index("ep")
    t = lax.axis_index("tp")
    tx = t + 1 - 2 * (t % 2)
    ty = (t + 2) % 4
    td = 3 - t
    z = me // 2
    core = me % 2
    mate = 2 * z + 1 - core
    inner = (z == 1) | (z == 2)
    partner = z + 1 - 2 * (z % 2)
    other = 3 - z
    far_end = 3 - partner
    near = [jnp.where(inner, a, b) for a, b in ((other, partner), (partner, far_end), (far_end, other))]
    half = n_ep // 2
    order = [me, mate]
    for chip in near:
        order += [2 * chip + core, 2 * chip + 1 - core]
    sides_of = [(z, near[0]), (near[1], near[2])]
    turns = [order[:half][::-1], order[half:][::-1]]
    first_to = []
    for chip in (partner, other, far_end):
        first_to += [2 * chip + core, 2 * chip + 1 - core]
    tokens = x_ref.shape[0]
    slab = disp.shape[2]
    rows = n_ep * cap

    width = x_ref.shape[1]
    ends = (0, width, width + head_dim, width + 2 * head_dim)
    ng_ref, kg_ref, qg_ref = [gains.at[:, ends[i] : ends[i + 1]] for i in range(3)]

    def load(i, a, b):
        return pltpu.make_async_copy(a, b, wsem.at[i])

    def loaded(i, ref):
        load(i, ref, ref).wait()

    load(0, x_hbm, x_ref).start()
    load(1, rt_hbm, rt_ref).start()

    barrier = pltpu.get_barrier_semaphore()
    for d in range(1, n_ep):
        pl.semaphore_signal(barrier, inc=1, device_id={"ep": (me + d) % n_ep}, device_id_type=MESH)
    for peer in (tx, ty, td):
        pl.semaphore_signal(barrier, inc=1, device_id={"tp": peer}, device_id_type=MESH)
    load(2, ng_hbm, ng_ref).start()
    load(2, kg_hbm, kg_ref).start()
    load(2, qg_hbm, qg_ref).start()
    load(3, k_hbm, k_ref).start()
    load(4, rope_hbm.at[:, pl.ds(pl.multiple_of(me * tokens, tokens), tokens), :], rope).start()
    for g in range(kv_here):
        load(5, v_hbm.at[:, g * head_dim : (g + 1) * head_dim], kv.at[g, core, z, 1]).start()
    load(6, q_hbm, q_ref).start()
    load(7, lg_hbm, lg_ref).start()
    load(8, wg_hbm.at[0], wgu.at[0]).start()
    load(8, wu_hbm.at[0], wgu.at[1]).start()
    load(9, wd_hbm.at[0], wd).start()
    load(10, wo_hbm, wo).start()

    loaded(1, rt_ref)
    wide = (tokens, tokens)
    lane = lax.broadcasted_iota(jnp.int32, wide, 1)
    sub = lax.broadcasted_iota(jnp.int32, wide, 0)
    routed = (sub == rt_ref[0:1, :]) | (sub == rt_ref[1:2, :])
    named_t = jnp.where(routed, 1.0, 0.0)
    upper = jnp.where(sub < lane, 1.0, 0.0).astype(bf16)
    rank_t = jnp.dot(named_t.astype(bf16), upper, preferred_element_type=f32)
    slot_iota = lax.broadcasted_iota(jnp.int32, (cap, tokens), 0).astype(f32)
    picks = [
        jnp.where((slot_iota == rank_t[e : e + 1, :]) & (named_t[e : e + 1, :] > 0.5), 1.0, 0.0)
        for e in range(n_ep)
    ]
    pick = jnp.concatenate(picks, axis=0).astype(bf16)

    loaded(2, gains)
    loaded(0, x_ref)
    x = x_ref[...].astype(f32)
    inv = lax.rsqrt(jnp.mean(x * x, axis=-1, keepdims=True) + 1e-06)
    cols = pl.ds(pl.multiple_of(t * slab, slab), slab)
    normed = (x_ref[:, cols].astype(f32) * inv * ng_ref[:, cols]).astype(bf16)
    sent = jnp.dot(pick, normed, preferred_element_type=f32)
    for e in range(n_ep):
        disp[e] = sent[e * cap : (e + 1) * cap].astype(bf16)
    xq[t, me] = disp[me]

    pl.semaphore_wait(barrier, n_ep - 1 + 3)

    def remote(a, b, s, r, **where):
        return pltpu.make_async_remote_copy(
            src_ref=a, dst_ref=b, send_sem=s, recv_sem=r, device_id=where, device_id_type=MESH
        )

    def wait_in(ref, sem):
        remote(ref, ref, ssem.at[0], sem, tp=tx).wait_recv()

    def wait_out(ref, sem):
        remote(ref, ref, sem, zr.at[0], tp=tx).wait_send()

    for e, i in zip([mate] + first_to, range(n_ep - 1)):
        remote(disp.at[e], xq.at[t, me], ssem.at[0], zr.at[i], ep=e).start()

    def spread(i):
        s = order[i]
        rest = half + i // half
        at_x, at_y = (i // 2, rest) if i % 2 == 0 else (rest, i // 2)
        remote(xq.at[t, s], xq.at[t, s], ssem.at[1], axr.at[at_x], tp=tx).start()
        remote(xq.at[t, s], xq.at[t, s], ssem.at[1], ayr.at[at_y], tp=ty).start()

    def forward(i):
        s = order[i]
        if i % 2 == 0:
            wait_in(xq.at[tx, s], axr.at[i // 2])
            remote(xq.at[tx, s], xq.at[tx, s], ssem.at[1], afr.at[i // half], tp=ty).start()
        else:
            wait_in(xq.at[ty, s], ayr.at[i // 2])
            remote(xq.at[ty, s], xq.at[ty, s], ssem.at[1], afr.at[i // half], tp=tx).start()

    spread(0)

    loaded(4, rope)
    cos = rope[0]
    sin = rope[1]
    even = lax.broadcasted_iota(jnp.int32, (tokens, head_dim), 1) % 2 == 0

    def turn(piece, gain):
        a = piece.astype(f32)
        y = a * lax.rsqrt(jnp.mean(a * a, axis=-1, keepdims=True) + 1e-06) * gain
        other = jnp.where(even, pltpu.roll(y, head_dim - 1, 1), pltpu.roll(y, 1, 1))
        return (y * cos + other * sin).astype(bf16)

    loaded(3, k_ref)
    for g in range(kv_here):
        kv[g, core, z, 0] = turn(k_ref[:, g * head_dim : (g + 1) * head_dim], kg_ref[...])

    def kv_send(g, chip, to, kind):
        block = kv.at[g, core, chip]
        remote(block, block, ssem.at[3], kvr.at[g, kind], ep=2 * to + core).start()

    def kv_mate(g, chip):
        block = kv.at[g, core, chip]
        remote(block, block, ssem.at[2], kvm.at[g], ep=mate).start()

    loaded(5, kv.at[0, 0, pl.ds(0, kv_here // 2)])

    def receive(i):
        kind = 0
        if i > 1:
            for_inner, for_end = ((3, 1), (4, 2), (1, 5), (2, 6), (5, 3), (6, 4))[i - 2]
            kind = jnp.where(inner, for_inner, for_end)
        wait_in(xq.at[t, order[i]], zr.at[kind])
        spread(i)

    receive(1)
    loaded(6, q_ref)
    for h in range(kv_here * group):
        qrot[h] = turn(q_ref[:, h * head_dim : (h + 1) * head_dim], qg_ref[...])
    q_of = lambda g: qrot.at[pl.ds(g * group, group)]

    def gate_up(q, k, first=False):
        pieces = [xq[q, pl.ds(2 * chip, 2)].astype(f32).reshape(2 * cap, slab) for chip in sides_of[k]]
        block = jnp.concatenate(pieces, axis=0).astype(bf16)
        at = pl.ds(pl.multiple_of(q * slab, slab), slab)
        g = lax.dot_general(block, wgu[0, :, at], (((1,), (1,)), ((), ())), preferred_element_type=f32)
        u = lax.dot_general(block, wgu[1, :, at], (((1,), (1,)), ((), ())), preferred_element_type=f32)
        if first:
            gacc[k] = g
            uacc[k] = u
        else:
            gacc[k] += g
            uacc[k] += u

    def sides(k):
        wait_in(xq.at[tx, pl.ds(0, half // 2)], axr.at[half + k])
        wait_in(xq.at[ty, pl.ds(0, half // 2)], ayr.at[half + k])

    def corner(k):
        wait_in(xq.at[td, pl.ds(0, half)], afr.at[k])

    def activate(k):
        gate = gacc[k]
        hid[k] = (gate / (1.0 + jnp.exp(-gate)) * uacc[k]).astype(bf16)

    def down(q, k):
        at = pl.ds(pl.multiple_of(q * slab, slab), slab)
        out = jnp.dot(hid[k], wd[:, at], preferred_element_type=f32)
        for s in range(half):
            part[q, 2 * sides_of[k][s // 2] + s % 2] = out[s * cap : (s + 1) * cap].astype(bf16)

    def rx_copy(k, j):
        s = turns[k][j]
        remote(part.at[tx, s], rs.at[0, s], ssem.at[6], rsr.at[k, j // 2], tp=tx).start()

    def ry_copy(k, j):
        s = turns[k][j]
        remote(part.at[ty, s], rs.at[1, s], ssem.at[6], rsr.at[k, j // 2], tp=ty).start()

    def send_far(k):
        for j, s in enumerate(turns[k]):
            to = tx if j % 2 == 0 else ty
            remote(part.at[td, s], rdiag.at[s], ssem.at[6], rdr.at[k, j // 2], tp=to).start()

    def send_near(k):
        for j in range(0, half, 2):
            rx_copy(k, j)
            ry_copy(k, j + 1)

    def corner_far(k):
        corner(k)
        gate_up(td, k)
        activate(k)
        down(td, k)

    def down_rest(k):
        down(tx, k)
        down(ty, k)
        down(t, k)

    receive(2)
    receive(3)

    @pl.when(~inner)
    def _():
        for g in range(kv_here):
            kv_send(g, z, partner, 0)
        for g in range(kv_here):
            remote(q_of(g), qship.at[g], ssem.at[3], qar.at[g], ep=2 * partner + core).start()

    forward(0)
    forward(1)

    loaded(8, wgu)

    @pl.when(~inner)
    def _():
        forward(2)
        forward(3)
        gate_up(t, 0, True)

    receive(4)
    receive(5)

    @pl.when(inner)
    def _():
        kv_send(0, z, other, 1)
        kv_mate(0, z)
        gate_up(t, 0, True)
        forward(2)
        forward(3)

    receive(6)
    receive(7)

    def own_kv(heads):
        @pl.when(inner)
        def _():
            for g in heads:
                kv_send(g, z, other, 1)
                kv_mate(g, z)

    def relay_kv(heads, source, kind):
        @pl.when(inner)
        def _():
            for g in heads:
                block = kv.at[g, core, source]
                wait_in(block, kvr.at[g, kind])
                if kind == 0:
                    kv_send(g, source, other, 2)
                kv_mate(g, source)

    own_kv((1,))
    scale = head_dim ** (-0.5) * 1.4426950408889634

    def attend_one(g, q2):
        keys = kv[g, :, :, 0].reshape(n_ep * tokens, head_dim)
        vals = kv[g, :, :, 1].reshape(n_ep * tokens, head_dim)
        q2 = q2.reshape(group * tokens, head_dim)
        s = lax.dot_general(q2, keys, (((1,), (1,)), ((), ())), preferred_element_type=f32)
        peak = jnp.max(s, axis=-1, keepdims=True)
        p = jnp.exp2((s - peak) * scale)
        total = jnp.sum(p, axis=-1, keepdims=True)
        out = jnp.dot(p.astype(bf16), vals, preferred_element_type=f32) / total
        return jnp.concatenate([out[r * tokens : (r + 1) * tokens] for r in range(group)], axis=1).astype(bf16)

    def attend_ship(heads):
        @pl.when(inner)
        def _():
            for g in heads:
                wait_in(qship.at[g], qar.at[g])
                wait_in(kv.at[g, 1 - core], kvm.at[g])
                aship[g] = attend_one(g, qship[g])
                remote(aship.at[g], att.at[g], ssem.at[3], qar.at[kv_here - 1 if g == kv_here - 1 else 0], ep=2 * partner + core).start()

    def meet(k):
        for j, s in enumerate(turns[k]):
            if j % 2 == 0:
                wait_in(rdiag.at[pl.ds(0, 2)], rdr.at[k, j // 2])
                part[ty, s] = (part[ty, s].astype(f32) + rdiag[s].astype(f32)).astype(bf16)
                ry_copy(k, j)
            else:
                part[tx, s] = (part[tx, s].astype(f32) + rdiag[s].astype(f32)).astype(bf16)
                rx_copy(k, j)

    def finish(k):
        for j, s in enumerate(turns[k]):
            if j % 2 == 0:
                wait_in(rs.at[0, pl.ds(0, 4)], rsr.at[k, j // 2])
            out = (part[t, s].astype(f32) + rs[0, s].astype(f32) + rs[1, s].astype(f32)).astype(bf16)
            if k == 0 and j == half - 1:
                ret[s] = out
            else:
                back[s] = out
                remote(back.at[s], ret.at[me], ssem.at[7], br.at[0], ep=s).start()

    share = tokens // 4
    chunk = width // 4

    loaded(9, wd)
    sides(0)
    gate_up(tx, 0)
    gate_up(ty, 0)

    @pl.when(~inner)
    def _():
        corner_far(0)
        down_rest(0)
        send_far(0)

    forward(4)
    forward(5)
    relay_kv((0,), partner, 0)
    own_kv((2,))

    @pl.when(inner)
    def _():
        corner_far(0)
        send_far(0)

    forward(6)
    forward(7)
    relay_kv((1,), partner, 0)
    own_kv((3,))
    relay_kv((0, 1), other, 1)

    @pl.when(inner)
    def _():
        down_rest(0)

    send_near(0)
    relay_kv((2, 3), partner, 0)
    relay_kv((0,), far_end, 2)
    gate_up(t, 1, True)
    sides(1)
    gate_up(tx, 1)
    gate_up(ty, 1)
    meet(0)
    attend_ship((0,))
    relay_kv((2,), other, 1)
    relay_kv((1,), far_end, 2)
    corner_far(1)
    send_far(1)
    down_rest(1)
    send_near(1)
    attend_ship((1,))
    relay_kv((3,), other, 1)
    relay_kv((2,), far_end, 2)
    relay_kv((3,), far_end, 2)
    attend_ship((2, 3))
    finish(0)
    meet(1)

    @pl.when(inner)
    def _():
        for g in range(kv_here):
            att[g] = attend_one(g, qrot[g * group : (g + 1) * group])


    @pl.when(inner)
    def _():
        finish(1)


    def attended(first, count, i):
        @pl.when(~inner)
        def _():
            wait_in(att.at[pl.ds(first, count)], qar.at[i])

    attended(0, kv_here - 1, 0)
    loaded(10, wo)
    cut = (kv_here - 1) * group * head_dim
    early = jnp.concatenate([att[g] for g in range(kv_here - 1)], axis=1)
    macc[...] = jnp.dot(early, wo[:cut, :], preferred_element_type=f32)
    attended(kv_here - 1, 1, kv_here - 1)
    def m_send(a, b, sem, to):
        remote(a, b, ssem.at[5], sem, tp=to).start()

    for c in (0, 2, 1, 3):
        at = slice(c * chunk, (c + 1) * chunk)
        out = macc[:, at] + jnp.dot(att[kv_here - 1], wo[cut:, at], preferred_element_type=f32)
        for j in range(4):
            mpart[c, j] = out[j * share : (j + 1) * share].astype(bf16)
        if c % 2 == 0:
            to = tx if c == 0 else ty
            m_send(mpart.at[c, td], mfar.at[c // 2], mf.at[c // 2], to)
            m_send(mpart.at[c, to], mrecv.at[c, c // 2], mr.at[c], to)
        else:
            for i, to in ((2, td), (0, tx), (1, ty)):
                m_send(mpart.at[c, to], mrecv.at[c, i], mr.at[c], to)

    @pl.when(~inner)
    def _():
        finish(1)

    loaded(7, lg_ref)
    ids = rt_ref[...].astype(f32)
    logits = lg_ref[...]
    stacked = jnp.where(
        sub == 0,
        ids[0:1, :],
        jnp.where(sub == 1, ids[1:2, :], jnp.where(sub == 2, logits[0:1, :], logits[1:2, :])),
    )
    columns = stacked.T
    r0 = columns[:, 0:1].astype(jnp.int32)
    r1 = columns[:, 1:2].astype(jnp.int32)
    lower = jnp.where(lane < sub, 1.0, 0.0).astype(bf16)
    rank = jnp.dot(lower, named_t.T.astype(bf16), preferred_element_type=f32)
    total_lane = lax.broadcasted_iota(jnp.int32, (tokens, rows), 1)

    def chosen(r):
        slot = jnp.sum(jnp.where(lane == r, rank, 0.0), axis=-1, keepdims=True)
        target = r * cap + slot.astype(jnp.int32)
        return jnp.where(total_lane == target, 1.0, 0.0).astype(bf16)

    c0 = chosen(r0)
    c1 = chosen(r1)
    l0 = columns[:, 2:3]
    l1 = columns[:, 3:4]
    w0 = jax.nn.sigmoid(l0 - l1)
    w1 = jax.nn.sigmoid(l1 - l0)
    for c in (0, 2):
        to = ty if c == 0 else tx
        wait_in(mfar.at[c // 2], mf.at[c // 2])
        mpart[c, to] = (mpart[c, to].astype(f32) + mfar[c // 2].astype(f32)).astype(bf16)
        m_send(mpart.at[c, to], mrecv.at[c, 1 - c // 2], mr.at[c], to)

    wait_in(ret.at[pl.ds(0, n_ep - 1)], br.at[0])
    results = ret[...].astype(f32).reshape(rows, slab).astype(bf16)
    both = jnp.dot(jnp.concatenate([c0, c1], axis=0), results, preferred_element_type=f32)
    eout_ref[...] = (w0 * both[:tokens] + w1 * both[tokens:]).astype(bf16)
    for c in (1, 3, 0, 2):
        count = 2 + c % 2
        wait_in(mrecv.at[c, pl.ds(0, count)], mr.at[c])
        summed = mpart[c, t].astype(f32)
        for i in range(count):
            summed = summed + mrecv[c, i].astype(f32)
        mixed_ref[:, c * chunk : (c + 1) * chunk] = summed.astype(bf16)

    wait_out(disp.at[pl.ds(0, n_ep - 1)], ssem.at[0])
    wait_out(xq.at[pl.ds(0, 3)], ssem.at[1])

    @pl.when(inner)
    def _():
        wait_out(kv.at[:, 0], ssem.at[2])
        wait_out(kv.at[pl.ds(0, 3), 0], ssem.at[3])

    @pl.when(~inner)
    def _():
        wait_out(kv.at[pl.ds(0, 2), 0], ssem.at[3])

    wait_out(mrecv, ssem.at[5])
    wait_out(part.at[pl.ds(0, 3)], ssem.at[6])
    wait_out(back.at[pl.ds(0, n_ep - 1)], ssem.at[7])


def hand_over(a_ref, b_ref, a_out, b_out, sem):
    one = pltpu.make_async_copy(a_ref, a_out, sem.at[0])
    two = pltpu.make_async_copy(b_ref, b_out, sem.at[1])
    one.start()
    two.start()
    one.wait()
    two.wait()


def kernel_form(
    queries,
    keys,
    values,
    query_gain,
    key_gain,
    out_weight,
    expert_input,
    norm_gain,
    routes,
    route_logits,
    gate_weight,
    up_weight,
    down_weight,
):
    bf16, f32 = jnp.bfloat16, jnp.float32
    n_ep = lax.axis_size("ep")
    tokens = queries.shape[0]
    head_dim = query_gain.shape[0]
    heads = queries.shape[1] // head_dim
    kv_here = keys.shape[1] // head_dim
    width = expert_input.shape[1]
    n_tp = lax.axis_size("tp")
    slab = width // n_tp
    cap = tokens * routes.shape[1] // n_ep * 5 // 4
    rows = n_ep * cap
    ff = gate_weight.shape[2]
    share = tokens // n_tp
    chunk = out_weight.shape[1] // 4
    table = jnp.asarray(rope_constants(tokens * n_ep, head_dim))
    vmem = pl.BlockSpec(memory_space=pltpu.VMEM)
    hbm = pl.BlockSpec(memory_space=pl.ANY)
    piece = (n_ep, cap, slab)
    dma = pltpu.SemaphoreType.DMA
    dims = (n_ep, cap, head_dim, kv_here, heads // kv_here)
    outs = pl.pallas_call(
        functools.partial(fused, dims),
        name="fused",
        out_shape=(
            pltpu.VMEM((share, out_weight.shape[1]), bf16),
            pltpu.VMEM((tokens, slab), bf16),
        ),
        in_specs=[hbm] * 14,
        out_specs=(vmem, vmem),
        scratch_shapes=[
            pltpu.VMEM(queries.shape, bf16),
            pltpu.VMEM(keys.shape, bf16),
            pltpu.VMEM(expert_input.shape, bf16),
            pltpu.VMEM((1, width + 2 * head_dim), f32),
            pltpu.VMEM((2, tokens), jnp.int32),
            pltpu.VMEM((2, tokens), f32),
            pltpu.VMEM(out_weight.shape, bf16),
            pltpu.VMEM((2, ff, width), bf16),
            pltpu.VMEM(down_weight.shape[1:], bf16),
            pltpu.VMEM((2, tokens, head_dim), f32),
            pltpu.VMEM(piece, bf16),
            pltpu.VMEM((n_tp,) + piece, bf16),
            pltpu.VMEM((2, rows // 2, ff), f32),
            pltpu.VMEM((2, rows // 2, ff), f32),
            pltpu.VMEM((2, rows // 2, ff), bf16),
            pltpu.VMEM((n_tp,) + piece, bf16),
            pltpu.VMEM(piece, bf16),
            pltpu.VMEM((2,) + piece, bf16),
            pltpu.VMEM(piece, bf16),
            pltpu.VMEM(piece, bf16),
            pltpu.VMEM((kv_here, 2, n_ep // 2, 2, tokens, head_dim), bf16),
            pltpu.VMEM((heads, tokens, head_dim), bf16),
            pltpu.VMEM((kv_here, heads // kv_here, tokens, head_dim), bf16),
            pltpu.VMEM((kv_here, tokens, heads // kv_here * head_dim), bf16),
            pltpu.VMEM((kv_here, tokens, heads // kv_here * head_dim), bf16),
            pltpu.VMEM((tokens, width), f32),
            pltpu.VMEM((4, n_tp, share, chunk), bf16),
            pltpu.VMEM((2, share, chunk), bf16),
            pltpu.VMEM((4, 3, share, chunk), bf16),
            dma((11,)),
            dma((8,)),
            dma((7,)),
            dma((n_ep // 2 + 2,)),
            dma((n_ep // 2 + 2,)),
            dma((2,)),
            dma((kv_here, 3)),
            dma((kv_here,)),
            dma((kv_here,)),
            dma((2, 2)),
            dma((2, 2)),
            dma((1,)),
            dma((2,)),
            dma((4,)),
        ],
        compiler_params=pltpu.CompilerParams(
            collective_id=0, has_side_effects=True, vmem_limit_bytes=60 * 1024 * 1024
        ),
    )(
        queries,
        keys,
        values,
        query_gain.reshape(1, -1),
        key_gain.reshape(1, -1),
        out_weight,
        expert_input,
        norm_gain.reshape(1, -1),
        routes.T,
        route_logits.T,
        jnp.swapaxes(gate_weight, 1, 2),
        jnp.swapaxes(up_weight, 1, 2),
        down_weight,
        table,
    )
    return pl.pallas_call(
        hand_over,
        name="hand_over",
        out_shape=tuple(jax.ShapeDtypeStruct(o.shape, o.dtype) for o in outs),
        in_specs=[vmem, vmem],
        out_specs=(hbm, hbm),
        scratch_shapes=[dma((2,))],
    )(*(pltpu.with_memory_space_constraint(o, pltpu.VMEM) for o in outs))


def dispatch_form(mesh, *args):
    queries, routes = args[0], args[8]
    tokens = queries.shape[0]
    n_ep, n_tp = mesh.shape["ep"], mesh.shape["tp"]
    cap = tokens * routes.shape[1] // n_ep * 5 // 4
    same = args[6].shape[0] == tokens and tokens % 128 == 0
    fits = n_tp == 4 and n_ep == 8 and cap % 8 == 0
    if same and fits and routes.shape[1] == 2 and tokens == 128:
        return kernel_form(*args)
    return local(*args)


def solution(mesh):
    placed = (
        P("ep", "tp"),
        P("ep", "tp"),
        P("ep", "tp"),
        P(),
        P(),
        P("tp", None),
        P("ep", None),
        P(),
        P("ep", None),
        P("ep", None),
        P("ep", None, "tp"),
        P("ep", None, "tp"),
        P("ep", "tp", None),
    )
    return jax.shard_map(
        functools.partial(dispatch_form, mesh),
        mesh=mesh,
        in_specs=placed,
        out_specs=(P(("ep", "tp"), None), P("ep", "tp")),
        check_vma=False,
    )
```
